32 devices in a mesh: sp: 4 (over z), fs: 4 (over y, x), tp: 2 (over core).
Axes of the slice: x: 2, y: 2, z: 4, core: 2. Of those that a mesh axis runs over, the one named last changes fastest.
Arguments:
- tokens: bfloat16 [512, 2048], P(('sp', 'fs', 'tp')), may hold values from -16 to 16
- in_gain: float32 [2048], replicated, may hold values from 0.1 to 1.9
- ret_query: bfloat16 [2048, 1024], P(None, ('fs', 'tp')), may hold values from -0.125 to 0.125
- ret_key: bfloat16 [2048, 1024], P(None, ('fs', 'tp')), may hold values from -0.125 to 0.125
- ret_value: bfloat16 [2048, 1024], P(None, ('fs', 'tp')), may hold values from -0.125 to 0.125
- decay_log: float32 [8, 512], P(('fs', 'tp'), 'sp'), may hold values from -1 to 0
- init_state: bfloat16 [8, 128, 128], P(('fs', 'tp')), may hold values from -24 to 24
- ret_gain: float32 [1024], P(('fs', 'tp')), may hold values from 0.1 to 1.9
- diff_query: bfloat16 [2, 2048, 512], P(None, None, ('fs', 'tp')), may hold values from -1 to 1
- diff_key: bfloat16 [2, 2048, 512], P(None, None, ('fs', 'tp')), may hold values from -1 to 1
- diff_value: bfloat16 [2048, 1024], P(None, ('fs', 'tp')), may hold values from -0.125 to 0.125
- diff_lambda: float32 [8], P(('fs', 'tp')), may hold values from 0.3 to 0.8
- diff_gain: float32 [1024], P(('fs', 'tp')), may hold values from 0.1 to 1.9
- out_weight: bfloat16 [2, 1024, 2048], P(None, ('fs', 'tp'), 'sp'), may hold values from -0.125 to 0.125
Outputs:
- mixed: bfloat16 [512, 2048], P(('sp', 'fs', 'tp'))
The draws below stay inside these ranges and needn't reach their ends.
All inputs are finite; a program needn't handle non-finite values.
Results may differ from the reference program's by a relative error of at most 0.017.
Values may be sent and summed in bfloat16 or wider, within the bound.
A program may use at most 64 MiB of HBM per device.

```python
import jax
import jax.numpy as jnp
from jax import lax

D = 2048
KEEPING_MIXERS = 8
DIFF_HEADS = 8
HEAD = 128
MAP = 64
RBLOCK = 128
SHARD_POSITIONS = 128
TOKEN_COUNT = 512
N_SP = 4


def draw_tokens(key, part):
    sample = jax.random.normal(jax.random.fold_in(key, 11), (TOKEN_COUNT, D), jnp.float32)
    return jnp.clip(sample, -16.0, 16.0).astype(jnp.bfloat16)


def projection_draw(key, salt):
    sample = jax.random.normal(jax.random.fold_in(key, salt), (2, D, DIFF_HEADS * MAP), jnp.float32) * (1.3 * D ** (-0.5))
    return jnp.clip(sample, -1.0, 1.0)


def draw_diff_query(key, part):
    return projection_draw(key, 21).astype(jnp.bfloat16)


def draw_diff_key(key, part):
    return projection_draw(key, 22).astype(jnp.bfloat16)


def draw_decay_log(key, part):
    head_shape = (KEEPING_MIXERS, 1)
    slow_share = 0.5
    slow_heads = jax.random.uniform(jax.random.fold_in(key, 31), head_shape) < slow_share
    fast_rate = jax.random.uniform(jax.random.fold_in(key, 32), head_shape, minval=1.0 / 60.0, maxval=1.0 / 30.0)
    slow_rate = jax.random.uniform(jax.random.fold_in(key, 33), head_shape, minval=0.05, maxval=0.3) / TOKEN_COUNT
    single_tick_fading = jnp.where(slow_heads, slow_rate, fast_rate)
    fading_multiplier = jax.random.uniform(jax.random.fold_in(key, 34), (1, TOKEN_COUNT // SHARD_POSITIONS, 1), minval=1.0, maxval=3.0)
    fading_multiplier = jnp.broadcast_to(fading_multiplier, (1, TOKEN_COUNT // SHARD_POSITIONS, SHARD_POSITIONS)).reshape(1, TOKEN_COUNT)
    spurt_clusters = jax.random.uniform(jax.random.fold_in(key, 35), (KEEPING_MIXERS, TOKEN_COUNT)) < 3.0 / TOKEN_COUNT
    fading_drops = jnp.log(jax.random.uniform(jax.random.fold_in(key, 36), (KEEPING_MIXERS, TOKEN_COUNT), minval=0.5, maxval=0.8))
    return -single_tick_fading * fading_multiplier + jnp.where(spurt_clusters, fading_drops, 0.0)


def level_of(key, extent, shards, smallest, largest):
    def one(axis_at, blocks):
        heights = jax.random.uniform(jax.random.fold_in(jax.random.fold_in(key, 6), axis_at), (blocks,), jnp.float32, smallest / len(shards), largest / len(shards))
        return jnp.repeat(jnp.exp(heights), extent[axis_at] // blocks).reshape((-1,) + (1,) * (len(extent) - axis_at - 1))

    level = one(*shards[0])
    for cut in shards[1:]:
        level = level * one(*cut)
    return level


def normal_values(rng, dims, spread, most, shards=(), kind=jnp.bfloat16):
    values = jax.random.normal(rng, dims, jnp.float32) * spread
    if len(shards) > 0:
        values = level_of(rng, dims, shards, -0.22, 0.18) * values
    return jnp.clip(values, min=-most, max=most).astype(kind)


def setup_inputs(seed: int = 0) -> dict:
    keys = jax.random.split(jax.random.key(seed), 15)
    return {
        "tokens": draw_tokens(jax.random.fold_in(keys[14], 71), 0),
        "in_gain": jnp.clip(1.0 + 0.18 * jax.random.normal(keys[1], (D,), jnp.float32), 0.1, 1.9),
        "ret_query": normal_values(keys[2], (D, KEEPING_MIXERS * HEAD), D ** -0.5, 0.125, ((1, 8),)),
        "ret_key": normal_values(keys[3], (D, KEEPING_MIXERS * HEAD), D ** -0.5, 0.125, ((1, 8),)),
        "ret_value": normal_values(keys[4], (D, KEEPING_MIXERS * HEAD), D ** -0.5, 0.125, ((1, 8),)),
        "decay_log": draw_decay_log(jax.random.fold_in(keys[14], 71), 0),
        "init_state": normal_values(keys[6], (KEEPING_MIXERS, HEAD, HEAD), 4.0, 24.0, ((0, 8),)),
        "ret_gain": jnp.clip(1.0 + 0.18 * jax.random.normal(keys[7], (KEEPING_MIXERS * HEAD,), jnp.float32), 0.1, 1.9),
        "diff_query": draw_diff_query(jax.random.fold_in(keys[14], 71), 0),
        "diff_key": draw_diff_key(jax.random.fold_in(keys[14], 71), 0),
        "diff_value": normal_values(keys[10], (D, DIFF_HEADS * HEAD), D ** -0.5, 0.125, ((1, 8),)),
        "diff_lambda": jnp.clip(0.3 + 0.5 * jax.random.uniform(keys[11], (DIFF_HEADS,), jnp.float32) ** level_of(keys[11], (DIFF_HEADS,), ((0, 8),), -0.2, 0.2), 0.3, 0.8),
        "diff_gain": jnp.clip(1.0 + 0.18 * jax.random.normal(keys[12], (DIFF_HEADS * HEAD,), jnp.float32), 0.1, 1.9),
        "out_weight": normal_values(keys[13], (2, KEEPING_MIXERS * HEAD, D), (2 * KEEPING_MIXERS * HEAD) ** -0.5, 0.125, ((1, 8), (2, 4))),
    }


EPS = 1e-06
HUGE = 1e+30
UPPER_LIMIT = lax.Precision.HIGHEST

def norm_rows(rows, gain):
    widened = rows.astype(jnp.float32)
    fading_multiplier = lax.rsqrt(lax.optimization_barrier(jnp.mean(widened * widened, axis=-1, keepdims=True)) + EPS)
    return (widened * fading_multiplier * gain).astype(jnp.bfloat16)

def split_heads(normed, weight, width):
    result = jnp.dot(normed, weight, preferred_element_type=jnp.float32).astype(jnp.bfloat16)
    return jnp.transpose(result.reshape(1, TOKEN_COUNT, -1, width), (2, 0, 1, 3))

def group_norm(output, gain):
    centre = output - lax.optimization_barrier(jnp.mean(output, axis=-1, keepdims=True))
    fading_multiplier = lax.rsqrt(lax.optimization_barrier(jnp.mean(centre * centre, axis=-1, keepdims=True)) + EPS)
    return (centre * fading_multiplier * gain).astype(jnp.bfloat16)

def retention_head(query_rows, key_rows, value_rows, log_rates, start_state):
    seq_total = query_rows.shape[0]
    head_size = query_rows.shape[2]
    blocks = TOKEN_COUNT // RBLOCK

    def to_blocks(array):
        return jnp.swapaxes(array.reshape((seq_total, blocks, RBLOCK) + array.shape[2:]), 0, 1)
    lower = jnp.arange(RBLOCK)[:, None] >= jnp.arange(RBLOCK)[None, :]

    def advance(carried_state, inputs):
        block_queries, block_keys, block_values, block_rates = inputs
        cumulative_decay = jnp.cumsum(block_rates, axis=-1)
        gaps = jnp.where(lower, cumulative_decay[:, :, None] - cumulative_decay[:, None, :], -HUGE)
        widened_queries = block_queries.astype(jnp.float32)
        keys_wide = block_keys.astype(jnp.float32)
        widened_values = block_values.astype(jnp.float32)
        scores = jnp.einsum('sik,sjk->sij', widened_queries, keys_wide) * head_size ** (-0.5) * jnp.exp(gaps)
        rounded = lax.optimization_barrier(scores.astype(jnp.bfloat16)).astype(jnp.float32)
        inner = jnp.einsum('sij,sjv->siv', rounded, widened_values)
        reached_length = jnp.einsum('wny,wyo->wno', widened_queries * jnp.exp(cumulative_decay)[:, :, None], carried_state, precision=UPPER_LIMIT)
        ending_index = cumulative_decay[:, -1]
        weighted_values = keys_wide * (jnp.exp(ending_index[:, None] - cumulative_decay) * head_size ** (-0.5))[:, :, None]
        carried_state = jnp.exp(ending_index)[:, None, None] * carried_state + jnp.einsum('bdg,bdl->bgl', weighted_values, widened_values, precision=UPPER_LIMIT)
        return (carried_state, inner + reached_length)
    _, output = lax.scan(advance, start_state, (to_blocks(query_rows), to_blocks(key_rows), to_blocks(value_rows), to_blocks(log_rates)))
    return jnp.swapaxes(output, 0, 1).reshape(seq_total, TOKEN_COUNT, head_size)

def absorb(running, query_rows, key_rows, value_rows, allowed):
    peak_old, total_old, sum_old = running
    scores = jnp.einsum('...qd,...kd->...qk', query_rows.astype(jnp.float32), key_rows.astype(jnp.float32)) * query_rows.shape[-1] ** (-0.5)
    if allowed is not None:
        scores = jnp.where(allowed, scores, -HUGE)
    block_peak = lax.optimization_barrier(jnp.max(scores, axis=-1))
    weights = jnp.exp(scores - block_peak[..., None])
    block_total = lax.optimization_barrier(jnp.sum(weights, axis=-1))
    rounded = lax.optimization_barrier(weights.astype(jnp.bfloat16)).astype(jnp.float32)
    block_sum = jnp.einsum('...qk,...kv->...qv', rounded, value_rows.astype(jnp.float32))
    new_peak = jnp.maximum(peak_old, block_peak)
    before = jnp.exp(peak_old - new_peak)
    after = jnp.exp(block_peak - new_peak)
    return (new_peak, total_old * before + block_total * after, sum_old * before[..., None] + block_sum * after[..., None])

def diff_head(first_query, second_query, first_key, second_key, value_rows, lambda_head, gain):
    seq_total = first_query.shape[0]
    blocks = N_SP

    def as_blocks(array):
        return array.reshape(seq_total, blocks, SHARD_POSITIONS, array.shape[-1])
    within = jnp.arange(SHARD_POSITIONS)[:, None] >= jnp.arange(SHARD_POSITIONS)[None, :]
    queries = (as_blocks(first_query), as_blocks(second_query))
    key_sets = (as_blocks(first_key), as_blocks(second_key))
    values = as_blocks(value_rows)
    results = []
    for branch in range(2):
        running = (jnp.full((seq_total, blocks, SHARD_POSITIONS), -HUGE, jnp.float32), jnp.zeros((seq_total, blocks, SHARD_POSITIONS), jnp.float32), jnp.zeros((seq_total, blocks, SHARD_POSITIONS, values.shape[-1]), jnp.float32))
        for distance in range(blocks):
            allowed = within if distance == 0 else None
            fresh = absorb(tuple((member[:, distance:] for member in running)), queries[branch][:, distance:], key_sets[branch][:, :blocks - distance], values[:, :blocks - distance], allowed)
            running = tuple((member.at[:, distance:].set(update) for member, update in zip(running, fresh)))
        results.append(running)
    mixed = results[0][2] / results[0][1][..., None] - lambda_head * results[1][2] / results[1][1][..., None]
    mixed = mixed.reshape(seq_total, TOKEN_COUNT, -1)
    fading_multiplier = lax.rsqrt(lax.optimization_barrier(jnp.mean(mixed * mixed, axis=-1, keepdims=True)) + EPS)
    return (mixed * fading_multiplier * gain).astype(jnp.bfloat16)

def reference(tokens, in_gain, ret_query, ret_key, ret_value, decay_log, init_state, ret_gain, diff_query, diff_key, diff_value, diff_lambda, diff_gain, out_weight):
    normed = norm_rows(tokens, in_gain)
    ret_queries = split_heads(normed, ret_query, HEAD)
    ret_keys = split_heads(normed, ret_key, HEAD)
    ret_values = split_heads(normed, ret_value, HEAD)
    first_query = split_heads(normed, diff_query[0], MAP)
    second_query = split_heads(normed, diff_query[1], MAP)
    first_key = split_heads(normed, diff_key[0], MAP)
    second_key = split_heads(normed, diff_key[1], MAP)
    diff_values = split_heads(normed, diff_value, HEAD)
    rates = decay_log.reshape(KEEPING_MIXERS, 1, TOKEN_COUNT)
    starts = init_state.astype(jnp.float32).reshape(KEEPING_MIXERS, 1, HEAD, HEAD)

    def retention_item(head_items):
        output = retention_head(head_items[0], head_items[1], head_items[2], head_items[3], head_items[4])
        return group_norm(output, head_items[5])
    ret_mix = lax.map(retention_item, (ret_queries, ret_keys, ret_values, rates, starts, ret_gain.reshape(KEEPING_MIXERS, HEAD)))

    def diff_item(head_items):
        return diff_head(head_items[0], head_items[1], head_items[2], head_items[3], head_items[4], head_items[5], head_items[6])
    diff_mix = lax.map(diff_item, (first_query, second_query, first_key, second_key, diff_values, diff_lambda, diff_gain.reshape(DIFF_HEADS, HEAD)))
    ret_rows = out_weight[0].reshape(KEEPING_MIXERS, HEAD, D)
    diff_rows = out_weight[1].reshape(DIFF_HEADS, HEAD, D)

    def add_head(running_total, head_items):
        ret_part, diff_part, ret_weight, diff_weight = head_items
        partial_value = jnp.dot(ret_part.reshape(-1, HEAD), ret_weight, preferred_element_type=jnp.float32)
        partial_value = partial_value + jnp.dot(diff_part.reshape(-1, HEAD), diff_weight, preferred_element_type=jnp.float32)
        return (running_total + lax.optimization_barrier(partial_value.astype(jnp.bfloat16)).astype(jnp.float32), None)
    summed, _ = lax.scan(add_head, jnp.zeros((TOKEN_COUNT, D), jnp.float32), (ret_mix, diff_mix, ret_rows, diff_rows))
    return summed.astype(jnp.bfloat16)
```

```python
import functools

import jax
import jax.numpy as jnp
from jax import lax
from jax.experimental import pallas as pl
from jax.experimental.pallas import tpu as pltpu
from jax.sharding import PartitionSpec as P

EPS = 1e-06
HUGE = 1e30
TOKEN_CHUNKS = 1
DIAG = "DDDD"
FAR = 9
SEQUENCE = ("c1", "s0", "c2", "d0", "s1", "c3", "p0", "d1", "s2", "p1", "d2", "s3", "d3", "p2", "p3")
f32 = jnp.float32
bf16 = jnp.bfloat16


def kernel(
    sizes,
    tokens,
    in_gain,
    ret_query,
    ret_key,
    ret_value,
    decay_log,
    init_state,
    ret_gain,
    diff_query,
    diff_key,
    diff_value,
    diff_lambda,
    diff_gain,
    out_weight,
    out,
    x_all,
    w_all,
    w_pair,
    tok_in,
    gain_in,
    decay_in,
    init_in,
    ret_gain_in,
    lambda_in,
    diff_gain_in,
    kv,
    st,
    wo,
    part,
    sib,
    red,
    rcv,
    load_sem,
    tok_send,
    tok_recv,
    fwd_send,
    kv_send,
    kv_recv,
    st_send,
    st_recv,
    wo_send,
    wo_recv,
    sib_send,
    sib_recv,
    rs_send,
    rs_recv,
):
    n_sp, n_fs, n_tp, ring = sizes
    own_rows, width = tokens.shape
    rows = own_rows * n_fs * n_tp
    head = ret_query.shape[1]
    maps = diff_query.shape[0] // 2
    sp, fs, tp = lax.axis_index("sp"), lax.axis_index("fs"), lax.axis_index("tp")
    half = max(n_fs // 2, 1)
    fs_peers = []
    for d in range(1, n_fs):
        if n_fs % 2 == 0:
            fs_peers.append(
                lax.rem(lax.div(fs, 2) + d // 2, half) * 2 + lax.rem(lax.rem(fs, 2) + d % 2, 2)
            )
        else:
            fs_peers.append(lax.rem(fs + d, n_fs))
    tp_peers = [lax.rem(tp + d, n_tp) for d in range(1, n_tp)]

    def remote(src, dst, send, recv, s, f, t):
        return pltpu.make_async_remote_copy(
            src_ref=src,
            dst_ref=dst,
            send_sem=send,
            recv_sem=recv,
            device_id=(s, f, t),
            device_id_type=pl.DeviceIdType.MESH,
        )

    barrier = pltpu.get_barrier_semaphore()

    def greet(s, f, t):
        pl.semaphore_signal(
            barrier, inc=1, device_id=(s, f, t), device_id_type=pl.DeviceIdType.MESH
        )

    for f in fs_peers:
        greet(sp, f, tp)
    for t in tp_peers:
        greet(sp, fs, t)

    def greet_sp(d, c):
        greet(lax.rem(sp + d, n_sp), fs, tp)
        return c

    if n_sp <= 8:
        for d in range(1, n_sp):
            greet_sp(d, 0)
    else:
        lax.fori_loop(1, n_sp, greet_sp, 0)

    def col(slot):
        return w_all.at[:, pl.ds(slot * head, head)]

    loads = [
        (tokens, tok_in),
        (in_gain, gain_in),
        (decay_log, decay_in),
        (init_state, init_in),
        (ret_gain, ret_gain_in),
        (diff_lambda, lambda_in),
        (diff_gain, diff_gain_in),
        (ret_query, col(0)),
        (ret_key, col(1)),
        (ret_value, col(2)),
        (diff_value, col(3)),
        (diff_key, w_pair.at[pl.ds(0, head)]),
        (diff_query, w_pair.at[pl.ds(head, head)]),
    ]
    load_copies = [
        pltpu.make_async_copy(src, dst, load_sem.at[i]) for i, (src, dst) in enumerate(loads)
    ]
    for c in load_copies:
        c.start()
    if ring:
        own_wo = pltpu.make_async_copy(out_weight, wo.at[sp], load_sem.at[len(loads)])
        own_wo.start()

    me = fs * n_tp + tp
    own = pl.ds(pl.multiple_of(me * own_rows, own_rows), own_rows)
    load_copies[0].wait()
    load_copies[1].wait()
    wide = tok_in[...].astype(f32)
    scale = lax.rsqrt(jnp.mean(wide * wide, axis=-1, keepdims=True) + EPS)
    x_all[own, :] = (wide * scale * gain_in[...].reshape(1, width)).astype(bf16)

    pl.semaphore_wait(barrier, len(fs_peers) + len(tp_peers) + n_sp - 1)

    cw = width // TOKEN_CHUNKS

    def block(rank, c):
        return x_all.at[
            pl.ds(pl.multiple_of(rank * own_rows, own_rows), own_rows), pl.ds(c * cw, cw)
        ]

    def tok_copy(c, rank, send, f, t):
        return remote(block(rank, c), block(rank, c), send, tok_recv.at[c, rank], sp, f, t)

    pending = []
    for c in range(TOKEN_CHUNKS):
        for i, f in enumerate(fs_peers):
            cp = tok_copy(c, me, tok_send.at[c, i], f, tp)
            cp.start()
            pending.append(cp)
        for i, t in enumerate(tp_peers):
            cp = tok_copy(c, me, fwd_send.at[c, n_fs - 1, i], fs, t)
            cp.start()
            pending.append(cp)

    def wo_copy(origin, way, step):
        src = out_weight if step == 0 else wo.at[origin]
        dest = sp + 1 - 2 * way
        return remote(
            src, wo.at[origin], wo_send.at[way, step], wo_recv.at[origin], dest, fs, tp
        )

    def each_way(step, go):
        for way in range(2):
            origin = sp - step if way == 0 else sp + step
            inside = origin >= 0 if way == 0 else origin < n_sp
            onward = sp < n_sp - 1 if way == 0 else sp > 0

            @pl.when(jnp.logical_and(inside, onward))
            def _():
                go(wo_copy(lax.rem(origin + n_sp, n_sp), way, step))

    def pass_on(step):
        def go(cp):
            if step:
                cp.wait_recv()
            cp.start()

        each_way(step, go)

    if ring:
        pass_on(0)

    load_copies[2].wait()
    d_row = decay_in[...]
    row_at = lax.broadcasted_iota(jnp.int32, (rows, rows), 0)
    col_at = lax.broadcasted_iota(jnp.int32, (rows, rows), 1)
    lower = row_at >= col_at
    d_wide = jnp.broadcast_to(d_row, (rows, rows))
    cum_col = jnp.sum(jnp.where(lower, d_wide, 0.0), axis=1, keepdims=True)
    d_col = jnp.sum(jnp.where(row_at == col_at, d_wide, 0.0), axis=1, keepdims=True)
    cum_row = jnp.sum(jnp.where(row_at <= col_at, d_col, 0.0), axis=0, keepdims=True)
    cum_last = jnp.sum(d_row, axis=1, keepdims=True)
    fade = jnp.exp(jnp.where(lower, cum_col - cum_row, -HUGE)) * head ** (-0.5)
    key_weight = jnp.exp(cum_last - cum_col) * head ** (-0.5)
    query_weight = jnp.exp(cum_col)
    decay = jnp.broadcast_to(jnp.exp(cum_last), (own_rows, head))
    decay_high = decay.astype(bf16).astype(f32)
    first = lax.broadcasted_iota(jnp.int32, (own_rows, head), 0) < own_rows // 2
    st[sp, pl.ds(head, own_rows), :] = jnp.where(first, decay_high, decay - decay_high).astype(bf16)

    for c in load_copies[3:]:
        c.wait()

    total = None
    for c in range(TOKEN_CHUNKS):
        if ring and c == TOKEN_CHUNKS - 1:
            pass_on(1)
        for k, f in enumerate(fs_peers):
            rank = f * n_tp + tp
            tok_copy(c, rank, tok_send.at[c, k], fs, tp).wait_recv()
            for i, t in enumerate(tp_peers):
                cp = tok_copy(c, rank, fwd_send.at[c, k, i], fs, t)
                cp.start()
                pending.append(cp)
        for t in tp_peers:
            for f in [fs] + fs_peers:
                tok_copy(c, f * n_tp + t, tok_send.at[c, 0], fs, tp).wait_recv()
        cols = slice(c * cw, (c + 1) * cw)
        piece = (
            jnp.dot(x_all[:, cols], w_all[cols, :], preferred_element_type=f32),
            lax.dot_general(
                x_all[:, cols],
                w_pair[:, cols],
                (((1,), (1,)), ((), ())),
                preferred_element_type=f32,
            ),
        )
        total = piece if total is None else (total[0] + piece[0], total[1] + piece[1])
    proj, pairs = total[0].astype(bf16), total[1].astype(bf16)
    ret_q, ret_k, ret_v, diff_v = (proj[:, i * head : (i + 1) * head] for i in range(4))
    diff_k, diff_q = pairs[:, :head], pairs[:, head:]
    kv[sp, :, :head] = diff_k
    kv[sp, :, head:] = diff_v

    def to_later(buf, send, recv, go):
        def one(d, c):
            @pl.when(sp + d < n_sp)
            def _():
                cp = remote(buf.at[sp], buf.at[sp], send.at[d], recv.at[sp], sp + d, fs, tp)
                go(cp)

            return c

        if n_sp <= 8:
            for d in range(n_sp - 1, 0, -1):
                one(d, 0)
        else:
            lax.fori_loop(1, n_sp, one, 0)

    to_later(kv, kv_send, kv_recv, lambda cp: cp.start())
    weighted = (ret_k.astype(f32) * key_weight).astype(bf16)
    state = lax.dot_general(
        weighted, ret_v, (((0,), (0,)), ((), ())), preferred_element_type=f32
    )
    st[sp, pl.ds(0, head), :] = state.astype(bf16)
    to_later(st, st_send, st_recv, lambda cp: cp.start())

    scores = lax.dot_general(ret_q, ret_k, (((1,), (1,)), ((), ())), preferred_element_type=f32)
    inner = jnp.dot((scores * fade).astype(bf16), ret_v, preferred_element_type=f32)
    lane = lax.broadcasted_iota(jnp.int32, (rows, 2 * maps), 1)
    zero = jnp.zeros_like(diff_q)
    pair_q = jnp.concatenate(
        [jnp.where(lane < maps, diff_q, zero), jnp.where(lane < maps, zero, diff_q)], axis=0
    )

    def one_block(keys, values, allowed):
        s = lax.dot_general(pair_q, keys, (((1,), (1,)), ((), ())), preferred_element_type=f32)
        s = s * maps ** (-0.5)
        if allowed is not None:
            s = jnp.where(allowed, s, -HUGE)
        peak = jnp.max(s, axis=1, keepdims=True)
        w = jnp.exp(s - peak)
        return (
            peak,
            jnp.sum(w, axis=1, keepdims=True),
            jnp.dot(w.astype(bf16), values, preferred_element_type=f32),
        )

    peak, whole, summed = one_block(diff_k, diff_v, jnp.concatenate([lower, lower], axis=0))

    if ring:
        for step in range(2, n_sp - 1):
            pass_on(step)

    def earlier(d, carry):
        peak, whole, summed, run, entering = carry
        b = sp - d
        remote(kv.at[b], kv.at[b], kv_send.at[0], kv_recv.at[b], sp, fs, tp).wait_recv()
        peak_b, whole_b, sum_b = one_block(kv[b, :, :head], kv[b, :, head:], None)
        top = jnp.maximum(peak, peak_b)
        before, after = jnp.exp(peak - top), jnp.exp(peak_b - top)
        remote(st.at[b], st.at[b], st_send.at[0], st_recv.at[b], sp, fs, tp).wait_recv()
        entering = entering + run * st[b, pl.ds(0, head), :].astype(f32)
        tail = st[b, pl.ds(head, own_rows), :].astype(f32)
        last = own_rows // 2
        return (
            top,
            whole * before + whole_b * after,
            summed * before + sum_b * after,
            run * (tail[0:1] + tail[last : last + 1]),
            entering,
        )

    peak, whole, summed, run, entering = lax.fori_loop(
        1,
        sp + 1,
        earlier,
        (peak, whole, summed, jnp.ones((1, head), f32), jnp.zeros((head, head), f32)),
    )
    entering = entering + run * init_in[0].astype(f32)
    reached = jnp.dot(ret_q, entering.astype(bf16), preferred_element_type=f32)
    ret_out = inner + query_weight * reached
    centre = ret_out - jnp.mean(ret_out, axis=-1, keepdims=True)
    ret_mix = (
        centre
        * lax.rsqrt(jnp.mean(centre * centre, axis=-1, keepdims=True) + EPS)
        * ret_gain_in[...].reshape(1, head)
    ).astype(bf16)
    lam = lambda_in[...].reshape(1, 1)
    ratio = summed / whole
    diff_out = ratio[:rows] - lam * ratio[rows:]
    diff_mix = (
        diff_out
        * lax.rsqrt(jnp.mean(diff_out * diff_out, axis=-1, keepdims=True) + EPS)
        * diff_gain_in[...].reshape(1, head)
    ).astype(bf16)
    mixed = jnp.concatenate([ret_mix, diff_mix], axis=1)

    if ring:
        own_wo.wait()
        order = [sp]
        low, high = sp - 1, sp + 1
        for _ in range(1, n_sp):
            down = jnp.logical_and(
                low >= 0, jnp.logical_or(high >= n_sp, sp - low <= high - sp)
            )
            order.append(jnp.where(down, low, high))
            low, high = jnp.where(down, low - 1, low), jnp.where(down, high, high + 1)
        span = out_weight.shape[2]
    else:
        order = list(range(4))
        span = width // 4

    def columns(s):
        if isinstance(s, int):
            return pl.ds(s * span, span)
        return pl.ds(pl.multiple_of(s * span, 128), span)

    def sib_copy(k, i, t):
        cols = columns(order[k])
        return remote(
            part.at[t, :, cols], sib.at[tp, :, cols], sib_send.at[k, i], sib_recv.at[k, tp], sp, fs, t
        )

    def rs_copy(k, i, f):
        cols = columns(order[k])
        return remote(
            red.at[f, :, cols], rcv.at[fs, :, cols], rs_send.at[k, i], rs_recv.at[k, fs], sp, f, tp
        )

    def reduce_pair(k):
        cols = columns(order[k])
        acc = part[tp, :, cols].astype(f32)
        for i, t in enumerate(tp_peers):
            remote(
                part.at[t, :, cols], sib.at[t, :, cols], sib_send.at[k, i], sib_recv.at[k, t], sp, fs, tp
            ).wait_recv()
            acc = acc + sib[t, :, cols].astype(f32)
        red[:, :, cols] = acc.astype(bf16).reshape(n_fs, own_rows, span)
        for i, f in enumerate(fs_peers):
            cp = rs_copy(k, i, f)
            cp.start()
            pending.append(cp)

    for k, s in enumerate(order):
        if ring and k:

            @pl.when(jnp.logical_or(sp == 0, sp == n_sp - 1))
            def _():
                wo_copy(s, 0, k).wait_recv()

        if ring:
            w = wo[s].reshape(2 * head, span)
        else:
            w = out_weight[:, :, s * span : (s + 1) * span].reshape(2 * head, span)
        value = jnp.dot(mixed, w, preferred_element_type=f32).astype(bf16)
        cols = columns(s)
        for f in range(n_fs):
            for t in range(n_tp):
                at = (f * n_tp + t) * own_rows
                part[t, pl.ds(f * own_rows, own_rows), cols] = value[at : at + own_rows]
        for i, t in enumerate(tp_peers):
            cp = sib_copy(k, i, t)
            cp.start()
            pending.append(cp)
        if k >= 1:
            reduce_pair(k - 1)
    reduce_pair(len(order) - 1)

    for k, s in enumerate(order):
        cols = columns(s)
        acc = red[fs, :, cols].astype(f32)
        for i, f in enumerate(fs_peers):
            remote(
                red.at[f, :, cols], rcv.at[f, :, cols], rs_send.at[k, i], rs_recv.at[k, f], sp, fs, tp
            ).wait_recv()
            acc = acc + rcv[f, :, cols].astype(f32)
        out[:, cols] = acc.astype(bf16)

    for cp in pending:
        cp.wait_send()
    if ring:
        for step in range(n_sp - 1):
            each_way(step, lambda cp: cp.wait_send())
    to_later(kv, kv_send, kv_recv, lambda cp: cp.wait_send())
    to_later(st, st_send, st_recv, lambda cp: cp.wait_send())


def plane_order(sp, n_sp):
    return [jnp.where(i <= sp, sp - i, i) for i in range(n_sp)]


def gather_plan(n_sp):
    plan = []
    for i in range(1, n_sp):
        plan.append(("own", i))
    for d in "XYDS" if DIAG[0] == "D" else "XYS":
        plan.append(("pass", "Z", 0, d))

    def column(i):
        plan.append(("wait", "Z", i))
        for d in "XYDS" if DIAG[i] == "D" else "XYS":
            plan.append(("pass", "Z", i, d))

    def sides(i):
        for k, other in (("X", "Y"), ("Y", "X")):
            plan.append(("wait", k, i))
            if DIAG[i] in (k, "P"):
                plan.append(("pass", k, i, other))
            plan.append(("pass", k, i, "S"))

    def corner(i):
        plan.append(("wait", "D", i))
        if i == 0:
            plan.extend(("far", j) for j in range(1, n_sp))
        plan.append(("pass", "D", i, "S"))

    for step in SEQUENCE:
        name, i = step[0], int(step[1])
        if i < n_sp:
            {"c": column, "s": sides, "d": corner, "p": lambda i: plan.append(("project", i))}[name](i)
    return plan


def whole_kernel(
    sizes,
    plan,
    tokens,
    in_gain,
    ret_query,
    ret_key,
    ret_value,
    decay_log,
    init_state,
    ret_gain,
    diff_query,
    diff_key,
    diff_value,
    diff_lambda,
    diff_gain,
    out_weight,
    out,
    x_all,
    w_all,
    w_pair,
    tok_in,
    gain_in,
    decays,
    init_in,
    ret_gain_in,
    lambda_in,
    diff_gain_in,
    wo,
    pair_q,
    ret_q,
    ret_k,
    ret_v,
    diff_k,
    diff_v,
    states,
    part,
    sib,
    red,
    rcv,
    fin,
    got,
    load_sem,
    tok_send,
    tok_recv,
    decay_send,
    decay_recv,
    sib_send,
    sib_recv,
    rs_send,
    rs_recv,
    fin_send,
    fin_recv,
):
    n_sp, n_fs, n_tp = sizes
    own_rows, width = tokens.shape
    rows = own_rows * n_fs * n_tp
    head = ret_query.shape[1]
    maps = diff_query.shape[0] // 2
    span = out_weight.shape[2]
    sp, fs, tp = lax.axis_index("sp"), lax.axis_index("fs"), lax.axis_index("tp")
    side = fs + 1 - 2 * lax.rem(fs, 2)
    ahead = lax.rem(fs + 2, 4)
    corner = side + ahead - fs
    mate = 1 - tp
    chip = {"Z": fs, "X": side, "Y": ahead, "D": corner}
    order = plane_order(sp, n_sp)

    def remote(src, dst, send, recv, s, f, t):
        return pltpu.make_async_remote_copy(
            src_ref=src,
            dst_ref=dst,
            send_sem=send,
            recv_sem=recv,
            device_id=(s, f, t),
            device_id_type=pl.DeviceIdType.MESH,
        )

    barrier = pltpu.get_barrier_semaphore()
    peers = [(order[i], fs, tp) for i in range(1, n_sp)]
    peers += [(sp, f, tp) for f in (side, ahead, corner)] + [(sp, fs, mate)]
    for peer in peers:
        pl.semaphore_signal(
            barrier, inc=1, device_id=peer, device_id_type=pl.DeviceIdType.MESH
        )

    def col(slot):
        return w_all.at[:, pl.ds(slot * head, head)]

    loads = [
        (tokens, tok_in),
        (in_gain, gain_in),
        (decay_log, decays.at[sp]),
        (init_state, init_in),
        (ret_gain, ret_gain_in),
        (diff_lambda, lambda_in),
        (diff_gain, diff_gain_in),
        (ret_query, col(0)),
        (ret_key, col(1)),
        (ret_value, col(2)),
        (diff_value, col(3)),
        (diff_key, w_pair.at[pl.ds(0, head)]),
        (diff_query, w_pair.at[pl.ds(head, head)]),
        (out_weight, wo),
    ]
    load_copies = [
        pltpu.make_async_copy(src, dst, load_sem.at[i]) for i, (src, dst) in enumerate(loads)
    ]
    for c in load_copies:
        c.start()
    me = (sp * n_fs + fs) * n_tp + tp
    own = pl.ds(pl.multiple_of(me * own_rows, own_rows), own_rows)
    load_copies[0].wait()
    load_copies[1].wait()
    wide = tok_in[...].astype(f32)
    scale = lax.rsqrt(jnp.mean(wide * wide, axis=-1, keepdims=True) + EPS)
    x_all[own, :] = (wide * scale * gain_in[...].reshape(1, width)).astype(bf16)
    load_copies[2].wait()
    pl.semaphore_wait(barrier, len(peers))

    pending = []

    def block(k, i, t):
        rank = (order[i] * n_fs + chip[k]) * n_tp + t
        return x_all.at[pl.ds(pl.multiple_of(rank * own_rows, own_rows), own_rows)]

    def tok_copy(k, i, t, n, s, f, dest):
        return remote(block(k, i, t), block(k, i, t), tok_send.at[n], tok_recv.at[order[i], chip[k], t], s, f, dest)

    def send_tok(k, i, s, f, dest, when=None):
        cp = tok_copy(k, i, tp, len(pending), s, f, dest)
        pending.append((cp, when))
        if when is None:
            cp.start()
        else:
            pl.when(when)(cp.start)

    def distant(i):
        gap = jnp.abs(order[i] - sp)
        return lax.rem(gap, 2) == 1 if FAR == "odd" else gap >= FAR

    row_at = lax.broadcasted_iota(jnp.int32, (rows, rows), 0)
    col_at = lax.broadcasted_iota(jnp.int32, (rows, rows), 1)
    lower = row_at >= col_at
    lane = lax.broadcasted_iota(jnp.int32, (rows, 2 * maps), 1)

    def cumulate(d_row):
        d_wide = jnp.broadcast_to(d_row, (rows, rows))
        return d_wide, jnp.sum(jnp.where(lower, d_wide, 0.0), axis=1, keepdims=True)

    def project(i):
        p = order[i]
        for k in "ZXYD":
            tok_copy(k, i, mate, 0, sp, fs, tp).wait_recv()
        if i:
            remote(
                decays.at[p], decays.at[p], decay_send.at[0], decay_recv.at[p], sp, fs, tp
            ).wait_recv()
        else:
            for c in load_copies[3:]:
                c.wait()
        x = x_all[pl.ds(pl.multiple_of(p * rows, rows), rows), :]
        proj = jnp.dot(x, w_all[...], preferred_element_type=f32).astype(bf16)
        pairs = lax.dot_general(
            x, w_pair[...], (((1,), (1,)), ((), ())), preferred_element_type=f32
        ).astype(bf16)
        q, k, v, dv = (proj[:, j * head : (j + 1) * head] for j in range(4))
        dk, dq = pairs[:, :head], pairs[:, head:]
        zero = jnp.zeros_like(dq)
        d_row = decays[p]
        cum_col = cumulate(d_row)[1]
        cum_last = jnp.sum(d_row, axis=1, keepdims=True)
        key_weight = jnp.exp(cum_last - cum_col) * head ** (-0.5)
        states[p] = lax.dot_general(
            (k.astype(f32) * key_weight).astype(bf16),
            v,
            (((0,), (0,)), ((), ())),
            preferred_element_type=f32,
        )
        ret_q[p], ret_k[p], ret_v[p], diff_k[p], diff_v[p] = q, k, v, dk, dv
        pair_q[p] = jnp.concatenate(
            [jnp.where(lane < maps, dq, zero), jnp.where(lane < maps, zero, dq)], axis=0
        )

    fs_peers = [side, ahead, corner]

    def sib_copy(r):
        return remote(part.at[r, mate], sib.at[r], sib_send.at[r], sib_recv.at[r], sp, fs, mate)

    def rs_copy(r, j):
        f = fs_peers[j]
        return remote(red.at[r, f], rcv.at[r, fs], rs_send.at[r, j], rs_recv.at[r, fs], sp, f, tp)

    def fin_copy(r):
        return remote(fin.at[r], got.at[sp], fin_send.at[r], fin_recv.at[sp], r, fs, tp)

    def finish(r):
        q, k, v = ret_q[r], ret_k[r], ret_v[r]
        scores = lax.dot_general(q, k, (((1,), (1,)), ((), ())), preferred_element_type=f32)
        keys = diff_k[0 : r + 1].reshape((r + 1) * rows, head)
        s = lax.dot_general(
            pair_q[r], keys, (((1,), (1,)), ((), ())), preferred_element_type=f32
        )
        s = [s[:, b * rows : (b + 1) * rows] for b in range(r + 1)]
        s[r] = jnp.where(jnp.concatenate([lower, lower], axis=0), s[r], -HUGE)
        entering = init_in[0].astype(f32)
        for b in range(r):
            entering = jnp.exp(jnp.sum(decays[b], axis=1, keepdims=True)) * entering + states[b]
        reached = jnp.dot(q, entering.astype(bf16), preferred_element_type=f32)
        d_wide, cum_col = cumulate(decays[r])
        d_col = jnp.sum(jnp.where(row_at == col_at, d_wide, 0.0), axis=1, keepdims=True)
        cum_row = jnp.sum(jnp.where(row_at <= col_at, d_col, 0.0), axis=0, keepdims=True)
        fade = jnp.exp(jnp.where(lower, cum_col - cum_row, -HUGE)) * head ** (-0.5)
        inner = jnp.dot((scores * fade).astype(bf16), v, preferred_element_type=f32)
        peak = jnp.max(functools.reduce(jnp.maximum, s), axis=1, keepdims=True)
        w = [jnp.exp((part_s - peak) * maps ** (-0.5)) for part_s in s]
        whole = jnp.sum(functools.reduce(jnp.add, w), axis=1, keepdims=True)
        summed = functools.reduce(
            jnp.add,
            [
                jnp.dot(w[b].astype(bf16), diff_v[b], preferred_element_type=f32)
                for b in range(r + 1)
            ],
        )
        ret_out = inner + jnp.exp(cum_col) * reached
        centre = ret_out - jnp.mean(ret_out, axis=-1, keepdims=True)
        ret_mix = (
            centre
            * lax.rsqrt(jnp.mean(centre * centre, axis=-1, keepdims=True) + EPS)
            * ret_gain_in[...].reshape(1, head)
        ).astype(bf16)
        ratio = summed * (1.0 / whole)
        diff_out = ratio[:rows] - lambda_in[...].reshape(1, 1) * ratio[rows:]
        diff_mix = (
            diff_out
            * lax.rsqrt(jnp.mean(diff_out * diff_out, axis=-1, keepdims=True) + EPS)
            * diff_gain_in[...].reshape(1, head)
        ).astype(bf16)
        mixed = jnp.concatenate([ret_mix, diff_mix], axis=1)
        value = jnp.dot(mixed, wo[...].reshape(2 * head, span), preferred_element_type=f32).astype(bf16)
        for f in range(n_fs):
            for t in range(n_tp):
                at = (f * n_tp + t) * own_rows
                part[r, t, pl.ds(f * own_rows, own_rows), :] = value[at : at + own_rows]
        sib_copy(r).start()

    def reduce_pair(r):
        sib_copy(r).wait_recv()
        total = part[r, tp].astype(f32) + sib[r].astype(f32)
        red[r] = total.astype(bf16).reshape(n_fs, own_rows, span)
        for j in range(3):
            rs_copy(r, j).start()

    def collect(r):
        total = red[r, fs].astype(f32)
        for f in fs_peers:
            remote(red.at[r, f], rcv.at[r, f], rs_send.at[r, 0], rs_recv.at[r, f], sp, fs, tp).wait_recv()
            total = total + rcv[r, f].astype(f32)
        fin[r] = total.astype(bf16)

        @pl.when(r != sp)
        def _():
            fin_copy(r).start()

    def done(i):
        return 0 if i < 0 else jnp.where(i < sp, 0, i + 1)

    def rows_of(stage, i):
        def body(r, c):
            stage(r)
            return c

        lax.fori_loop(done(i - 1), done(i), body, 0)

    dest = {"X": (sp, side, tp), "Y": (sp, ahead, tp), "D": (sp, corner, tp), "S": (sp, fs, mate)}
    for step in plan:
        if step[0] == "own":
            i = step[1]
            send_tok("Z", 0, order[i], fs, tp)
            cp = remote(
                decays.at[sp], decays.at[sp], decay_send.at[i], decay_recv.at[sp], order[i], fs, tp
            )
            cp.start()
        elif step[0] == "pass":
            k, i, d = step[1:]
            cornered = (k == "Z" and d == "D") or (k in "XY" and d in "XY")
            when = jnp.logical_not(distant(i)) if cornered and i else None
            if cornered and DIAG[i] == "P":
                mine = tp == (0 if k == "X" else 1)
                when = mine if when is None else jnp.logical_and(when, mine)
            send_tok(k, i, *dest[d], when=when)
        elif step[0] == "far":
            send_tok("D", 0, order[step[1]], fs, tp, when=distant(step[1]))
        elif step[0] == "wait":
            tok_copy(step[1], step[2], tp, 0, sp, fs, tp).wait_recv()
        else:
            i = step[1]
            project(i)
            if i:
                rows_of(reduce_pair, i - 1)
            if i > 1:
                rows_of(collect, i - 2)
            for r in range(i + 1):
                pl.when(sp <= i if r == i else sp == i)(functools.partial(finish, r))
                if i == n_sp - 1 and r:
                    pl.when(sp == i)(functools.partial(reduce_pair, r - 1))

    last = n_sp - 1
    reduce_pair(last)
    for cp, when in pending:
        if when is None:
            cp.wait_send()
        else:
            pl.when(when)(cp.wait_send)
    rows_of(collect, last - 1)
    rows_of(collect, last)
    for c in range(n_sp):
        cols = slice(c * span, (c + 1) * span)

        @pl.when(sp == c)
        def _():
            out[:, cols] = fin[c]

        @pl.when(sp != c)
        def _():
            remote(fin.at[c], got.at[c], fin_send.at[0], fin_recv.at[c], sp, fs, tp).wait_recv()
            out[:, cols] = got[c]

    for i in range(1, n_sp):
        remote(
            decays.at[sp], decays.at[sp], decay_send.at[i], decay_recv.at[sp], order[i], fs, tp
        ).wait_send()
        fin_copy(order[i]).wait_send()
    for r in range(n_sp):
        sib_copy(r).wait_send()
        for j in range(3):
            rs_copy(r, j).wait_send()


def whole_call(mesh_sizes, args):
    n_sp, n_fs, n_tp = mesh_sizes
    tokens, ret_query, diff_query, out_weight = args[0], args[2], args[8], args[13]
    own_rows, width = tokens.shape
    rows = own_rows * n_fs * n_tp
    head = ret_query.shape[1]
    span = out_weight.shape[2]
    plan = gather_plan(n_sp)
    sends = sum(1 for step in plan if step[0] in ("own", "pass", "far"))
    hbm = pl.BlockSpec(memory_space=pltpu.HBM)
    dma = pltpu.SemaphoreType.DMA
    loaded = lambda i: pltpu.VMEM(args[i].shape, args[i].dtype)
    return pl.pallas_call(
        functools.partial(whole_kernel, mesh_sizes, plan),
        out_shape=pltpu.VMEM(tokens.shape, bf16),
        in_specs=[hbm] * 14,
        out_specs=pl.BlockSpec(memory_space=pltpu.VMEM),
        scratch_shapes=[
            pltpu.VMEM((n_sp * rows, width), bf16),
            pltpu.VMEM((width, 4 * head), bf16),
            pltpu.VMEM((2 * head, width), bf16),
            loaded(0),
            loaded(1),
            pltpu.VMEM((n_sp,) + args[5].shape, f32),
            *[loaded(i) for i in (6, 7, 11, 12)],
            loaded(13),
            pltpu.VMEM((n_sp, 2 * rows, head), bf16),
            *[pltpu.VMEM((n_sp, rows, head), bf16) for _ in range(5)],
            pltpu.VMEM((n_sp, head, head), f32),
            pltpu.VMEM((n_sp, n_tp, n_fs * own_rows, span), bf16),
            pltpu.VMEM((n_sp, n_fs * own_rows, span), bf16),
            *[pltpu.VMEM((n_sp, n_fs, own_rows, span), bf16) for _ in range(2)],
            *[pltpu.VMEM((n_sp, own_rows, span), bf16) for _ in range(2)],
            dma((14,)),
            dma((sends,)),
            dma((n_sp, n_fs, n_tp)),
            dma((n_sp,)),
            dma((n_sp,)),
            dma((n_sp,)),
            dma((n_sp,)),
            dma((n_sp, 3)),
            dma((n_sp, n_fs)),
            dma((n_sp,)),
            dma((n_sp,)),
        ],
        compiler_params=pltpu.CompilerParams(
            collective_id=0, has_side_effects=True, vmem_limit_bytes=66900000
        ),
        name="layer",
    )(*args)


def solution(mesh):
    n_sp, n_fs, n_tp = (mesh.shape[a] for a in ("sp", "fs", "tp"))

    def local(*args):
        args = list(args)
        tokens, ret_query, diff_query, out_weight = args[0], args[2], args[8], args[13]
        own_rows, width = tokens.shape
        rows = own_rows * n_fs * n_tp
        head = ret_query.shape[1]
        maps = diff_query.shape[2]
        assert 2 * maps == head
        assert args[5].shape[1] == rows == head
        ring = out_weight.shape[2] % 128 == 0 and 1 < n_sp <= 8
        whole = ring and n_sp <= 4 and n_fs == 4 and n_tp == 2
        if not ring:
            args[13] = lax.all_gather(out_weight, "sp", axis=2, tiled=True)
        for i in (8, 9):
            args[i] = jnp.swapaxes(args[i], 1, 2).reshape(2 * maps, width)
        if whole:
            return whole_call((n_sp, n_fs, n_tp), args)
        chunks = n_sp if ring else 4
        vmem = pl.BlockSpec(memory_space=pltpu.VMEM)
        hbm = pl.BlockSpec(memory_space=pltpu.HBM)
        in_specs = [hbm] * 13 + [hbm if ring else vmem]
        dma = pltpu.SemaphoreType.DMA
        wo_shape = (n_sp,) + out_weight.shape if ring else (1, 2, 16, 128)
        return pl.pallas_call(
            functools.partial(kernel, (n_sp, n_fs, n_tp, ring)),
            out_shape=jax.ShapeDtypeStruct(tokens.shape, bf16),
            in_specs=in_specs,
            out_specs=vmem,
            scratch_shapes=[
                pltpu.VMEM((rows, width), bf16),
                pltpu.VMEM((width, 4 * head), bf16),
                pltpu.VMEM((4 * maps, width), bf16),
                *[pltpu.VMEM(args[i].shape, args[i].dtype) for i in (0, 1, 5, 6, 7, 11, 12)],
                pltpu.VMEM((n_sp, rows, 2 * head), bf16),
                pltpu.VMEM((n_sp, head + own_rows, head), bf16),
                pltpu.VMEM(wo_shape, bf16),
                pltpu.VMEM((n_tp, n_fs * own_rows, width), bf16),
                pltpu.VMEM((n_tp, n_fs * own_rows, width), bf16),
                pltpu.VMEM((n_fs, own_rows, width), bf16),
                pltpu.VMEM((n_fs, own_rows, width), bf16),
                dma((14,)),
                dma((TOKEN_CHUNKS, n_fs)),
                dma((TOKEN_CHUNKS, n_fs * n_tp)),
                dma((TOKEN_CHUNKS, n_fs, n_tp)),
                dma((n_sp,)),
                dma((n_sp,)),
                dma((n_sp,)),
                dma((n_sp,)),
                dma((2, n_sp)),
                dma((n_sp,)),
                dma((chunks, n_tp)),
                dma((chunks, n_tp)),
                dma((chunks, n_fs)),
                dma((chunks, n_fs)),
            ],
            compiler_params=pltpu.CompilerParams(
                collective_id=0, has_side_effects=True, vmem_limit_bytes=67043328
            ),
            name="layer",
        )(*args)

    in_specs = (
        P(("sp", "fs", "tp"), None),
        P(),
        P(None, ("fs", "tp")),
        P(None, ("fs", "tp")),
        P(None, ("fs", "tp")),
        P(("fs", "tp"), "sp"),
        P(("fs", "tp"), None, None),
        P(("fs", "tp")),
        P(None, None, ("fs", "tp")),
        P(None, None, ("fs", "tp")),
        P(None, ("fs", "tp")),
        P(("fs", "tp")),
        P(("fs", "tp")),
        P(None, ("fs", "tp"), "sp"),
    )
    out_specs = P(("sp", "fs", "tp"), None)
    return jax.shard_map(local, mesh=mesh, in_specs=in_specs, out_specs=out_specs, check_vma=False)
```

```python
import functools

import jax
import jax.numpy as jnp
from jax import lax
from jax.experimental import pallas as pl
from jax.experimental.pallas import tpu as pltpu
from jax.sharding import PartitionSpec as P

EPS = 1e-06
HUGE = 1e30
TOKEN_CHUNKS = 1
SEQUENCE = ("c1", "s0", "d0a", "c2b", "d0b", "s1b", "c3b", "c2+a", "s1+a", "c3+a", "p0a", "q0", "c2-a", "s1-a", "c3-a", "d1+", "s2+", "d2+", "p0b", "s3+", "d3+", "d1-", "s2-", "p1", "d2-", "q1", "p2", "s3-", "d3-", "q2", "p3", "q3")
f32 = jnp.float32
bf16 = jnp.bfloat16


def kernel(
    sizes,
    tokens,
    in_gain,
    ret_query,
    ret_key,
    ret_value,
    decay_log,
    init_state,
    ret_gain,
    diff_query,
    diff_key,
    diff_value,
    diff_lambda,
    diff_gain,
    out_weight,
    out,
    x_all,
    w_all,
    w_pair,
    tok_in,
    gain_in,
    decay_in,
    init_in,
    ret_gain_in,
    lambda_in,
    diff_gain_in,
    kv,
    st,
    wo,
    part,
    sib,
    red,
    rcv,
    load_sem,
    tok_send,
    tok_recv,
    fwd_send,
    kv_send,
    kv_recv,
    st_send,
    st_recv,
    wo_send,
    wo_recv,
    sib_send,
    sib_recv,
    rs_send,
    rs_recv,
):
    n_sp, n_fs, n_tp, ring = sizes
    own_rows, width = tokens.shape
    rows = own_rows * n_fs * n_tp
    head = ret_query.shape[1]
    maps = diff_query.shape[0] // 2
    sp, fs, tp = lax.axis_index("sp"), lax.axis_index("fs"), lax.axis_index("tp")
    half = max(n_fs // 2, 1)
    fs_peers = []
    for d in range(1, n_fs):
        if n_fs % 2 == 0:
            fs_peers.append(
                lax.rem(lax.div(fs, 2) + d // 2, half) * 2 + lax.rem(lax.rem(fs, 2) + d % 2, 2)
            )
        else:
            fs_peers.append(lax.rem(fs + d, n_fs))
    tp_peers = [lax.rem(tp + d, n_tp) for d in range(1, n_tp)]

    def remote(src, dst, send, recv, s, f, t):
        return pltpu.make_async_remote_copy(
            src_ref=src,
            dst_ref=dst,
            send_sem=send,
            recv_sem=recv,
            device_id=(s, f, t),
            device_id_type=pl.DeviceIdType.MESH,
        )

    barrier = pltpu.get_barrier_semaphore()

    def greet(s, f, t):
        pl.semaphore_signal(
            barrier, inc=1, device_id=(s, f, t), device_id_type=pl.DeviceIdType.MESH
        )

    for f in fs_peers:
        greet(sp, f, tp)
    for t in tp_peers:
        greet(sp, fs, t)

    def greet_sp(d, c):
        greet(lax.rem(sp + d, n_sp), fs, tp)
        return c

    if n_sp <= 8:
        for d in range(1, n_sp):
            greet_sp(d, 0)
    else:
        lax.fori_loop(1, n_sp, greet_sp, 0)

    def col(slot):
        return w_all.at[:, pl.ds(slot * head, head)]

    loads = [
        (tokens, tok_in),
        (in_gain, gain_in),
        (decay_log, decay_in),
        (init_state, init_in),
        (ret_gain, ret_gain_in),
        (diff_lambda, lambda_in),
        (diff_gain, diff_gain_in),
        (ret_query, col(0)),
        (ret_key, col(1)),
        (ret_value, col(2)),
        (diff_value, col(3)),
        (diff_key, w_pair.at[pl.ds(0, head)]),
        (diff_query, w_pair.at[pl.ds(head, head)]),
    ]
    load_copies = [
        pltpu.make_async_copy(src, dst, load_sem.at[i]) for i, (src, dst) in enumerate(loads)
    ]
    for c in load_copies:
        c.start()
    if ring:
        own_wo = pltpu.make_async_copy(out_weight, wo.at[sp], load_sem.at[len(loads)])
        own_wo.start()

    me = fs * n_tp + tp
    own = pl.ds(pl.multiple_of(me * own_rows, own_rows), own_rows)
    load_copies[0].wait()
    load_copies[1].wait()
    wide = tok_in[...].astype(f32)
    scale = lax.rsqrt(jnp.mean(wide * wide, axis=-1, keepdims=True) + EPS)
    x_all[own, :] = (wide * scale * gain_in[...].reshape(1, width)).astype(bf16)

    pl.semaphore_wait(barrier, len(fs_peers) + len(tp_peers) + n_sp - 1)

    cw = width // TOKEN_CHUNKS

    def block(rank, c):
        return x_all.at[
            pl.ds(pl.multiple_of(rank * own_rows, own_rows), own_rows), pl.ds(c * cw, cw)
        ]

    def tok_copy(c, rank, send, f, t):
        return remote(block(rank, c), block(rank, c), send, tok_recv.at[c, rank], sp, f, t)

    pending = []
    for c in range(TOKEN_CHUNKS):
        for i, f in enumerate(fs_peers):
            cp = tok_copy(c, me, tok_send.at[c, i], f, tp)
            cp.start()
            pending.append(cp)
        for i, t in enumerate(tp_peers):
            cp = tok_copy(c, me, fwd_send.at[c, n_fs - 1, i], fs, t)
            cp.start()
            pending.append(cp)

    def wo_copy(origin, way, step):
        src = out_weight if step == 0 else wo.at[origin]
        dest = sp + 1 - 2 * way
        return remote(
            src, wo.at[origin], wo_send.at[way, step], wo_recv.at[origin], dest, fs, tp
        )

    def each_way(step, go):
        for way in range(2):
            origin = sp - step if way == 0 else sp + step
            inside = origin >= 0 if way == 0 else origin < n_sp
            onward = sp < n_sp - 1 if way == 0 else sp > 0

            @pl.when(jnp.logical_and(inside, onward))
            def _():
                go(wo_copy(lax.rem(origin + n_sp, n_sp), way, step))

    def pass_on(step):
        def go(cp):
            if step:
                cp.wait_recv()
            cp.start()

        each_way(step, go)

    if ring:
        pass_on(0)

    load_copies[2].wait()
    d_row = decay_in[...]
    row_at = lax.broadcasted_iota(jnp.int32, (rows, rows), 0)
    col_at = lax.broadcasted_iota(jnp.int32, (rows, rows), 1)
    lower = row_at >= col_at
    d_wide = jnp.broadcast_to(d_row, (rows, rows))
    cum_col = jnp.sum(jnp.where(lower, d_wide, 0.0), axis=1, keepdims=True)
    d_col = jnp.sum(jnp.where(row_at == col_at, d_wide, 0.0), axis=1, keepdims=True)
    cum_row = jnp.sum(jnp.where(row_at <= col_at, d_col, 0.0), axis=0, keepdims=True)
    cum_last = jnp.sum(d_row, axis=1, keepdims=True)
    fade = jnp.exp(jnp.where(lower, cum_col - cum_row, -HUGE)) * head ** (-0.5)
    key_weight = jnp.exp(cum_last - cum_col) * head ** (-0.5)
    query_weight = jnp.exp(cum_col)
    decay = jnp.broadcast_to(jnp.exp(cum_last), (own_rows, head))
    decay_high = decay.astype(bf16).astype(f32)
    first = lax.broadcasted_iota(jnp.int32, (own_rows, head), 0) < own_rows // 2
    st[sp, pl.ds(head, own_rows), :] = jnp.where(first, decay_high, decay - decay_high).astype(bf16)

    for c in load_copies[3:]:
        c.wait()

    total = None
    for c in range(TOKEN_CHUNKS):
        if ring and c == TOKEN_CHUNKS - 1:
            pass_on(1)
        for k, f in enumerate(fs_peers):
            rank = f * n_tp + tp
            tok_copy(c, rank, tok_send.at[c, k], fs, tp).wait_recv()
            for i, t in enumerate(tp_peers):
                cp = tok_copy(c, rank, fwd_send.at[c, k, i], fs, t)
                cp.start()
                pending.append(cp)
        for t in tp_peers:
            for f in [fs] + fs_peers:
                tok_copy(c, f * n_tp + t, tok_send.at[c, 0], fs, tp).wait_recv()
        cols = slice(c * cw, (c + 1) * cw)
        piece = (
            jnp.dot(x_all[:, cols], w_all[cols, :], preferred_element_type=f32),
            lax.dot_general(
                x_all[:, cols],
                w_pair[:, cols],
                (((1,), (1,)), ((), ())),
                preferred_element_type=f32,
            ),
        )
        total = piece if total is None else (total[0] + piece[0], total[1] + piece[1])
    proj, pairs = total[0].astype(bf16), total[1].astype(bf16)
    ret_q, ret_k, ret_v, diff_v = (proj[:, i * head : (i + 1) * head] for i in range(4))
    diff_k, diff_q = pairs[:, :head], pairs[:, head:]
    kv[sp, :, :head] = diff_k
    kv[sp, :, head:] = diff_v

    def to_later(buf, send, recv, go):
        def one(d, c):
            @pl.when(sp + d < n_sp)
            def _():
                cp = remote(buf.at[sp], buf.at[sp], send.at[d], recv.at[sp], sp + d, fs, tp)
                go(cp)

            return c

        if n_sp <= 8:
            for d in range(n_sp - 1, 0, -1):
                one(d, 0)
        else:
            lax.fori_loop(1, n_sp, one, 0)

    to_later(kv, kv_send, kv_recv, lambda cp: cp.start())
    weighted = (ret_k.astype(f32) * key_weight).astype(bf16)
    state = lax.dot_general(
        weighted, ret_v, (((0,), (0,)), ((), ())), preferred_element_type=f32
    )
    st[sp, pl.ds(0, head), :] = state.astype(bf16)
    to_later(st, st_send, st_recv, lambda cp: cp.start())

    scores = lax.dot_general(ret_q, ret_k, (((1,), (1,)), ((), ())), preferred_element_type=f32)
    inner = jnp.dot((scores * fade).astype(bf16), ret_v, preferred_element_type=f32)
    lane = lax.broadcasted_iota(jnp.int32, (rows, 2 * maps), 1)
    zero = jnp.zeros_like(diff_q)
    pair_q = jnp.concatenate(
        [jnp.where(lane < maps, diff_q, zero), jnp.where(lane < maps, zero, diff_q)], axis=0
    )

    def one_block(keys, values, allowed):
        s = lax.dot_general(pair_q, keys, (((1,), (1,)), ((), ())), preferred_element_type=f32)
        s = s * maps ** (-0.5)
        if allowed is not None:
            s = jnp.where(allowed, s, -HUGE)
        peak = jnp.max(s, axis=1, keepdims=True)
        w = jnp.exp(s - peak)
        return (
            peak,
            jnp.sum(w, axis=1, keepdims=True),
            jnp.dot(w.astype(bf16), values, preferred_element_type=f32),
        )

    peak, whole, summed = one_block(diff_k, diff_v, jnp.concatenate([lower, lower], axis=0))

    if ring:
        for step in range(2, n_sp - 1):
            pass_on(step)

    def earlier(d, carry):
        peak, whole, summed, run, entering = carry
        b = sp - d
        remote(kv.at[b], kv.at[b], kv_send.at[0], kv_recv.at[b], sp, fs, tp).wait_recv()
        peak_b, whole_b, sum_b = one_block(kv[b, :, :head], kv[b, :, head:], None)
        top = jnp.maximum(peak, peak_b)
        before, after = jnp.exp(peak - top), jnp.exp(peak_b - top)
        remote(st.at[b], st.at[b], st_send.at[0], st_recv.at[b], sp, fs, tp).wait_recv()
        entering = entering + run * st[b, pl.ds(0, head), :].astype(f32)
        tail = st[b, pl.ds(head, own_rows), :].astype(f32)
        last = own_rows // 2
        return (
            top,
            whole * before + whole_b * after,
            summed * before + sum_b * after,
            run * (tail[0:1] + tail[last : last + 1]),
            entering,
        )

    peak, whole, summed, run, entering = lax.fori_loop(
        1,
        sp + 1,
        earlier,
        (peak, whole, summed, jnp.ones((1, head), f32), jnp.zeros((head, head), f32)),
    )
    entering = entering + run * init_in[0].astype(f32)
    reached = jnp.dot(ret_q, entering.astype(bf16), preferred_element_type=f32)
    ret_out = inner + query_weight * reached
    centre = ret_out - jnp.mean(ret_out, axis=-1, keepdims=True)
    ret_mix = (
        centre
        * lax.rsqrt(jnp.mean(centre * centre, axis=-1, keepdims=True) + EPS)
        * ret_gain_in[...].reshape(1, head)
    ).astype(bf16)
    lam = lambda_in[...].reshape(1, 1)
    ratio = summed / whole
    diff_out = ratio[:rows] - lam * ratio[rows:]
    diff_mix = (
        diff_out
        * lax.rsqrt(jnp.mean(diff_out * diff_out, axis=-1, keepdims=True) + EPS)
        * diff_gain_in[...].reshape(1, head)
    ).astype(bf16)
    mixed = jnp.concatenate([ret_mix, diff_mix], axis=1)

    if ring:
        own_wo.wait()
        order = [sp]
        low, high = sp - 1, sp + 1
        for _ in range(1, n_sp):
            down = jnp.logical_and(
                low >= 0, jnp.logical_or(high >= n_sp, sp - low <= high - sp)
            )
            order.append(jnp.where(down, low, high))
            low, high = jnp.where(down, low - 1, low), jnp.where(down, high, high + 1)
        span = out_weight.shape[2]
    else:
        order = list(range(4))
        span = width // 4

    def columns(s):
        if isinstance(s, int):
            return pl.ds(s * span, span)
        return pl.ds(pl.multiple_of(s * span, 128), span)

    def sib_copy(k, i, t):
        cols = columns(order[k])
        return remote(
            part.at[t, :, cols], sib.at[tp, :, cols], sib_send.at[k, i], sib_recv.at[k, tp], sp, fs, t
        )

    def rs_copy(k, i, f):
        cols = columns(order[k])
        return remote(
            red.at[f, :, cols], rcv.at[fs, :, cols], rs_send.at[k, i], rs_recv.at[k, fs], sp, f, tp
        )

    def reduce_pair(k):
        cols = columns(order[k])
        acc = part[tp, :, cols].astype(f32)
        for i, t in enumerate(tp_peers):
            remote(
                part.at[t, :, cols], sib.at[t, :, cols], sib_send.at[k, i], sib_recv.at[k, t], sp, fs, tp
            ).wait_recv()
            acc = acc + sib[t, :, cols].astype(f32)
        red[:, :, cols] = acc.astype(bf16).reshape(n_fs, own_rows, span)
        for i, f in enumerate(fs_peers):
            cp = rs_copy(k, i, f)
            cp.start()
            pending.append(cp)

    for k, s in enumerate(order):
        if ring and k:

            @pl.when(jnp.logical_or(sp == 0, sp == n_sp - 1))
            def _():
                wo_copy(s, 0, k).wait_recv()

        if ring:
            w = wo[s].reshape(2 * head, span)
        else:
            w = out_weight[:, :, s * span : (s + 1) * span].reshape(2 * head, span)
        value = jnp.dot(mixed, w, preferred_element_type=f32).astype(bf16)
        cols = columns(s)
        for f in range(n_fs):
            for t in range(n_tp):
                at = (f * n_tp + t) * own_rows
                part[t, pl.ds(f * own_rows, own_rows), cols] = value[at : at + own_rows]
        for i, t in enumerate(tp_peers):
            cp = sib_copy(k, i, t)
            cp.start()
            pending.append(cp)
        if k >= 1:
            reduce_pair(k - 1)
    reduce_pair(len(order) - 1)

    for k, s in enumerate(order):
        cols = columns(s)
        acc = red[fs, :, cols].astype(f32)
        for i, f in enumerate(fs_peers):
            remote(
                red.at[f, :, cols], rcv.at[f, :, cols], rs_send.at[k, i], rs_recv.at[k, f], sp, fs, tp
            ).wait_recv()
            acc = acc + rcv[f, :, cols].astype(f32)
        out[:, cols] = acc.astype(bf16)

    for cp in pending:
        cp.wait_send()
    if ring:
        for step in range(n_sp - 1):
            each_way(step, lambda cp: cp.wait_send())
    to_later(kv, kv_send, kv_recv, lambda cp: cp.wait_send())
    to_later(st, st_send, st_recv, lambda cp: cp.wait_send())


def plane_order(sp, n_sp):
    return [jnp.where(i <= sp, sp - i, i) for i in range(n_sp)]


def gather_plan(n_sp):
    plan = []
    for i in range(1, n_sp):
        plan.append(("", "own", i))
    for d in "XYDS":
        plan.append(("", "pass", "Z", 0, d))

    def column(i):
        plan.append(("wait", "Z", i))
        plan.extend(("pass", "Z", i, d) for d in "XYDS")

    def sides(i):
        for k in "XY":
            plan.append(("wait", k, i))
            plan.append(("pass", k, i, "S"))

    def corner(i):
        plan.append(("wait", "D", i))
        plan.append(("pass", "D", i, "S"))

    for step in SEQUENCE:
        name, i, flags = step[0], int(step[1]), step[2:]
        begin = len(plan)
        if name in "pq":
            plan.append(({"p": "project", "q": "rows"}[name], i))
        else:
            {"c": column, "s": sides, "d": corner}[name](i)
        plan[begin:] = [(flags,) + entry for entry in plan[begin:]]
    return plan


def row_plan(n_sp, plane):
    last = n_sp - 1
    steps, waiting, late, own = [], [], [], []
    for i in range(n_sp):
        ready = list(range(i + 1)) if i == plane else [i] if i > plane else []
        if plane:
            ready = [r for r in ready if r]
        if plane < i == last - 1:
            late, ready = ready, []
        elif 0 < i == plane < last - 1:
            own, ready = ready[-1:], ready[:-1]
        if i == last:
            ready = ready + late + own
        ops, fresh = [], []
        if plane and i == max(1, plane - 1):
            ops.append(("borrow", 0))
        if plane and i == max(1, plane - 1) + 1:
            ops.append(("reduce", 0))
        for n, r in enumerate(ready):
            ops.append(("finish", r))
            if i == last and n == 0:
                ops += [("reduce", b) for b in waiting]
            if fresh and i >= last - 1:
                ops.append(("reduce", fresh.pop(0)))
            fresh.append(r)
        if i == last:
            if plane:
                ops.append(("collect", 0))
            ops += [("reduce", r) for r in fresh]
            done = [op[1] for step in steps + [ops] for op in step if op[0] == "reduce"]
            ops += [("collect", r) for r in done if r or not plane]
        else:
            waiting += fresh
        steps.append(ops)
    return steps


def whole_kernel(
    sizes,
    plan,
    tokens,
    in_gain,
    ret_query,
    ret_key,
    ret_value,
    decay_log,
    init_state,
    ret_gain,
    diff_query,
    diff_key,
    diff_value,
    diff_lambda,
    diff_gain,
    out_weight,
    out,
    x_all,
    w_all,
    w_pair,
    tok_in,
    gain_in,
    decays,
    init_in,
    ret_gain_in,
    lambda_in,
    diff_gain_in,
    wo,
    pair_q,
    ret_q,
    ret_k,
    ret_v,
    diff_k,
    diff_v,
    states,
    mix,
    part,
    sib,
    red,
    rcv,
    fin,
    got,
    load_sem,
    tok_send,
    tok_recv,
    mate_recv,
    decay_send,
    decay_recv,
    sib_send,
    sib_recv,
    rs_send,
    rs_recv,
    fin_send,
    fin_recv,
    mix_send,
    mix_recv,
):
    n_sp, n_fs, n_tp = sizes
    own_rows, width = tokens.shape
    rows = own_rows * n_fs * n_tp
    head = ret_query.shape[1]
    maps = diff_query.shape[0] // 2
    span = out_weight.shape[2]
    sp, fs, tp = lax.axis_index("sp"), lax.axis_index("fs"), lax.axis_index("tp")
    side = fs + 1 - 2 * lax.rem(fs, 2)
    ahead = lax.rem(fs + 2, 4)
    corner = side + ahead - fs
    mate = 1 - tp
    chip = {"Z": fs, "X": side, "Y": ahead, "D": corner}
    order = plane_order(sp, n_sp)

    def remote(src, dst, send, recv, s, f, t):
        return pltpu.make_async_remote_copy(
            src_ref=src,
            dst_ref=dst,
            send_sem=send,
            recv_sem=recv,
            device_id=(s, f, t),
            device_id_type=pl.DeviceIdType.MESH,
        )

    barrier = pltpu.get_barrier_semaphore()
    peers = [(order[i], fs, tp) for i in range(1, n_sp)]
    peers += [(sp, f, tp) for f in (side, ahead, corner)] + [(sp, fs, mate)]
    for peer in peers:
        pl.semaphore_signal(
            barrier, inc=1, device_id=peer, device_id_type=pl.DeviceIdType.MESH
        )

    def col(slot):
        return w_all.at[:, pl.ds(slot * head, head)]

    loads = [
        (tokens, tok_in),
        (in_gain, gain_in),
        (decay_log, decays.at[sp]),
        (init_state, init_in),
        (ret_gain, ret_gain_in),
        (diff_lambda, lambda_in),
        (diff_gain, diff_gain_in),
        (ret_query, col(0)),
        (ret_key, col(1)),
        (ret_value, col(2)),
        (diff_value, col(3)),
        (diff_key, w_pair.at[pl.ds(0, head)]),
        (diff_query, w_pair.at[pl.ds(head, head)]),
        (out_weight, wo),
    ]
    groups = [0, 1, 2, 3, 4, 5, 6, 7, 7, 7, 7, 8, 8, 9]
    load_copies = [
        pltpu.make_async_copy(src, dst, load_sem.at[i]) for i, (src, dst) in zip(groups, loads)
    ]
    later_loads = load_copies[3:7] + [
        pltpu.make_async_copy(w_all, w_all, load_sem.at[7]),
        pltpu.make_async_copy(w_pair, w_pair, load_sem.at[8]),
        load_copies[13],
    ]
    for c in load_copies:
        c.start()
    me = (sp * n_fs + fs) * n_tp + tp
    own = pl.ds(pl.multiple_of(me * own_rows, own_rows), own_rows)
    load_copies[0].wait()
    load_copies[1].wait()
    wide = tok_in[...].astype(f32)
    scale = lax.rsqrt(jnp.mean(wide * wide, axis=-1, keepdims=True) + EPS)
    x_all[own, :] = (wide * scale * gain_in[...].reshape(1, width)).astype(bf16)
    load_copies[2].wait()
    pl.semaphore_wait(barrier, len(peers))

    pending = []

    def block(k, i, t):
        rank = (order[i] * n_fs + chip[k]) * n_tp + t
        return x_all.at[pl.ds(pl.multiple_of(rank * own_rows, own_rows), own_rows)]

    def tok_copy(k, i, s, f, dest):
        recv = mate_recv.at[order[i]] if dest is mate else tok_recv.at[order[i], chip[k]]
        return remote(block(k, i, tp), block(k, i, tp), tok_send, recv, s, f, dest)

    tests = {"+": tp == 1, "-": tp == 0, "a": sp == 0, "b": sp > 0}

    def run(flags, go):
        if flags:
            pl.when(functools.reduce(jnp.logical_and, [tests[f] for f in flags]))(go)
        else:
            go()

    def send_tok(flags, *where):
        if "-" not in flags and "b" not in flags:
            pending.append(where)
        run(flags, tok_copy(*where).start)

    row_at = lax.broadcasted_iota(jnp.int32, (rows, rows), 0)
    col_at = lax.broadcasted_iota(jnp.int32, (rows, rows), 1)
    lower = row_at >= col_at
    lane = lax.broadcasted_iota(jnp.int32, (rows, 2 * maps), 1)

    def cumulate(d_row):
        d_wide = jnp.broadcast_to(d_row, (rows, rows))
        return d_wide, jnp.sum(jnp.where(lower, d_wide, 0.0), axis=1, keepdims=True)

    def project(i):
        p = order[i]
        quarter = x_all.at[pl.ds(0, n_fs * own_rows)]
        remote(quarter, quarter, tok_send, mate_recv.at[p], sp, fs, tp).wait_recv()
        if i == 1:
            far_decays.wait_recv()
        if i == 0:
            for c in later_loads:
                c.wait()
        x = x_all[pl.ds(pl.multiple_of(p * rows, rows), rows), :]
        proj = jnp.dot(x, w_all[...], preferred_element_type=f32).astype(bf16)
        pairs = lax.dot_general(
            x, w_pair[...], (((1,), (1,)), ((), ())), preferred_element_type=f32
        ).astype(bf16)
        q, k, v, dv = (proj[:, j * head : (j + 1) * head] for j in range(4))
        dk, dq = pairs[:, :head], pairs[:, head:]
        zero = jnp.zeros_like(dq)
        d_row = decays[p]
        cum_col = cumulate(d_row)[1]
        cum_last = jnp.sum(d_row, axis=1, keepdims=True)
        key_weight = jnp.exp(cum_last - cum_col) * head ** (-0.5)
        states[p] = lax.dot_general(
            (k.astype(f32) * key_weight).astype(bf16),
            v,
            (((0,), (0,)), ((), ())),
            preferred_element_type=f32,
        )
        ret_q[p], ret_k[p], ret_v[p], diff_k[p], diff_v[p] = q, k, v, dk, dv
        pair_q[p] = jnp.concatenate(
            [jnp.where(lane < maps, dq, zero), jnp.where(lane < maps, zero, dq)], axis=0
        )

    fs_peers = [side, ahead, corner]

    def sib_copy(r):
        return remote(part.at[r, mate], sib.at[r], sib_send, sib_recv.at[r], sp, fs, mate)

    def place(f):
        return jnp.where(fs > f, fs - 1, fs)

    def rs_copy(r, j):
        f = fs_peers[j]
        return remote(red.at[r, f], rcv.at[r, place(f)], rs_send.at[r], rs_recv.at[r], sp, f, tp)

    def fin_copy(r):
        return remote(fin.at[r], got.at[sp], fin_send, fin_recv, r, fs, tp)

    def finish(r):
        q, k, v = ret_q[r], ret_k[r], ret_v[r]
        scores = lax.dot_general(q, k, (((1,), (1,)), ((), ())), preferred_element_type=f32)
        keys = diff_k[0 : r + 1].reshape((r + 1) * rows, head)
        s = lax.dot_general(
            pair_q[r], keys, (((1,), (1,)), ((), ())), preferred_element_type=f32
        )
        s = [s[:, b * rows : (b + 1) * rows] for b in range(r + 1)]
        s[r] = jnp.where(jnp.concatenate([lower, lower], axis=0), s[r], -HUGE)
        entering = init_in[0].astype(f32)
        for b in range(r):
            entering = jnp.exp(jnp.sum(decays[b], axis=1, keepdims=True)) * entering + states[b]
        reached = jnp.dot(q, entering.astype(bf16), preferred_element_type=f32)
        d_wide, cum_col = cumulate(decays[r])
        d_col = jnp.sum(jnp.where(row_at == col_at, d_wide, 0.0), axis=1, keepdims=True)
        cum_row = jnp.sum(jnp.where(row_at <= col_at, d_col, 0.0), axis=0, keepdims=True)
        fade = jnp.exp(jnp.where(lower, cum_col - cum_row, -HUGE)) * head ** (-0.5)
        inner = jnp.dot((scores * fade).astype(bf16), v, preferred_element_type=f32)
        peak = jnp.max(functools.reduce(jnp.maximum, s), axis=1, keepdims=True)
        w = [jnp.exp((part_s - peak) * maps ** (-0.5)) for part_s in s]
        whole = jnp.sum(functools.reduce(jnp.add, w), axis=1, keepdims=True)
        summed = functools.reduce(
            jnp.add,
            [
                jnp.dot(w[b].astype(bf16), diff_v[b], preferred_element_type=f32)
                for b in range(r + 1)
            ],
        )
        ret_out = inner + jnp.exp(cum_col) * reached
        centre = ret_out - jnp.mean(ret_out, axis=-1, keepdims=True)
        ret_mix = (
            centre
            * lax.rsqrt(jnp.mean(centre * centre, axis=-1, keepdims=True) + EPS)
            * ret_gain_in[...].reshape(1, head)
        ).astype(bf16)
        ratio = summed * (1.0 / whole)
        diff_out = ratio[:rows] - lambda_in[...].reshape(1, 1) * ratio[rows:]
        diff_mix = (
            diff_out
            * lax.rsqrt(jnp.mean(diff_out * diff_out, axis=-1, keepdims=True) + EPS)
            * diff_gain_in[...].reshape(1, head)
        ).astype(bf16)
        mixed = jnp.concatenate([ret_mix, diff_mix], axis=1)
        if r == 0:
            mix[...] = mixed
            for i in range(1, n_sp):
                mix_copy(i).start()
        emit(r, mixed)

    def mix_copy(i):
        return remote(mix, mix, mix_send.at[i], mix_recv, order[i], fs, tp)

    def borrow(r):
        mix_copy(0).wait_recv()
        emit(r, mix[...])

    def emit(r, mixed):
        value = jnp.dot(mixed, wo[...].reshape(2 * head, span), preferred_element_type=f32).astype(bf16)
        for f in range(n_fs):
            for t in range(n_tp):
                at = (f * n_tp + t) * own_rows
                part[r, t, pl.ds(f * own_rows, own_rows), :] = value[at : at + own_rows]
        sib_copy(r).start()

    def reduce_pair(r):
        sib_copy(r).wait_recv()
        total = part[r, tp].astype(f32) + sib[r].astype(f32)
        red[r] = total.astype(bf16).reshape(n_fs, own_rows, span)
        for j in range(3):
            rs_copy(r, j).start()

    def collect(r):
        shares = rcv.at[r]
        remote(shares, shares, rs_send.at[r], rs_recv.at[r], sp, fs, tp).wait_recv()
        total = red[r, fs].astype(f32)
        for j in range(n_fs - 1):
            total = total + rcv[r, j].astype(f32)
        fin[r] = total.astype(bf16)

        @pl.when(r != sp)
        def _():
            fin_copy(r).start()

    dest = {"X": (sp, side, tp), "Y": (sp, ahead, tp), "D": (sp, corner, tp), "S": (sp, fs, mate)}
    stages = {"finish": finish, "borrow": borrow, "reduce": reduce_pair, "collect": collect}
    row_plans = [row_plan(n_sp, plane) for plane in range(n_sp)]

    all_decays = decays.at[pl.ds(0, n_sp - 1)]
    far_decays = remote(all_decays, all_decays, decay_send, decay_recv, sp, fs, tp)
    for flags, kind, *step in plan:
        if kind == "own":
            i = step[0]
            send_tok(flags, "Z", 0, order[i], fs, tp)
            remote(
                decays.at[sp], decays.at[sp], decay_send, decay_recv, order[i], fs, tp
            ).start()
        elif kind == "pass":
            send_tok(flags, *step[:2], *dest[step[2]])
        elif kind == "wait":
            run(flags, tok_copy(*step, sp, fs, tp).wait_recv)
        elif kind == "project":
            run(flags, functools.partial(project, step[0]))
        else:
            i = step[0]
            for plane in range(n_sp):

                def rows_done(ops=row_plans[plane][i]):
                    for stage, r in ops:
                        stages[stage](r)

                if row_plans[plane][i]:
                    pl.when(sp == plane)(rows_done)

    others = got.at[pl.ds(0, n_sp - 1)]
    arrived = remote(others, others, fin_send, fin_recv, sp, fs, tp)
    arrived.wait_recv()
    for c in range(n_sp):
        out[:, c * span : (c + 1) * span] = jnp.where(sp == c, fin[c], got[c])

    sent = x_all.at[pl.ds(0, len(pending) * own_rows)]
    remote(sent, sent, tok_send, mate_recv.at[0], sp, fs, tp).wait_send()
    far_decays.wait_send()
    halves = part.at[:, 0]
    remote(halves, halves, sib_send, sib_recv.at[0], sp, fs, tp).wait_send()
    for r in range(n_sp):
        shares = rcv.at[r]
        remote(shares, shares, rs_send.at[r], rs_recv.at[r], sp, fs, tp).wait_send()
    arrived.wait_send()

    @pl.when(sp == 0)
    def _():
        for i in range(1, n_sp):
            mix_copy(i).wait_send()


def whole_call(mesh_sizes, args):
    n_sp, n_fs, n_tp = mesh_sizes
    tokens, ret_query, diff_query, out_weight = args[0], args[2], args[8], args[13]
    own_rows, width = tokens.shape
    rows = own_rows * n_fs * n_tp
    head = ret_query.shape[1]
    span = out_weight.shape[2]
    plan = gather_plan(n_sp)
    hbm = pl.BlockSpec(memory_space=pltpu.HBM)
    dma = pltpu.SemaphoreType.DMA
    loaded = lambda i: pltpu.VMEM(args[i].shape, args[i].dtype)
    return pl.pallas_call(
        functools.partial(whole_kernel, mesh_sizes, plan),
        out_shape=pltpu.VMEM(tokens.shape, bf16),
        in_specs=[hbm] * 14,
        out_specs=pl.BlockSpec(memory_space=pltpu.VMEM),
        scratch_shapes=[
            pltpu.VMEM((n_sp * rows, width), bf16),
            pltpu.VMEM((width, 4 * head), bf16),
            pltpu.VMEM((2 * head, width), bf16),
            loaded(0),
            loaded(1),
            pltpu.VMEM((n_sp,) + args[5].shape, f32),
            *[loaded(i) for i in (6, 7, 11, 12)],
            loaded(13),
            pltpu.VMEM((n_sp, 2 * rows, head), bf16),
            *[pltpu.VMEM((n_sp, rows, head), bf16) for _ in range(5)],
            pltpu.VMEM((n_sp, head, head), f32),
            pltpu.VMEM((rows, 2 * head), bf16),
            pltpu.VMEM((n_sp, n_tp, n_fs * own_rows, span), bf16),
            pltpu.VMEM((n_sp, n_fs * own_rows, span), bf16),
            pltpu.VMEM((n_sp, n_fs, own_rows, span), bf16),
            pltpu.VMEM((n_sp, n_fs - 1, own_rows, span), bf16),
            *[pltpu.VMEM((n_sp, own_rows, span), bf16) for _ in range(2)],
            dma((10,)),
            dma,
            dma((n_sp, n_fs)),
            dma((n_sp,)),
            dma,
            dma,
            dma,
            dma((n_sp,)),
            dma((n_sp,)),
            dma((n_sp,)),
            dma,
            dma,
            dma((n_sp,)),
            dma,
        ],
        compiler_params=pltpu.CompilerParams(
            collective_id=0, has_side_effects=True, vmem_limit_bytes=66900000
        ),
        name="layer",
    )(*args)


def solution(mesh):
    n_sp, n_fs, n_tp = (mesh.shape[a] for a in ("sp", "fs", "tp"))

    def local(*args):
        args = list(args)
        tokens, ret_query, diff_query, out_weight = args[0], args[2], args[8], args[13]
        own_rows, width = tokens.shape
        rows = own_rows * n_fs * n_tp
        head = ret_query.shape[1]
        maps = diff_query.shape[2]
        assert 2 * maps == head
        assert args[5].shape[1] == rows == head
        ring = out_weight.shape[2] % 128 == 0 and 1 < n_sp <= 8
        whole = ring and n_sp == 4 and n_fs == 4 and n_tp == 2
        if not ring:
            args[13] = lax.all_gather(out_weight, "sp", axis=2, tiled=True)
        for i in (8, 9):
            args[i] = jnp.swapaxes(args[i], 1, 2).reshape(2 * maps, width)
        if whole:
            return whole_call((n_sp, n_fs, n_tp), args)
        chunks = n_sp if ring else 4
        vmem = pl.BlockSpec(memory_space=pltpu.VMEM)
        hbm = pl.BlockSpec(memory_space=pltpu.HBM)
        in_specs = [hbm] * 13 + [hbm if ring else vmem]
        dma = pltpu.SemaphoreType.DMA
        wo_shape = (n_sp,) + out_weight.shape if ring else (1, 2, 16, 128)
        return pl.pallas_call(
            functools.partial(kernel, (n_sp, n_fs, n_tp, ring)),
            out_shape=jax.ShapeDtypeStruct(tokens.shape, bf16),
            in_specs=in_specs,
            out_specs=vmem,
            scratch_shapes=[
                pltpu.VMEM((rows, width), bf16),
                pltpu.VMEM((width, 4 * head), bf16),
                pltpu.VMEM((4 * maps, width), bf16),
                *[pltpu.VMEM(args[i].shape, args[i].dtype) for i in (0, 1, 5, 6, 7, 11, 12)],
                pltpu.VMEM((n_sp, rows, 2 * head), bf16),
                pltpu.VMEM((n_sp, head + own_rows, head), bf16),
                pltpu.VMEM(wo_shape, bf16),
                pltpu.VMEM((n_tp, n_fs * own_rows, width), bf16),
                pltpu.VMEM((n_tp, n_fs * own_rows, width), bf16),
                pltpu.VMEM((n_fs, own_rows, width), bf16),
                pltpu.VMEM((n_fs, own_rows, width), bf16),
                dma((14,)),
                dma((TOKEN_CHUNKS, n_fs)),
                dma((TOKEN_CHUNKS, n_fs * n_tp)),
                dma((TOKEN_CHUNKS, n_fs, n_tp)),
                dma((n_sp,)),
                dma((n_sp,)),
                dma((n_sp,)),
                dma((n_sp,)),
                dma((2, n_sp)),
                dma((n_sp,)),
                dma((chunks, n_tp)),
                dma((chunks, n_tp)),
                dma((chunks, n_fs)),
                dma((chunks, n_fs)),
            ],
            compiler_params=pltpu.CompilerParams(
                collective_id=0, has_side_effects=True, vmem_limit_bytes=67043328
            ),
            name="layer",
        )(*args)

    in_specs = (
        P(("sp", "fs", "tp"), None),
        P(),
        P(None, ("fs", "tp")),
        P(None, ("fs", "tp")),
        P(None, ("fs", "tp")),
        P(("fs", "tp"), "sp"),
        P(("fs", "tp"), None, None),
        P(("fs", "tp")),
        P(None, None, ("fs", "tp")),
        P(None, None, ("fs", "tp")),
        P(None, ("fs", "tp")),
        P(("fs", "tp")),
        P(("fs", "tp")),
        P(None, ("fs", "tp"), "sp"),
    )
    out_specs = P(("sp", "fs", "tp"), None)
    return jax.shard_map(local, mesh=mesh, in_specs=in_specs, out_specs=out_specs, check_vma=False)
```

```python
import functools

import jax
import jax.numpy as jnp
from jax import lax
from jax.experimental import pallas as pl
from jax.experimental.pallas import tpu as pltpu
from jax.sharding import PartitionSpec as P

EPS = 1e-06
HUGE = 1e30
TOKEN_CHUNKS = 1
DOWN = True
SEQUENCE = ("c1", "s0", "d0", "c2b", "s1b", "c3b", "c2+a", "s1+a", "c3+a", "p0a", "q0", "c2-a", "s1-a", "c3-a", "d1+", "s2+", "d2+", "s3+", "d3+", "p0b", "d1-a", "s2-a", "d2-a", "d3-a", "d1-b", "s2-b", "p1", "d2-b", "s3-a", "q1", "p2", "s3-b", "d3-b", "q2", "p3", "q3")
f32 = jnp.float32
bf16 = jnp.bfloat16


def kernel(
    sizes,
    tokens,
    in_gain,
    ret_query,
    ret_key,
    ret_value,
    decay_log,
    init_state,
    ret_gain,
    diff_query,
    diff_key,
    diff_value,
    diff_lambda,
    diff_gain,
    out_weight,
    out,
    x_all,
    w_all,
    w_pair,
    tok_in,
    gain_in,
    decay_in,
    init_in,
    ret_gain_in,
    lambda_in,
    diff_gain_in,
    kv,
    st,
    wo,
    part,
    sib,
    red,
    rcv,
    load_sem,
    tok_send,
    tok_recv,
    fwd_send,
    kv_send,
    kv_recv,
    st_send,
    st_recv,
    wo_send,
    wo_recv,
    sib_send,
    sib_recv,
    rs_send,
    rs_recv,
):
    n_sp, n_fs, n_tp, ring = sizes
    own_rows, width = tokens.shape
    rows = own_rows * n_fs * n_tp
    head = ret_query.shape[1]
    maps = diff_query.shape[0] // 2
    sp, fs, tp = lax.axis_index("sp"), lax.axis_index("fs"), lax.axis_index("tp")
    half = max(n_fs // 2, 1)
    fs_peers = []
    for d in range(1, n_fs):
        if n_fs % 2 == 0:
            fs_peers.append(
                lax.rem(lax.div(fs, 2) + d // 2, half) * 2 + lax.rem(lax.rem(fs, 2) + d % 2, 2)
            )
        else:
            fs_peers.append(lax.rem(fs + d, n_fs))
    tp_peers = [lax.rem(tp + d, n_tp) for d in range(1, n_tp)]

    def remote(src, dst, send, recv, s, f, t):
        return pltpu.make_async_remote_copy(
            src_ref=src,
            dst_ref=dst,
            send_sem=send,
            recv_sem=recv,
            device_id=(s, f, t),
            device_id_type=pl.DeviceIdType.MESH,
        )

    barrier = pltpu.get_barrier_semaphore()

    def greet(s, f, t):
        pl.semaphore_signal(
            barrier, inc=1, device_id=(s, f, t), device_id_type=pl.DeviceIdType.MESH
        )

    for f in fs_peers:
        greet(sp, f, tp)
    for t in tp_peers:
        greet(sp, fs, t)

    def greet_sp(d, c):
        greet(lax.rem(sp + d, n_sp), fs, tp)
        return c

    if n_sp <= 8:
        for d in range(1, n_sp):
            greet_sp(d, 0)
    else:
        lax.fori_loop(1, n_sp, greet_sp, 0)

    def col(slot):
        return w_all.at[:, pl.ds(slot * head, head)]

    loads = [
        (tokens, tok_in),
        (in_gain, gain_in),
        (decay_log, decay_in),
        (init_state, init_in),
        (ret_gain, ret_gain_in),
        (diff_lambda, lambda_in),
        (diff_gain, diff_gain_in),
        (ret_query, col(0)),
        (ret_key, col(1)),
        (ret_value, col(2)),
        (diff_value, col(3)),
        (diff_key, w_pair.at[pl.ds(0, head)]),
        (diff_query, w_pair.at[pl.ds(head, head)]),
    ]
    load_copies = [
        pltpu.make_async_copy(src, dst, load_sem.at[i]) for i, (src, dst) in enumerate(loads)
    ]
    for c in load_copies:
        c.start()
    if ring:
        own_wo = pltpu.make_async_copy(out_weight, wo.at[sp], load_sem.at[len(loads)])
        own_wo.start()

    me = fs * n_tp + tp
    own = pl.ds(pl.multiple_of(me * own_rows, own_rows), own_rows)
    load_copies[0].wait()
    load_copies[1].wait()
    wide = tok_in[...].astype(f32)
    scale = lax.rsqrt(jnp.mean(wide * wide, axis=-1, keepdims=True) + EPS)
    x_all[own, :] = (wide * scale * gain_in[...].reshape(1, width)).astype(bf16)

    pl.semaphore_wait(barrier, len(fs_peers) + len(tp_peers) + n_sp - 1)

    cw = width // TOKEN_CHUNKS

    def block(rank, c):
        return x_all.at[
            pl.ds(pl.multiple_of(rank * own_rows, own_rows), own_rows), pl.ds(c * cw, cw)
        ]

    def tok_copy(c, rank, send, f, t):
        return remote(block(rank, c), block(rank, c), send, tok_recv.at[c, rank], sp, f, t)

    pending = []
    for c in range(TOKEN_CHUNKS):
        for i, f in enumerate(fs_peers):
            cp = tok_copy(c, me, tok_send.at[c, i], f, tp)
            cp.start()
            pending.append(cp)
        for i, t in enumerate(tp_peers):
            cp = tok_copy(c, me, fwd_send.at[c, n_fs - 1, i], fs, t)
            cp.start()
            pending.append(cp)

    def wo_copy(origin, way, step):
        src = out_weight if step == 0 else wo.at[origin]
        dest = sp + 1 - 2 * way
        return remote(
            src, wo.at[origin], wo_send.at[way, step], wo_recv.at[origin], dest, fs, tp
        )

    def each_way(step, go):
        for way in range(2):
            origin = sp - step if way == 0 else sp + step
            inside = origin >= 0 if way == 0 else origin < n_sp
            onward = sp < n_sp - 1 if way == 0 else sp > 0

            @pl.when(jnp.logical_and(inside, onward))
            def _():
                go(wo_copy(lax.rem(origin + n_sp, n_sp), way, step))

    def pass_on(step):
        def go(cp):
            if step:
                cp.wait_recv()
            cp.start()

        each_way(step, go)

    if ring:
        pass_on(0)

    load_copies[2].wait()
    d_row = decay_in[...]
    row_at = lax.broadcasted_iota(jnp.int32, (rows, rows), 0)
    col_at = lax.broadcasted_iota(jnp.int32, (rows, rows), 1)
    lower = row_at >= col_at
    d_wide = jnp.broadcast_to(d_row, (rows, rows))
    cum_col = jnp.sum(jnp.where(lower, d_wide, 0.0), axis=1, keepdims=True)
    d_col = jnp.sum(jnp.where(row_at == col_at, d_wide, 0.0), axis=1, keepdims=True)
    cum_row = jnp.sum(jnp.where(row_at <= col_at, d_col, 0.0), axis=0, keepdims=True)
    cum_last = jnp.sum(d_row, axis=1, keepdims=True)
    fade = jnp.exp(jnp.where(lower, cum_col - cum_row, -HUGE)) * head ** (-0.5)
    key_weight = jnp.exp(cum_last - cum_col) * head ** (-0.5)
    query_weight = jnp.exp(cum_col)
    decay = jnp.broadcast_to(jnp.exp(cum_last), (own_rows, head))
    decay_high = decay.astype(bf16).astype(f32)
    first = lax.broadcasted_iota(jnp.int32, (own_rows, head), 0) < own_rows // 2
    st[sp, pl.ds(head, own_rows), :] = jnp.where(first, decay_high, decay - decay_high).astype(bf16)

    for c in load_copies[3:]:
        c.wait()

    total = None
    for c in range(TOKEN_CHUNKS):
        if ring and c == TOKEN_CHUNKS - 1:
            pass_on(1)
        for k, f in enumerate(fs_peers):
            rank = f * n_tp + tp
            tok_copy(c, rank, tok_send.at[c, k], fs, tp).wait_recv()
            for i, t in enumerate(tp_peers):
                cp = tok_copy(c, rank, fwd_send.at[c, k, i], fs, t)
                cp.start()
                pending.append(cp)
        for t in tp_peers:
            for f in [fs] + fs_peers:
                tok_copy(c, f * n_tp + t, tok_send.at[c, 0], fs, tp).wait_recv()
        cols = slice(c * cw, (c + 1) * cw)
        piece = (
            jnp.dot(x_all[:, cols], w_all[cols, :], preferred_element_type=f32),
            lax.dot_general(
                x_all[:, cols],
                w_pair[:, cols],
                (((1,), (1,)), ((), ())),
                preferred_element_type=f32,
            ),
        )
        total = piece if total is None else (total[0] + piece[0], total[1] + piece[1])
    proj, pairs = total[0].astype(bf16), total[1].astype(bf16)
    ret_q, ret_k, ret_v, diff_v = (proj[:, i * head : (i + 1) * head] for i in range(4))
    diff_k, diff_q = pairs[:, :head], pairs[:, head:]
    kv[sp, :, :head] = diff_k
    kv[sp, :, head:] = diff_v

    def to_later(buf, send, recv, go):
        def one(d, c):
            @pl.when(sp + d < n_sp)
            def _():
                cp = remote(buf.at[sp], buf.at[sp], send.at[d], recv.at[sp], sp + d, fs, tp)
                go(cp)

            return c

        if n_sp <= 8:
            for d in range(n_sp - 1, 0, -1):
                one(d, 0)
        else:
            lax.fori_loop(1, n_sp, one, 0)

    to_later(kv, kv_send, kv_recv, lambda cp: cp.start())
    weighted = (ret_k.astype(f32) * key_weight).astype(bf16)
    state = lax.dot_general(
        weighted, ret_v, (((0,), (0,)), ((), ())), preferred_element_type=f32
    )
    st[sp, pl.ds(0, head), :] = state.astype(bf16)
    to_later(st, st_send, st_recv, lambda cp: cp.start())

    scores = lax.dot_general(ret_q, ret_k, (((1,), (1,)), ((), ())), preferred_element_type=f32)
    inner = jnp.dot((scores * fade).astype(bf16), ret_v, preferred_element_type=f32)
    lane = lax.broadcasted_iota(jnp.int32, (rows, 2 * maps), 1)
    zero = jnp.zeros_like(diff_q)
    pair_q = jnp.concatenate(
        [jnp.where(lane < maps, diff_q, zero), jnp.where(lane < maps, zero, diff_q)], axis=0
    )

    def one_block(keys, values, allowed):
        s = lax.dot_general(pair_q, keys, (((1,), (1,)), ((), ())), preferred_element_type=f32)
        s = s * maps ** (-0.5)
        if allowed is not None:
            s = jnp.where(allowed, s, -HUGE)
        peak = jnp.max(s, axis=1, keepdims=True)
        w = jnp.exp(s - peak)
        return (
            peak,
            jnp.sum(w, axis=1, keepdims=True),
            jnp.dot(w.astype(bf16), values, preferred_element_type=f32),
        )

    peak, whole, summed = one_block(diff_k, diff_v, jnp.concatenate([lower, lower], axis=0))

    if ring:
        for step in range(2, n_sp - 1):
            pass_on(step)

    def earlier(d, carry):
        peak, whole, summed, run, entering = carry
        b = sp - d
        remote(kv.at[b], kv.at[b], kv_send.at[0], kv_recv.at[b], sp, fs, tp).wait_recv()
        peak_b, whole_b, sum_b = one_block(kv[b, :, :head], kv[b, :, head:], None)
        top = jnp.maximum(peak, peak_b)
        before, after = jnp.exp(peak - top), jnp.exp(peak_b - top)
        remote(st.at[b], st.at[b], st_send.at[0], st_recv.at[b], sp, fs, tp).wait_recv()
        entering = entering + run * st[b, pl.ds(0, head), :].astype(f32)
        tail = st[b, pl.ds(head, own_rows), :].astype(f32)
        last = own_rows // 2
        return (
            top,
            whole * before + whole_b * after,
            summed * before + sum_b * after,
            run * (tail[0:1] + tail[last : last + 1]),
            entering,
        )

    peak, whole, summed, run, entering = lax.fori_loop(
        1,
        sp + 1,
        earlier,
        (peak, whole, summed, jnp.ones((1, head), f32), jnp.zeros((head, head), f32)),
    )
    entering = entering + run * init_in[0].astype(f32)
    reached = jnp.dot(ret_q, entering.astype(bf16), preferred_element_type=f32)
    ret_out = inner + query_weight * reached
    centre = ret_out - jnp.mean(ret_out, axis=-1, keepdims=True)
    ret_mix = (
        centre
        * lax.rsqrt(jnp.mean(centre * centre, axis=-1, keepdims=True) + EPS)
        * ret_gain_in[...].reshape(1, head)
    ).astype(bf16)
    lam = lambda_in[...].reshape(1, 1)
    ratio = summed / whole
    diff_out = ratio[:rows] - lam * ratio[rows:]
    diff_mix = (
        diff_out
        * lax.rsqrt(jnp.mean(diff_out * diff_out, axis=-1, keepdims=True) + EPS)
        * diff_gain_in[...].reshape(1, head)
    ).astype(bf16)
    mixed = jnp.concatenate([ret_mix, diff_mix], axis=1)

    if ring:
        own_wo.wait()
        order = [sp]
        low, high = sp - 1, sp + 1
        for _ in range(1, n_sp):
            down = jnp.logical_and(
                low >= 0, jnp.logical_or(high >= n_sp, sp - low <= high - sp)
            )
            order.append(jnp.where(down, low, high))
            low, high = jnp.where(down, low - 1, low), jnp.where(down, high, high + 1)
        span = out_weight.shape[2]
    else:
        order = list(range(4))
        span = width // 4

    def columns(s):
        if isinstance(s, int):
            return pl.ds(s * span, span)
        return pl.ds(pl.multiple_of(s * span, 128), span)

    def sib_copy(k, i, t):
        cols = columns(order[k])
        return remote(
            part.at[t, :, cols], sib.at[tp, :, cols], sib_send.at[k, i], sib_recv.at[k, tp], sp, fs, t
        )

    def rs_copy(k, i, f):
        cols = columns(order[k])
        return remote(
            red.at[f, :, cols], rcv.at[fs, :, cols], rs_send.at[k, i], rs_recv.at[k, fs], sp, f, tp
        )

    def reduce_pair(k):
        cols = columns(order[k])
        acc = part[tp, :, cols].astype(f32)
        for i, t in enumerate(tp_peers):
            remote(
                part.at[t, :, cols], sib.at[t, :, cols], sib_send.at[k, i], sib_recv.at[k, t], sp, fs, tp
            ).wait_recv()
            acc = acc + sib[t, :, cols].astype(f32)
        red[:, :, cols] = acc.astype(bf16).reshape(n_fs, own_rows, span)
        for i, f in enumerate(fs_peers):
            cp = rs_copy(k, i, f)
            cp.start()
            pending.append(cp)

    for k, s in enumerate(order):
        if ring and k:

            @pl.when(jnp.logical_or(sp == 0, sp == n_sp - 1))
            def _():
                wo_copy(s, 0, k).wait_recv()

        if ring:
            w = wo[s].reshape(2 * head, span)
        else:
            w = out_weight[:, :, s * span : (s + 1) * span].reshape(2 * head, span)
        value = jnp.dot(mixed, w, preferred_element_type=f32).astype(bf16)
        cols = columns(s)
        for f in range(n_fs):
            for t in range(n_tp):
                at = (f * n_tp + t) * own_rows
                part[t, pl.ds(f * own_rows, own_rows), cols] = value[at : at + own_rows]
        for i, t in enumerate(tp_peers):
            cp = sib_copy(k, i, t)
            cp.start()
            pending.append(cp)
        if k >= 1:
            reduce_pair(k - 1)
    reduce_pair(len(order) - 1)

    for k, s in enumerate(order):
        cols = columns(s)
        acc = red[fs, :, cols].astype(f32)
        for i, f in enumerate(fs_peers):
            remote(
                red.at[f, :, cols], rcv.at[f, :, cols], rs_send.at[k, i], rs_recv.at[k, f], sp, fs, tp
            ).wait_recv()
            acc = acc + rcv[f, :, cols].astype(f32)
        out[:, cols] = acc.astype(bf16)

    for cp in pending:
        cp.wait_send()
    if ring:
        for step in range(n_sp - 1):
            each_way(step, lambda cp: cp.wait_send())
    to_later(kv, kv_send, kv_recv, lambda cp: cp.wait_send())
    to_later(st, st_send, st_recv, lambda cp: cp.wait_send())


def plane_order(sp, n_sp):
    return [jnp.where(i <= sp, sp - i, i) for i in range(n_sp)]


def gather_plan(n_sp):
    plan = []
    for i in range(1, n_sp):
        plan.append(("", "own", i))
    for d in "XYDS":
        plan.append(("", "pass", "Z", 0, d))

    def column(i):
        plan.append(("wait", "Z", i))
        plan.extend(("pass", "Z", i, d) for d in "XYS")
        plan.append(("corner", i))

    def sides(i):
        for k in "XY":
            plan.append(("wait", k, i))
            plan.append(("pass", k, i, "S"))

    def corner(i):
        plan.append(("wait", "D", i))
        if i == 0 and DOWN:
            plan.append(("down",))
        plan.append(("pass", "D", i, "S"))

    for step in SEQUENCE:
        name, i, flags = step[0], int(step[1]), step[2:]
        begin = len(plan)
        if name in "pq":
            plan.append(({"p": "project", "q": "rows"}[name], i))
        else:
            {"c": column, "s": sides, "d": corner}[name](i)
        plan[begin:] = [(flags,) + entry for entry in plan[begin:]]
    return plan


def row_plan(n_sp, plane):
    last = n_sp - 1
    steps, waiting, late, own = [], [], [], []
    for i in range(n_sp):
        ready = list(range(i + 1)) if i == plane else [i] if i > plane else []
        if plane:
            ready = [r for r in ready if r]
        if plane < i == last - 1:
            late, ready = ready, []
        elif 0 < i == plane < last - 1:
            own, ready = ready[-1:], ready[:-1]
        if i == last:
            ready = ready + late + own
        ops, fresh = [], []
        if plane and i == last - 1:
            ops.append(("borrow", 0))
            fresh.append(0)
        if plane == last == i:
            ops.append(("reduce", waiting.pop()))
        for n, r in enumerate(ready):
            ops.append(("finish", r))
            if i == last and n == 0:
                ops += [("reduce", b) for b in waiting]
            if fresh and i >= last - 1:
                ops.append(("reduce", fresh.pop(0)))
            fresh.append(r)
        if i == last:
            if plane:
                ops.append(("collect", 0))
            ops += [("reduce", r) for r in fresh]
            done = [op[1] for step in steps + [ops] for op in step if op[0] == "reduce"]
            ops += [("collect", r) for r in done if r or not plane]
        else:
            waiting += fresh
        steps.append(ops)
    return steps


def whole_kernel(
    sizes,
    plan,
    tokens,
    in_gain,
    ret_query,
    ret_key,
    ret_value,
    decay_log,
    init_state,
    ret_gain,
    diff_query,
    diff_key,
    diff_value,
    diff_lambda,
    diff_gain,
    out_weight,
    out,
    x_all,
    w_all,
    w_pair,
    tok_in,
    gain_in,
    decays,
    init_in,
    ret_gain_in,
    lambda_in,
    diff_gain_in,
    wo,
    pair_q,
    ret_q,
    ret_k,
    ret_v,
    diff_k,
    diff_v,
    states,
    mix,
    part,
    sib,
    red,
    rcv,
    fin,
    got,
    load_sem,
    tok_send,
    tok_recv,
    mate_recv,
    decay_send,
    decay_recv,
    sib_send,
    sib_recv,
    rs_send,
    rs_recv,
    fin_send,
    fin_recv,
    mix_send,
    mix_recv,
):
    n_sp, n_fs, n_tp = sizes
    own_rows, width = tokens.shape
    rows = own_rows * n_fs * n_tp
    head = ret_query.shape[1]
    maps = diff_query.shape[0] // 2
    span = out_weight.shape[2]
    sp, fs, tp = lax.axis_index("sp"), lax.axis_index("fs"), lax.axis_index("tp")
    side = fs + 1 - 2 * lax.rem(fs, 2)
    ahead = lax.rem(fs + 2, 4)
    corner = side + ahead - fs
    mate = 1 - tp
    chip = {"Z": fs, "X": side, "Y": ahead, "D": corner}
    order = plane_order(sp, n_sp)

    def remote(src, dst, send, recv, s, f, t):
        return pltpu.make_async_remote_copy(
            src_ref=src,
            dst_ref=dst,
            send_sem=send,
            recv_sem=recv,
            device_id=(s, f, t),
            device_id_type=pl.DeviceIdType.MESH,
        )

    barrier = pltpu.get_barrier_semaphore()
    peers = [(order[i], fs, tp) for i in range(1, n_sp)]
    peers += [(sp, f, tp) for f in (side, ahead, corner)] + [(sp, fs, mate)]
    for peer in peers:
        pl.semaphore_signal(
            barrier, inc=1, device_id=peer, device_id_type=pl.DeviceIdType.MESH
        )

    def col(slot):
        return w_all.at[:, pl.ds(slot * head, head)]

    loads = [
        (tokens, tok_in),
        (in_gain, gain_in),
        (decay_log, decays.at[sp]),
        (init_state, init_in),
        (ret_gain, ret_gain_in),
        (diff_lambda, lambda_in),
        (diff_gain, diff_gain_in),
        (ret_query, col(0)),
        (ret_key, col(1)),
        (ret_value, col(2)),
        (diff_value, col(3)),
        (diff_key, w_pair.at[pl.ds(0, head)]),
        (diff_query, w_pair.at[pl.ds(head, head)]),
        (out_weight, wo),
    ]
    groups = [0, 1, 2, 3, 4, 5, 6, 7, 7, 7, 7, 8, 8, 9]
    load_copies = [
        pltpu.make_async_copy(src, dst, load_sem.at[i]) for i, (src, dst) in zip(groups, loads)
    ]
    later_loads = load_copies[3:7] + [
        pltpu.make_async_copy(w_all, w_all, load_sem.at[7]),
        pltpu.make_async_copy(w_pair, w_pair, load_sem.at[8]),
        load_copies[13],
    ]
    for c in load_copies:
        c.start()
    me = (sp * n_fs + fs) * n_tp + tp
    own = pl.ds(pl.multiple_of(me * own_rows, own_rows), own_rows)
    load_copies[0].wait()
    load_copies[1].wait()
    wide = tok_in[...].astype(f32)
    scale = lax.rsqrt(jnp.mean(wide * wide, axis=-1, keepdims=True) + EPS)
    x_all[own, :] = (wide * scale * gain_in[...].reshape(1, width)).astype(bf16)
    load_copies[2].wait()
    pl.semaphore_wait(barrier, len(peers))

    pending = {}

    def block(k, i, t):
        rank = (order[i] * n_fs + chip[k]) * n_tp + t
        return x_all.at[pl.ds(pl.multiple_of(rank * own_rows, own_rows), own_rows)]

    def tok_copy(k, i, s, f, dest):
        recv = mate_recv.at[order[i]] if dest is mate else tok_recv.at[order[i], chip[k]]
        return remote(block(k, i, tp), block(k, i, tp), tok_send, recv, s, f, dest)

    tests = {"+": tp == 1, "-": tp == 0, "a": sp == 0, "b": sp > 0}

    def run(flags, go):
        if flags:
            pl.when(functools.reduce(jnp.logical_and, [tests[f] for f in flags]))(go)
        else:
            go()

    def send_tok(flags, *where):
        if "-" not in flags:
            for kind in "ab":
                if kind in flags or not set("ab") & set(flags):
                    pending[kind] = pending.get(kind, 0) + 1
        run(flags, tok_copy(*where).start)

    row_at = lax.broadcasted_iota(jnp.int32, (rows, rows), 0)
    col_at = lax.broadcasted_iota(jnp.int32, (rows, rows), 1)
    lower = row_at >= col_at
    lane = lax.broadcasted_iota(jnp.int32, (rows, 2 * maps), 1)

    def cumulate(d_row):
        d_wide = jnp.broadcast_to(d_row, (rows, rows))
        return d_wide, jnp.sum(jnp.where(lower, d_wide, 0.0), axis=1, keepdims=True)

    def project(i):
        p = order[i]
        quarter = x_all.at[pl.ds(0, n_fs * own_rows)]
        remote(quarter, quarter, tok_send, mate_recv.at[p], sp, fs, tp).wait_recv()
        if i == 1:
            far_decays.wait_recv()
        if i == 0:
            for c in later_loads:
                c.wait()
        x = x_all[pl.ds(pl.multiple_of(p * rows, rows), rows), :]
        proj = jnp.dot(x, w_all[...], preferred_element_type=f32).astype(bf16)
        pairs = lax.dot_general(
            x, w_pair[...], (((1,), (1,)), ((), ())), preferred_element_type=f32
        ).astype(bf16)
        q, k, v, dv = (proj[:, j * head : (j + 1) * head] for j in range(4))
        dk, dq = pairs[:, :head], pairs[:, head:]
        zero = jnp.zeros_like(dq)
        d_row = decays[p]
        cum_col = cumulate(d_row)[1]
        cum_last = jnp.sum(d_row, axis=1, keepdims=True)
        key_weight = jnp.exp(cum_last - cum_col) * head ** (-0.5)
        states[p] = lax.dot_general(
            (k.astype(f32) * key_weight).astype(bf16),
            v,
            (((0,), (0,)), ((), ())),
            preferred_element_type=f32,
        )
        ret_q[p], ret_k[p], ret_v[p], diff_k[p], diff_v[p] = q, k, v, dk, dv
        pair_q[p] = jnp.concatenate(
            [jnp.where(lane < maps, dq, zero), jnp.where(lane < maps, zero, dq)], axis=0
        )

    fs_peers = [side, ahead, corner]

    def sib_copy(r):
        return remote(part.at[r, mate], sib.at[r], sib_send, sib_recv.at[r], sp, fs, mate)

    def place(f):
        return jnp.where(fs > f, fs - 1, fs)

    def rs_copy(r, j):
        f = fs_peers[j]
        return remote(red.at[r, f], rcv.at[r, place(f)], rs_send.at[r], rs_recv.at[r], sp, f, tp)

    def fin_copy(r):
        return remote(fin.at[r], got.at[sp], fin_send, fin_recv, r, fs, tp)

    def finish(r):
        q, k, v = ret_q[r], ret_k[r], ret_v[r]
        scores = lax.dot_general(q, k, (((1,), (1,)), ((), ())), preferred_element_type=f32)
        keys = diff_k[0 : r + 1].reshape((r + 1) * rows, head)
        s = lax.dot_general(
            pair_q[r], keys, (((1,), (1,)), ((), ())), preferred_element_type=f32
        )
        s = [s[:, b * rows : (b + 1) * rows] for b in range(r + 1)]
        s[r] = jnp.where(jnp.concatenate([lower, lower], axis=0), s[r], -HUGE)
        entering = init_in[0].astype(f32)
        for b in range(r):
            entering = jnp.exp(jnp.sum(decays[b], axis=1, keepdims=True)) * entering + states[b]
        reached = jnp.dot(q, entering.astype(bf16), preferred_element_type=f32)
        d_wide, cum_col = cumulate(decays[r])
        d_col = jnp.sum(jnp.where(row_at == col_at, d_wide, 0.0), axis=1, keepdims=True)
        cum_row = jnp.sum(jnp.where(row_at <= col_at, d_col, 0.0), axis=0, keepdims=True)
        fade = jnp.exp(jnp.where(lower, cum_col - cum_row, -HUGE)) * head ** (-0.5)
        inner = jnp.dot((scores * fade).astype(bf16), v, preferred_element_type=f32)
        peak = jnp.max(functools.reduce(jnp.maximum, s), axis=1, keepdims=True)
        w = [jnp.exp((part_s - peak) * maps ** (-0.5)) for part_s in s]
        whole = jnp.sum(functools.reduce(jnp.add, w), axis=1, keepdims=True)
        summed = functools.reduce(
            jnp.add,
            [
                jnp.dot(w[b].astype(bf16), diff_v[b], preferred_element_type=f32)
                for b in range(r + 1)
            ],
        )
        ret_out = inner + jnp.exp(cum_col) * reached
        centre = ret_out - jnp.mean(ret_out, axis=-1, keepdims=True)
        ret_mix = (
            centre
            * lax.rsqrt(jnp.mean(centre * centre, axis=-1, keepdims=True) + EPS)
            * ret_gain_in[...].reshape(1, head)
        ).astype(bf16)
        ratio = summed * (1.0 / whole)
        diff_out = ratio[:rows] - lambda_in[...].reshape(1, 1) * ratio[rows:]
        diff_mix = (
            diff_out
            * lax.rsqrt(jnp.mean(diff_out * diff_out, axis=-1, keepdims=True) + EPS)
            * diff_gain_in[...].reshape(1, head)
        ).astype(bf16)
        mixed = jnp.concatenate([ret_mix, diff_mix], axis=1)
        if r == 0:
            mix[...] = mixed
            for i in range(n_sp - 1, 0, -1):
                mix_copy(i).start()
        emit(r, mixed)

    def mix_copy(i):
        return remote(mix, mix, mix_send.at[i], mix_recv, order[i], fs, tp)

    def borrow(r):
        mix_copy(0).wait_recv()
        emit(r, mix[...])

    def emit(r, mixed):
        value = jnp.dot(mixed, wo[...].reshape(2 * head, span), preferred_element_type=f32).astype(bf16)
        for f in range(n_fs):
            for t in range(n_tp):
                at = (f * n_tp + t) * own_rows
                part[r, t, pl.ds(f * own_rows, own_rows), :] = value[at : at + own_rows]
        sib_copy(r).start()

    def reduce_pair(r):
        sib_copy(r).wait_recv()
        total = part[r, tp].astype(f32) + sib[r].astype(f32)
        red[r] = total.astype(bf16).reshape(n_fs, own_rows, span)
        for j in range(3):
            rs_copy(r, j).start()

    def collect(r):
        shares = rcv.at[r]
        remote(shares, shares, rs_send.at[r], rs_recv.at[r], sp, fs, tp).wait_recv()
        total = red[r, fs].astype(f32)
        for j in range(n_fs - 1):
            total = total + rcv[r, j].astype(f32)
        fin[r] = total.astype(bf16)

        @pl.when(r != sp)
        def _():
            fin_copy(r).start()

    dest = {"X": (sp, side, tp), "Y": (sp, ahead, tp), "D": (sp, corner, tp), "S": (sp, fs, mate)}
    stages = {"finish": finish, "borrow": borrow, "reduce": reduce_pair, "collect": collect}
    row_plans = [row_plan(n_sp, plane) for plane in range(n_sp)]

    all_decays = decays.at[pl.ds(0, n_sp - 1)]
    far_decays = remote(all_decays, all_decays, decay_send, decay_recv, sp, fs, tp)
    for flags, kind, *step in plan:
        if kind == "own":
            i = step[0]
            send_tok(flags, "Z", 0, order[i], fs, tp)
            remote(
                decays.at[sp], decays.at[sp], decay_send, decay_recv, order[i], fs, tp
            ).start()
        elif kind == "pass":
            send_tok(flags, *step[:2], *dest[step[2]])
        elif kind == "corner":
            if not (DOWN and "a" in flags):
                send_tok(flags + ("b" if DOWN and "b" not in flags else ""), "Z", step[0], *dest["D"])
        elif kind == "down":
            if "a" not in flags:
                send_tok(flags + ("" if "b" in flags else "b"), "D", 0, 0, fs, tp)
        elif kind == "wait":
            run(flags, tok_copy(*step, sp, fs, tp).wait_recv)
        elif kind == "project":
            run(flags, functools.partial(project, step[0]))
        else:
            i = step[0]
            for plane in range(n_sp):

                def rows_done(ops=row_plans[plane][i]):
                    for stage, r in ops:
                        stages[stage](r)

                if row_plans[plane][i]:
                    pl.when(sp == plane)(rows_done)

    others = got.at[pl.ds(0, n_sp - 1)]
    arrived = remote(others, others, fin_send, fin_recv, sp, fs, tp)
    arrived.wait_recv()
    for c in range(n_sp):
        out[:, c * span : (c + 1) * span] = jnp.where(sp == c, fin[c], got[c])

    for flag, count in pending.items():
        sent = x_all.at[pl.ds(0, count * own_rows)]
        run(flag, remote(sent, sent, tok_send, mate_recv.at[0], sp, fs, tp).wait_send)
    far_decays.wait_send()
    halves = part.at[:, 0]
    remote(halves, halves, sib_send, sib_recv.at[0], sp, fs, tp).wait_send()
    for r in range(n_sp):
        shares = rcv.at[r]
        remote(shares, shares, rs_send.at[r], rs_recv.at[r], sp, fs, tp).wait_send()
    arrived.wait_send()

    @pl.when(sp == 0)
    def _():
        for i in range(1, n_sp):
            mix_copy(i).wait_send()


def whole_call(mesh_sizes, args):
    n_sp, n_fs, n_tp = mesh_sizes
    tokens, ret_query, diff_query, out_weight = args[0], args[2], args[8], args[13]
    own_rows, width = tokens.shape
    rows = own_rows * n_fs * n_tp
    head = ret_query.shape[1]
    span = out_weight.shape[2]
    plan = gather_plan(n_sp)
    hbm = pl.BlockSpec(memory_space=pltpu.HBM)
    dma = pltpu.SemaphoreType.DMA
    loaded = lambda i: pltpu.VMEM(args[i].shape, args[i].dtype)
    return pl.pallas_call(
        functools.partial(whole_kernel, mesh_sizes, plan),
        out_shape=pltpu.VMEM(tokens.shape, bf16),
        in_specs=[hbm] * 14,
        out_specs=pl.BlockSpec(memory_space=pltpu.VMEM),
        scratch_shapes=[
            pltpu.VMEM((n_sp * rows, width), bf16),
            pltpu.VMEM((width, 4 * head), bf16),
            pltpu.VMEM((2 * head, width), bf16),
            loaded(0),
            loaded(1),
            pltpu.VMEM((n_sp,) + args[5].shape, f32),
            *[loaded(i) for i in (6, 7, 11, 12)],
            loaded(13),
            pltpu.VMEM((n_sp, 2 * rows, head), bf16),
            *[pltpu.VMEM((n_sp, rows, head), bf16) for _ in range(5)],
            pltpu.VMEM((n_sp, head, head), f32),
            pltpu.VMEM((rows, 2 * head), bf16),
            pltpu.VMEM((n_sp, n_tp, n_fs * own_rows, span), bf16),
            pltpu.VMEM((n_sp, n_fs * own_rows, span), bf16),
            pltpu.VMEM((n_sp, n_fs, own_rows, span), bf16),
            pltpu.VMEM((n_sp, n_fs - 1, own_rows, span), bf16),
            *[pltpu.VMEM((n_sp, own_rows, span), bf16) for _ in range(2)],
            dma((10,)),
            dma,
            dma((n_sp, n_fs)),
            dma((n_sp,)),
            dma,
            dma,
            dma,
            dma((n_sp,)),
            dma((n_sp,)),
            dma((n_sp,)),
            dma,
            dma,
            dma((n_sp,)),
            dma,
        ],
        compiler_params=pltpu.CompilerParams(
            collective_id=0, has_side_effects=True, vmem_limit_bytes=66900000
        ),
        name="layer",
    )(*args)


def solution(mesh):
    n_sp, n_fs, n_tp = (mesh.shape[a] for a in ("sp", "fs", "tp"))

    def local(*args):
        args = list(args)
        tokens, ret_query, diff_query, out_weight = args[0], args[2], args[8], args[13]
        own_rows, width = tokens.shape
        rows = own_rows * n_fs * n_tp
        head = ret_query.shape[1]
        maps = diff_query.shape[2]
        assert 2 * maps == head
        assert args[5].shape[1] == rows == head
        ring = out_weight.shape[2] % 128 == 0 and 1 < n_sp <= 8
        whole = ring and n_sp == 4 and n_fs == 4 and n_tp == 2
        if not ring:
            args[13] = lax.all_gather(out_weight, "sp", axis=2, tiled=True)
        for i in (8, 9):
            args[i] = jnp.swapaxes(args[i], 1, 2).reshape(2 * maps, width)
        if whole:
            return whole_call((n_sp, n_fs, n_tp), args)
        chunks = n_sp if ring else 4
        vmem = pl.BlockSpec(memory_space=pltpu.VMEM)
        hbm = pl.BlockSpec(memory_space=pltpu.HBM)
        in_specs = [hbm] * 13 + [hbm if ring else vmem]
        dma = pltpu.SemaphoreType.DMA
        wo_shape = (n_sp,) + out_weight.shape if ring else (1, 2, 16, 128)
        return pl.pallas_call(
            functools.partial(kernel, (n_sp, n_fs, n_tp, ring)),
            out_shape=jax.ShapeDtypeStruct(tokens.shape, bf16),
            in_specs=in_specs,
            out_specs=vmem,
            scratch_shapes=[
                pltpu.VMEM((rows, width), bf16),
                pltpu.VMEM((width, 4 * head), bf16),
                pltpu.VMEM((4 * maps, width), bf16),
                *[pltpu.VMEM(args[i].shape, args[i].dtype) for i in (0, 1, 5, 6, 7, 11, 12)],
                pltpu.VMEM((n_sp, rows, 2 * head), bf16),
                pltpu.VMEM((n_sp, head + own_rows, head), bf16),
                pltpu.VMEM(wo_shape, bf16),
                pltpu.VMEM((n_tp, n_fs * own_rows, width), bf16),
                pltpu.VMEM((n_tp, n_fs * own_rows, width), bf16),
                pltpu.VMEM((n_fs, own_rows, width), bf16),
                pltpu.VMEM((n_fs, own_rows, width), bf16),
                dma((14,)),
                dma((TOKEN_CHUNKS, n_fs)),
                dma((TOKEN_CHUNKS, n_fs * n_tp)),
                dma((TOKEN_CHUNKS, n_fs, n_tp)),
                dma((n_sp,)),
                dma((n_sp,)),
                dma((n_sp,)),
                dma((n_sp,)),
                dma((2, n_sp)),
                dma((n_sp,)),
                dma((chunks, n_tp)),
                dma((chunks, n_tp)),
                dma((chunks, n_fs)),
                dma((chunks, n_fs)),
            ],
            compiler_params=pltpu.CompilerParams(
                collective_id=0, has_side_effects=True, vmem_limit_bytes=67043328
            ),
            name="layer",
        )(*args)

    in_specs = (
        P(("sp", "fs", "tp"), None),
        P(),
        P(None, ("fs", "tp")),
        P(None, ("fs", "tp")),
        P(None, ("fs", "tp")),
        P(("fs", "tp"), "sp"),
        P(("fs", "tp"), None, None),
        P(("fs", "tp")),
        P(None, None, ("fs", "tp")),
        P(None, None, ("fs", "tp")),
        P(None, ("fs", "tp")),
        P(("fs", "tp")),
        P(("fs", "tp")),
        P(None, ("fs", "tp"), "sp"),
    )
    out_specs = P(("sp", "fs", "tp"), None)
    return jax.shard_map(local, mesh=mesh, in_specs=in_specs, out_specs=out_specs, check_vma=False)
```

```python
import functools

import jax
import jax.numpy as jnp
from jax import lax
from jax.experimental import pallas as pl
from jax.experimental.pallas import tpu as pltpu
from jax.sharding import PartitionSpec as P

EPS = 1e-06
HUGE = 1e30
TOKEN_CHUNKS = 1
DOWN = 2
EARLY = True
SEQUENCE = ("c1", "s0", "d0", "c2b", "s1b", "c3b", "c2+a", "s1+a", "c3+a", "p0a", "q0", "c2-a", "s1-a", "c3-a", "d1+", "s2+", "d2+", "s3+", "d3+", "p0b", "d1-a", "p1a", "s2-a", "d2-a", "d3-a", "q1", "s3-a", "d1-b", "s2-b", "p1b", "d2-b", "p2", "s3-b", "d3-b", "q2", "p3", "q3")
f32 = jnp.float32
bf16 = jnp.bfloat16


def kernel(
    sizes,
    tokens,
    in_gain,
    ret_query,
    ret_key,
    ret_value,
    decay_log,
    init_state,
    ret_gain,
    diff_query,
    diff_key,
    diff_value,
    diff_lambda,
    diff_gain,
    out_weight,
    out,
    x_all,
    w_all,
    w_pair,
    tok_in,
    gain_in,
    decay_in,
    init_in,
    ret_gain_in,
    lambda_in,
    diff_gain_in,
    kv,
    st,
    wo,
    part,
    sib,
    red,
    rcv,
    load_sem,
    tok_send,
    tok_recv,
    fwd_send,
    kv_send,
    kv_recv,
    st_send,
    st_recv,
    wo_send,
    wo_recv,
    sib_send,
    sib_recv,
    rs_send,
    rs_recv,
):
    n_sp, n_fs, n_tp, ring = sizes
    own_rows, width = tokens.shape
    rows = own_rows * n_fs * n_tp
    head = ret_query.shape[1]
    maps = diff_query.shape[0] // 2
    sp, fs, tp = lax.axis_index("sp"), lax.axis_index("fs"), lax.axis_index("tp")
    half = max(n_fs // 2, 1)
    fs_peers = []
    for d in range(1, n_fs):
        if n_fs % 2 == 0:
            fs_peers.append(
                lax.rem(lax.div(fs, 2) + d // 2, half) * 2 + lax.rem(lax.rem(fs, 2) + d % 2, 2)
            )
        else:
            fs_peers.append(lax.rem(fs + d, n_fs))
    tp_peers = [lax.rem(tp + d, n_tp) for d in range(1, n_tp)]

    def remote(src, dst, send, recv, s, f, t):
        return pltpu.make_async_remote_copy(
            src_ref=src,
            dst_ref=dst,
            send_sem=send,
            recv_sem=recv,
            device_id=(s, f, t),
            device_id_type=pl.DeviceIdType.MESH,
        )

    barrier = pltpu.get_barrier_semaphore()

    def greet(s, f, t):
        pl.semaphore_signal(
            barrier, inc=1, device_id=(s, f, t), device_id_type=pl.DeviceIdType.MESH
        )

    for f in fs_peers:
        greet(sp, f, tp)
    for t in tp_peers:
        greet(sp, fs, t)

    def greet_sp(d, c):
        greet(lax.rem(sp + d, n_sp), fs, tp)
        return c

    if n_sp <= 8:
        for d in range(1, n_sp):
            greet_sp(d, 0)
    else:
        lax.fori_loop(1, n_sp, greet_sp, 0)

    def col(slot):
        return w_all.at[:, pl.ds(slot * head, head)]

    loads = [
        (tokens, tok_in),
        (in_gain, gain_in),
        (decay_log, decay_in),
        (init_state, init_in),
        (ret_gain, ret_gain_in),
        (diff_lambda, lambda_in),
        (diff_gain, diff_gain_in),
        (ret_query, col(0)),
        (ret_key, col(1)),
        (ret_value, col(2)),
        (diff_value, col(3)),
        (diff_key, w_pair.at[pl.ds(0, head)]),
        (diff_query, w_pair.at[pl.ds(head, head)]),
    ]
    load_copies = [
        pltpu.make_async_copy(src, dst, load_sem.at[i]) for i, (src, dst) in enumerate(loads)
    ]
    for c in load_copies:
        c.start()
    if ring:
        own_wo = pltpu.make_async_copy(out_weight, wo.at[sp], load_sem.at[len(loads)])
        own_wo.start()

    me = fs * n_tp + tp
    own = pl.ds(pl.multiple_of(me * own_rows, own_rows), own_rows)
    load_copies[0].wait()
    load_copies[1].wait()
    wide = tok_in[...].astype(f32)
    scale = lax.rsqrt(jnp.mean(wide * wide, axis=-1, keepdims=True) + EPS)
    x_all[own, :] = (wide * scale * gain_in[...].reshape(1, width)).astype(bf16)

    pl.semaphore_wait(barrier, len(fs_peers) + len(tp_peers) + n_sp - 1)

    cw = width // TOKEN_CHUNKS

    def block(rank, c):
        return x_all.at[
            pl.ds(pl.multiple_of(rank * own_rows, own_rows), own_rows), pl.ds(c * cw, cw)
        ]

    def tok_copy(c, rank, send, f, t):
        return remote(block(rank, c), block(rank, c), send, tok_recv.at[c, rank], sp, f, t)

    pending = []
    for c in range(TOKEN_CHUNKS):
        for i, f in enumerate(fs_peers):
            cp = tok_copy(c, me, tok_send.at[c, i], f, tp)
            cp.start()
            pending.append(cp)
        for i, t in enumerate(tp_peers):
            cp = tok_copy(c, me, fwd_send.at[c, n_fs - 1, i], fs, t)
            cp.start()
            pending.append(cp)

    def wo_copy(origin, way, step):
        src = out_weight if step == 0 else wo.at[origin]
        dest = sp + 1 - 2 * way
        return remote(
            src, wo.at[origin], wo_send.at[way, step], wo_recv.at[origin], dest, fs, tp
        )

    def each_way(step, go):
        for way in range(2):
            origin = sp - step if way == 0 else sp + step
            inside = origin >= 0 if way == 0 else origin < n_sp
            onward = sp < n_sp - 1 if way == 0 else sp > 0

            @pl.when(jnp.logical_and(inside, onward))
            def _():
                go(wo_copy(lax.rem(origin + n_sp, n_sp), way, step))

    def pass_on(step):
        def go(cp):
            if step:
                cp.wait_recv()
            cp.start()

        each_way(step, go)

    if ring:
        pass_on(0)

    load_copies[2].wait()
    d_row = decay_in[...]
    row_at = lax.broadcasted_iota(jnp.int32, (rows, rows), 0)
    col_at = lax.broadcasted_iota(jnp.int32, (rows, rows), 1)
    lower = row_at >= col_at
    d_wide = jnp.broadcast_to(d_row, (rows, rows))
    cum_col = jnp.sum(jnp.where(lower, d_wide, 0.0), axis=1, keepdims=True)
    d_col = jnp.sum(jnp.where(row_at == col_at, d_wide, 0.0), axis=1, keepdims=True)
    cum_row = jnp.sum(jnp.where(row_at <= col_at, d_col, 0.0), axis=0, keepdims=True)
    cum_last = jnp.sum(d_row, axis=1, keepdims=True)
    fade = jnp.exp(jnp.where(lower, cum_col - cum_row, -HUGE)) * head ** (-0.5)
    key_weight = jnp.exp(cum_last - cum_col) * head ** (-0.5)
    query_weight = jnp.exp(cum_col)
    decay = jnp.broadcast_to(jnp.exp(cum_last), (own_rows, head))
    decay_high = decay.astype(bf16).astype(f32)
    first = lax.broadcasted_iota(jnp.int32, (own_rows, head), 0) < own_rows // 2
    st[sp, pl.ds(head, own_rows), :] = jnp.where(first, decay_high, decay - decay_high).astype(bf16)

    for c in load_copies[3:]:
        c.wait()

    total = None
    for c in range(TOKEN_CHUNKS):
        if ring and c == TOKEN_CHUNKS - 1:
            pass_on(1)
        for k, f in enumerate(fs_peers):
            rank = f * n_tp + tp
            tok_copy(c, rank, tok_send.at[c, k], fs, tp).wait_recv()
            for i, t in enumerate(tp_peers):
                cp = tok_copy(c, rank, fwd_send.at[c, k, i], fs, t)
                cp.start()
                pending.append(cp)
        for t in tp_peers:
            for f in [fs] + fs_peers:
                tok_copy(c, f * n_tp + t, tok_send.at[c, 0], fs, tp).wait_recv()
        cols = slice(c * cw, (c + 1) * cw)
        piece = (
            jnp.dot(x_all[:, cols], w_all[cols, :], preferred_element_type=f32),
            lax.dot_general(
                x_all[:, cols],
                w_pair[:, cols],
                (((1,), (1,)), ((), ())),
                preferred_element_type=f32,
            ),
        )
        total = piece if total is None else (total[0] + piece[0], total[1] + piece[1])
    proj, pairs = total[0].astype(bf16), total[1].astype(bf16)
    ret_q, ret_k, ret_v, diff_v = (proj[:, i * head : (i + 1) * head] for i in range(4))
    diff_k, diff_q = pairs[:, :head], pairs[:, head:]
    kv[sp, :, :head] = diff_k
    kv[sp, :, head:] = diff_v

    def to_later(buf, send, recv, go):
        def one(d, c):
            @pl.when(sp + d < n_sp)
            def _():
                cp = remote(buf.at[sp], buf.at[sp], send.at[d], recv.at[sp], sp + d, fs, tp)
                go(cp)

            return c

        if n_sp <= 8:
            for d in range(n_sp - 1, 0, -1):
                one(d, 0)
        else:
            lax.fori_loop(1, n_sp, one, 0)

    to_later(kv, kv_send, kv_recv, lambda cp: cp.start())
    weighted = (ret_k.astype(f32) * key_weight).astype(bf16)
    state = lax.dot_general(
        weighted, ret_v, (((0,), (0,)), ((), ())), preferred_element_type=f32
    )
    st[sp, pl.ds(0, head), :] = state.astype(bf16)
    to_later(st, st_send, st_recv, lambda cp: cp.start())

    scores = lax.dot_general(ret_q, ret_k, (((1,), (1,)), ((), ())), preferred_element_type=f32)
    inner = jnp.dot((scores * fade).astype(bf16), ret_v, preferred_element_type=f32)
    lane = lax.broadcasted_iota(jnp.int32, (rows, 2 * maps), 1)
    zero = jnp.zeros_like(diff_q)
    pair_q = jnp.concatenate(
        [jnp.where(lane < maps, diff_q, zero), jnp.where(lane < maps, zero, diff_q)], axis=0
    )

    def one_block(keys, values, allowed):
        s = lax.dot_general(pair_q, keys, (((1,), (1,)), ((), ())), preferred_element_type=f32)
        s = s * maps ** (-0.5)
        if allowed is not None:
            s = jnp.where(allowed, s, -HUGE)
        peak = jnp.max(s, axis=1, keepdims=True)
        w = jnp.exp(s - peak)
        return (
            peak,
            jnp.sum(w, axis=1, keepdims=True),
            jnp.dot(w.astype(bf16), values, preferred_element_type=f32),
        )

    peak, whole, summed = one_block(diff_k, diff_v, jnp.concatenate([lower, lower], axis=0))

    if ring:
        for step in range(2, n_sp - 1):
            pass_on(step)

    def earlier(d, carry):
        peak, whole, summed, run, entering = carry
        b = sp - d
        remote(kv.at[b], kv.at[b], kv_send.at[0], kv_recv.at[b], sp, fs, tp).wait_recv()
        peak_b, whole_b, sum_b = one_block(kv[b, :, :head], kv[b, :, head:], None)
        top = jnp.maximum(peak, peak_b)
        before, after = jnp.exp(peak - top), jnp.exp(peak_b - top)
        remote(st.at[b], st.at[b], st_send.at[0], st_recv.at[b], sp, fs, tp).wait_recv()
        entering = entering + run * st[b, pl.ds(0, head), :].astype(f32)
        tail = st[b, pl.ds(head, own_rows), :].astype(f32)
        last = own_rows // 2
        return (
            top,
            whole * before + whole_b * after,
            summed * before + sum_b * after,
            run * (tail[0:1] + tail[last : last + 1]),
            entering,
        )

    peak, whole, summed, run, entering = lax.fori_loop(
        1,
        sp + 1,
        earlier,
        (peak, whole, summed, jnp.ones((1, head), f32), jnp.zeros((head, head), f32)),
    )
    entering = entering + run * init_in[0].astype(f32)
    reached = jnp.dot(ret_q, entering.astype(bf16), preferred_element_type=f32)
    ret_out = inner + query_weight * reached
    centre = ret_out - jnp.mean(ret_out, axis=-1, keepdims=True)
    ret_mix = (
        centre
        * lax.rsqrt(jnp.mean(centre * centre, axis=-1, keepdims=True) + EPS)
        * ret_gain_in[...].reshape(1, head)
    ).astype(bf16)
    lam = lambda_in[...].reshape(1, 1)
    ratio = summed / whole
    diff_out = ratio[:rows] - lam * ratio[rows:]
    diff_mix = (
        diff_out
        * lax.rsqrt(jnp.mean(diff_out * diff_out, axis=-1, keepdims=True) + EPS)
        * diff_gain_in[...].reshape(1, head)
    ).astype(bf16)
    mixed = jnp.concatenate([ret_mix, diff_mix], axis=1)

    if ring:
        own_wo.wait()
        order = [sp]
        low, high = sp - 1, sp + 1
        for _ in range(1, n_sp):
            down = jnp.logical_and(
                low >= 0, jnp.logical_or(high >= n_sp, sp - low <= high - sp)
            )
            order.append(jnp.where(down, low, high))
            low, high = jnp.where(down, low - 1, low), jnp.where(down, high, high + 1)
        span = out_weight.shape[2]
    else:
        order = list(range(4))
        span = width // 4

    def columns(s):
        if isinstance(s, int):
            return pl.ds(s * span, span)
        return pl.ds(pl.multiple_of(s * span, 128), span)

    def sib_copy(k, i, t):
        cols = columns(order[k])
        return remote(
            part.at[t, :, cols], sib.at[tp, :, cols], sib_send.at[k, i], sib_recv.at[k, tp], sp, fs, t
        )

    def rs_copy(k, i, f):
        cols = columns(order[k])
        return remote(
            red.at[f, :, cols], rcv.at[fs, :, cols], rs_send.at[k, i], rs_recv.at[k, fs], sp, f, tp
        )

    def reduce_pair(k):
        cols = columns(order[k])
        acc = part[tp, :, cols].astype(f32)
        for i, t in enumerate(tp_peers):
            remote(
                part.at[t, :, cols], sib.at[t, :, cols], sib_send.at[k, i], sib_recv.at[k, t], sp, fs, tp
            ).wait_recv()
            acc = acc + sib[t, :, cols].astype(f32)
        red[:, :, cols] = acc.astype(bf16).reshape(n_fs, own_rows, span)
        for i, f in enumerate(fs_peers):
            cp = rs_copy(k, i, f)
            cp.start()
            pending.append(cp)

    for k, s in enumerate(order):
        if ring and k:

            @pl.when(jnp.logical_or(sp == 0, sp == n_sp - 1))
            def _():
                wo_copy(s, 0, k).wait_recv()

        if ring:
            w = wo[s].reshape(2 * head, span)
        else:
            w = out_weight[:, :, s * span : (s + 1) * span].reshape(2 * head, span)
        value = jnp.dot(mixed, w, preferred_element_type=f32).astype(bf16)
        cols = columns(s)
        for f in range(n_fs):
            for t in range(n_tp):
                at = (f * n_tp + t) * own_rows
                part[t, pl.ds(f * own_rows, own_rows), cols] = value[at : at + own_rows]
        for i, t in enumerate(tp_peers):
            cp = sib_copy(k, i, t)
            cp.start()
            pending.append(cp)
        if k >= 1:
            reduce_pair(k - 1)
    reduce_pair(len(order) - 1)

    for k, s in enumerate(order):
        cols = columns(s)
        acc = red[fs, :, cols].astype(f32)
        for i, f in enumerate(fs_peers):
            remote(
                red.at[f, :, cols], rcv.at[f, :, cols], rs_send.at[k, i], rs_recv.at[k, f], sp, fs, tp
            ).wait_recv()
            acc = acc + rcv[f, :, cols].astype(f32)
        out[:, cols] = acc.astype(bf16)

    for cp in pending:
        cp.wait_send()
    if ring:
        for step in range(n_sp - 1):
            each_way(step, lambda cp: cp.wait_send())
    to_later(kv, kv_send, kv_recv, lambda cp: cp.wait_send())
    to_later(st, st_send, st_recv, lambda cp: cp.wait_send())


def plane_order(sp, n_sp):
    return [jnp.where(i <= sp, sp - i, i) for i in range(n_sp)]


def gather_plan(n_sp):
    plan = []
    for i in range(1, n_sp):
        plan.append(("", "own", i))
    for d in "XYDS":
        plan.append(("", "pass", "Z", 0, d))

    def column(i):
        plan.append(("wait", "Z", i))
        plan.extend(("pass", "Z", i, d) for d in "XYS")
        plan.append(("corner", i))

    def sides(i):
        for k in "XY":
            plan.append(("wait", k, i))
            plan.append(("pass", k, i, "S"))

    def corner(i):
        plan.append(("wait", "D", i))
        if i == 0:
            plan.append(("down",))
        plan.append(("pass", "D", i, "S"))

    for step in SEQUENCE:
        name, i, flags = step[0], int(step[1]), step[2:]
        begin = len(plan)
        if name in "pq":
            plan.append(({"p": "project", "q": "rows"}[name], i))
        else:
            {"c": column, "s": sides, "d": corner}[name](i)
        plan[begin:] = [(flags,) + entry for entry in plan[begin:]]
    return plan


def row_plan(n_sp, plane):
    last = n_sp - 1
    steps, waiting, late, own = [], [], [], []
    for i in range(n_sp):
        ready = list(range(i + 1)) if i == plane else [i] if i > plane else []
        if plane:
            ready = [r for r in ready if r]
        if plane < i == last - 1:
            late, ready = ready, []
        elif 0 < i == plane < last - 1:
            own, ready = ready[-1:], ready[:-1]
        if i == last:
            ready = ready + late + own
        ops, fresh = [], []
        if plane and i == last - 1:
            ops.append(("borrow", 0))
            fresh.append(0)
        if plane == last == i or (EARLY and plane == 0 and i == 1):
            ops.append(("reduce", waiting.pop()))
        for n, r in enumerate(ready):
            ops.append(("finish", r))
            if i == last and n == 0:
                ops += [("reduce", b) for b in waiting]
            if fresh and i >= last - 1:
                ops.append(("reduce", fresh.pop(0)))
            fresh.append(r)
        if i == last:
            if plane:
                ops.append(("collect", 0))
            ops += [("reduce", r) for r in fresh]
            done = [op[1] for step in steps + [ops] for op in step if op[0] == "reduce"]
            ops += [("collect", r) for r in done if r or not plane]
        else:
            waiting += fresh
        steps.append(ops)
    return steps


def whole_kernel(
    sizes,
    plan,
    tokens,
    in_gain,
    ret_query,
    ret_key,
    ret_value,
    decay_log,
    init_state,
    ret_gain,
    diff_query,
    diff_key,
    diff_value,
    diff_lambda,
    diff_gain,
    out_weight,
    out,
    x_all,
    w_all,
    w_pair,
    tok_in,
    gain_in,
    decays,
    init_in,
    ret_gain_in,
    lambda_in,
    diff_gain_in,
    wo,
    pair_q,
    ret_q,
    ret_k,
    ret_v,
    diff_k,
    diff_v,
    states,
    mix,
    part,
    sib,
    red,
    rcv,
    fin,
    got,
    load_sem,
    tok_send,
    tok_recv,
    mate_recv,
    decay_send,
    decay_recv,
    sib_send,
    sib_recv,
    rs_send,
    rs_recv,
    fin_send,
    fin_recv,
    mix_send,
    mix_recv,
):
    n_sp, n_fs, n_tp = sizes
    own_rows, width = tokens.shape
    rows = own_rows * n_fs * n_tp
    head = ret_query.shape[1]
    maps = diff_query.shape[0] // 2
    span = out_weight.shape[2]
    sp, fs, tp = lax.axis_index("sp"), lax.axis_index("fs"), lax.axis_index("tp")
    side = fs + 1 - 2 * lax.rem(fs, 2)
    ahead = lax.rem(fs + 2, 4)
    corner = side + ahead - fs
    mate = 1 - tp
    chip = {"Z": fs, "X": side, "Y": ahead, "D": corner}
    order = plane_order(sp, n_sp)

    def remote(src, dst, send, recv, s, f, t):
        return pltpu.make_async_remote_copy(
            src_ref=src,
            dst_ref=dst,
            send_sem=send,
            recv_sem=recv,
            device_id=(s, f, t),
            device_id_type=pl.DeviceIdType.MESH,
        )

    barrier = pltpu.get_barrier_semaphore()
    peers = [(order[i], fs, tp) for i in range(1, n_sp)]
    peers += [(sp, f, tp) for f in (side, ahead, corner)] + [(sp, fs, mate)]
    for peer in peers:
        pl.semaphore_signal(
            barrier, inc=1, device_id=peer, device_id_type=pl.DeviceIdType.MESH
        )

    def col(slot):
        return w_all.at[:, pl.ds(slot * head, head)]

    loads = [
        (tokens, tok_in),
        (in_gain, gain_in),
        (decay_log, decays.at[sp]),
        (init_state, init_in),
        (ret_gain, ret_gain_in),
        (diff_lambda, lambda_in),
        (diff_gain, diff_gain_in),
        (ret_query, col(0)),
        (ret_key, col(1)),
        (ret_value, col(2)),
        (diff_value, col(3)),
        (diff_key, w_pair.at[pl.ds(0, head)]),
        (diff_query, w_pair.at[pl.ds(head, head)]),
        (out_weight, wo),
    ]
    groups = [0, 1, 2, 3, 4, 5, 6, 7, 7, 7, 7, 8, 8, 9]
    load_copies = [
        pltpu.make_async_copy(src, dst, load_sem.at[i]) for i, (src, dst) in zip(groups, loads)
    ]
    later_loads = load_copies[3:7] + [
        pltpu.make_async_copy(w_all, w_all, load_sem.at[7]),
        pltpu.make_async_copy(w_pair, w_pair, load_sem.at[8]),
        load_copies[13],
    ]
    for c in load_copies:
        c.start()
    me = (sp * n_fs + fs) * n_tp + tp
    own = pl.ds(pl.multiple_of(me * own_rows, own_rows), own_rows)
    load_copies[0].wait()
    load_copies[1].wait()
    wide = tok_in[...].astype(f32)
    scale = lax.rsqrt(jnp.mean(wide * wide, axis=-1, keepdims=True) + EPS)
    x_all[own, :] = (wide * scale * gain_in[...].reshape(1, width)).astype(bf16)
    load_copies[2].wait()
    pl.semaphore_wait(barrier, len(peers))

    pending = [0] * n_sp

    def block(k, i, t):
        rank = (order[i] * n_fs + chip[k]) * n_tp + t
        return x_all.at[pl.ds(pl.multiple_of(rank * own_rows, own_rows), own_rows)]

    def tok_copy(k, i, s, f, dest):
        recv = mate_recv.at[order[i]] if dest is mate else tok_recv.at[order[i], chip[k]]
        return remote(block(k, i, tp), block(k, i, tp), tok_send, recv, s, f, dest)

    tests = {"+": tp == 1, "-": tp == 0, "a": sp == 0, "b": sp > 0, "h": sp >= DOWN}
    least = {"b": 1, "h": DOWN}

    def run(flags, go):
        if flags:
            pl.when(functools.reduce(jnp.logical_and, [tests[f] for f in flags]))(go)
        else:
            go()

    def send_tok(flags, *where):
        if "-" not in flags:
            for plane in range(n_sp):
                if plane >= max(least.get(f, 0) for f in flags + "+") and not ("a" in flags and plane):
                    pending[plane] += 1
        run(flags, tok_copy(*where).start)

    row_at = lax.broadcasted_iota(jnp.int32, (rows, rows), 0)
    col_at = lax.broadcasted_iota(jnp.int32, (rows, rows), 1)
    lower = row_at >= col_at
    lane = lax.broadcasted_iota(jnp.int32, (rows, 2 * maps), 1)

    def cumulate(d_row):
        d_wide = jnp.broadcast_to(d_row, (rows, rows))
        return d_wide, jnp.sum(jnp.where(lower, d_wide, 0.0), axis=1, keepdims=True)

    def project(i):
        p = order[i]
        quarter = x_all.at[pl.ds(0, n_fs * own_rows)]
        remote(quarter, quarter, tok_send, mate_recv.at[p], sp, fs, tp).wait_recv()
        if i == 1:
            far_decays.wait_recv()
        if i == 0:
            for c in later_loads:
                c.wait()
        x = x_all[pl.ds(pl.multiple_of(p * rows, rows), rows), :]
        proj = jnp.dot(x, w_all[...], preferred_element_type=f32).astype(bf16)
        pairs = lax.dot_general(
            x, w_pair[...], (((1,), (1,)), ((), ())), preferred_element_type=f32
        ).astype(bf16)
        q, k, v, dv = (proj[:, j * head : (j + 1) * head] for j in range(4))
        dk, dq = pairs[:, :head], pairs[:, head:]
        zero = jnp.zeros_like(dq)
        d_row = decays[p]
        cum_col = cumulate(d_row)[1]
        cum_last = jnp.sum(d_row, axis=1, keepdims=True)
        key_weight = jnp.exp(cum_last - cum_col) * head ** (-0.5)
        states[p] = lax.dot_general(
            (k.astype(f32) * key_weight).astype(bf16),
            v,
            (((0,), (0,)), ((), ())),
            preferred_element_type=f32,
        )
        ret_q[p], ret_k[p], ret_v[p], diff_k[p], diff_v[p] = q, k, v, dk, dv
        pair_q[p] = jnp.concatenate(
            [jnp.where(lane < maps, dq, zero), jnp.where(lane < maps, zero, dq)], axis=0
        )

    fs_peers = [corner, side, ahead]

    def sib_copy(r):
        return remote(part.at[r, mate], sib.at[r], sib_send, sib_recv.at[r], sp, fs, mate)

    def place(f):
        return jnp.where(fs > f, fs - 1, fs)

    def rs_copy(r, j):
        f = fs_peers[j]
        return remote(red.at[r, f], rcv.at[r, place(f)], rs_send.at[r], rs_recv.at[r], sp, f, tp)

    def fin_copy(r):
        return remote(fin.at[r], got.at[sp], fin_send, fin_recv, r, fs, tp)

    def finish(r):
        q, k, v = ret_q[r], ret_k[r], ret_v[r]
        scores = lax.dot_general(q, k, (((1,), (1,)), ((), ())), preferred_element_type=f32)
        keys = diff_k[0 : r + 1].reshape((r + 1) * rows, head)
        s = lax.dot_general(
            pair_q[r], keys, (((1,), (1,)), ((), ())), preferred_element_type=f32
        )
        s = [s[:, b * rows : (b + 1) * rows] for b in range(r + 1)]
        s[r] = jnp.where(jnp.concatenate([lower, lower], axis=0), s[r], -HUGE)
        entering = init_in[0].astype(f32)
        for b in range(r):
            entering = jnp.exp(jnp.sum(decays[b], axis=1, keepdims=True)) * entering + states[b]
        reached = jnp.dot(q, entering.astype(bf16), preferred_element_type=f32)
        d_wide, cum_col = cumulate(decays[r])
        d_col = jnp.sum(jnp.where(row_at == col_at, d_wide, 0.0), axis=1, keepdims=True)
        cum_row = jnp.sum(jnp.where(row_at <= col_at, d_col, 0.0), axis=0, keepdims=True)
        fade = jnp.exp(jnp.where(lower, cum_col - cum_row, -HUGE)) * head ** (-0.5)
        inner = jnp.dot((scores * fade).astype(bf16), v, preferred_element_type=f32)
        peak = jnp.max(functools.reduce(jnp.maximum, s), axis=1, keepdims=True)
        w = [jnp.exp((part_s - peak) * maps ** (-0.5)) for part_s in s]
        whole = jnp.sum(functools.reduce(jnp.add, w), axis=1, keepdims=True)
        summed = functools.reduce(
            jnp.add,
            [
                jnp.dot(w[b].astype(bf16), diff_v[b], preferred_element_type=f32)
                for b in range(r + 1)
            ],
        )
        ret_out = inner + jnp.exp(cum_col) * reached
        centre = ret_out - jnp.mean(ret_out, axis=-1, keepdims=True)
        ret_mix = (
            centre
            * lax.rsqrt(jnp.mean(centre * centre, axis=-1, keepdims=True) + EPS)
            * ret_gain_in[...].reshape(1, head)
        ).astype(bf16)
        ratio = summed * (1.0 / whole)
        diff_out = ratio[:rows] - lambda_in[...].reshape(1, 1) * ratio[rows:]
        diff_mix = (
            diff_out
            * lax.rsqrt(jnp.mean(diff_out * diff_out, axis=-1, keepdims=True) + EPS)
            * diff_gain_in[...].reshape(1, head)
        ).astype(bf16)
        mixed = jnp.concatenate([ret_mix, diff_mix], axis=1)
        if r == 0:
            mix[...] = mixed
            for i in range(n_sp - 1, 0, -1):
                mix_copy(i).start()
        emit(r, mixed)

    def mix_copy(i):
        return remote(mix, mix, mix_send.at[i], mix_recv, order[i], fs, tp)

    def borrow(r):
        mix_copy(0).wait_recv()
        emit(r, mix[...])

    def emit(r, mixed):
        value = jnp.dot(mixed, wo[...].reshape(2 * head, span), preferred_element_type=f32).astype(bf16)
        for f in range(n_fs):
            for t in range(n_tp):
                at = (f * n_tp + t) * own_rows
                part[r, t, pl.ds(f * own_rows, own_rows), :] = value[at : at + own_rows]
        sib_copy(r).start()

    def reduce_pair(r):
        sib_copy(r).wait_recv()
        total = part[r, tp].astype(f32) + sib[r].astype(f32)
        red[r] = total.astype(bf16).reshape(n_fs, own_rows, span)
        for j in range(3):
            rs_copy(r, j).start()

    def collect(r):
        shares = rcv.at[r]
        remote(shares, shares, rs_send.at[r], rs_recv.at[r], sp, fs, tp).wait_recv()
        total = red[r, fs].astype(f32)
        for j in range(n_fs - 1):
            total = total + rcv[r, j].astype(f32)
        fin[r] = total.astype(bf16)

        @pl.when(r != sp)
        def _():
            fin_copy(r).start()

    dest = {"X": (sp, side, tp), "Y": (sp, ahead, tp), "D": (sp, corner, tp), "S": (sp, fs, mate)}
    stages = {"finish": finish, "borrow": borrow, "reduce": reduce_pair, "collect": collect}
    row_plans = [row_plan(n_sp, plane) for plane in range(n_sp)]

    all_decays = decays.at[pl.ds(0, n_sp - 1)]
    far_decays = remote(all_decays, all_decays, decay_send, decay_recv, sp, fs, tp)
    for flags, kind, *step in plan:
        if kind == "own":
            i = step[0]
            send_tok(flags, "Z", 0, order[i], fs, tp)
            remote(
                decays.at[sp], decays.at[sp], decay_send, decay_recv, order[i], fs, tp
            ).start()
        elif kind == "pass":
            send_tok(flags, *step[:2], *dest[step[2]])
        elif kind == "corner":
            far = step[0] >= DOWN
            if not (far and "a" in flags):
                send_tok(flags + "b" * (far and "b" not in flags), "Z", step[0], *dest["D"])
        elif kind == "down":
            if "a" not in flags:
                send_tok(flags + "h", "D", 0, 0, fs, tp)
        elif kind == "wait":
            run(flags, tok_copy(*step, sp, fs, tp).wait_recv)
        elif kind == "project":
            run(flags, functools.partial(project, step[0]))
        else:
            i = step[0]
            for plane in range(n_sp):

                def rows_done(ops=row_plans[plane][i]):
                    for stage, r in ops:
                        stages[stage](r)

                if row_plans[plane][i]:
                    pl.when(sp == plane)(rows_done)

    others = got.at[pl.ds(0, n_sp - 1)]
    arrived = remote(others, others, fin_send, fin_recv, sp, fs, tp)
    arrived.wait_recv()
    for c in range(n_sp):
        out[:, c * span : (c + 1) * span] = jnp.where(sp == c, fin[c], got[c])

    for plane, count in enumerate(pending):
        sent = x_all.at[pl.ds(0, count * own_rows)]
        pl.when(sp == plane)(
            remote(sent, sent, tok_send, mate_recv.at[0], sp, fs, tp).wait_send
        )
    far_decays.wait_send()
    halves = part.at[:, 0]
    remote(halves, halves, sib_send, sib_recv.at[0], sp, fs, tp).wait_send()
    for r in range(n_sp):
        shares = rcv.at[r]
        remote(shares, shares, rs_send.at[r], rs_recv.at[r], sp, fs, tp).wait_send()
    arrived.wait_send()

    @pl.when(sp == 0)
    def _():
        for i in range(1, n_sp):
            mix_copy(i).wait_send()


def whole_call(mesh_sizes, args):
    n_sp, n_fs, n_tp = mesh_sizes
    tokens, ret_query, diff_query, out_weight = args[0], args[2], args[8], args[13]
    own_rows, width = tokens.shape
    rows = own_rows * n_fs * n_tp
    head = ret_query.shape[1]
    span = out_weight.shape[2]
    plan = gather_plan(n_sp)
    hbm = pl.BlockSpec(memory_space=pltpu.HBM)
    dma = pltpu.SemaphoreType.DMA
    loaded = lambda i: pltpu.VMEM(args[i].shape, args[i].dtype)
    return pl.pallas_call(
        functools.partial(whole_kernel, mesh_sizes, plan),
        out_shape=pltpu.VMEM(tokens.shape, bf16),
        in_specs=[hbm] * 14,
        out_specs=pl.BlockSpec(memory_space=pltpu.VMEM),
        scratch_shapes=[
            pltpu.VMEM((n_sp * rows, width), bf16),
            pltpu.VMEM((width, 4 * head), bf16),
            pltpu.VMEM((2 * head, width), bf16),
            loaded(0),
            loaded(1),
            pltpu.VMEM((n_sp,) + args[5].shape, f32),
            *[loaded(i) for i in (6, 7, 11, 12)],
            loaded(13),
            pltpu.VMEM((n_sp, 2 * rows, head), bf16),
            *[pltpu.VMEM((n_sp, rows, head), bf16) for _ in range(5)],
            pltpu.VMEM((n_sp, head, head), f32),
            pltpu.VMEM((rows, 2 * head), bf16),
            pltpu.VMEM((n_sp, n_tp, n_fs * own_rows, span), bf16),
            pltpu.VMEM((n_sp, n_fs * own_rows, span), bf16),
            pltpu.VMEM((n_sp, n_fs, own_rows, span), bf16),
            pltpu.VMEM((n_sp, n_fs - 1, own_rows, span), bf16),
            *[pltpu.VMEM((n_sp, own_rows, span), bf16) for _ in range(2)],
            dma((10,)),
            dma,
            dma((n_sp, n_fs)),
            dma((n_sp,)),
            dma,
            dma,
            dma,
            dma((n_sp,)),
            dma((n_sp,)),
            dma((n_sp,)),
            dma,
            dma,
            dma((n_sp,)),
            dma,
        ],
        compiler_params=pltpu.CompilerParams(
            collective_id=0, has_side_effects=True, vmem_limit_bytes=66900000
        ),
        name="layer",
    )(*args)


def solution(mesh):
    n_sp, n_fs, n_tp = (mesh.shape[a] for a in ("sp", "fs", "tp"))

    def local(*args):
        args = list(args)
        tokens, ret_query, diff_query, out_weight = args[0], args[2], args[8], args[13]
        own_rows, width = tokens.shape
        rows = own_rows * n_fs * n_tp
        head = ret_query.shape[1]
        maps = diff_query.shape[2]
        assert 2 * maps == head
        assert args[5].shape[1] == rows == head
        ring = out_weight.shape[2] % 128 == 0 and 1 < n_sp <= 8
        whole = ring and n_sp == 4 and n_fs == 4 and n_tp == 2
        if not ring:
            args[13] = lax.all_gather(out_weight, "sp", axis=2, tiled=True)
        for i in (8, 9):
            args[i] = jnp.swapaxes(args[i], 1, 2).reshape(2 * maps, width)
        if whole:
            return whole_call((n_sp, n_fs, n_tp), args)
        chunks = n_sp if ring else 4
        vmem = pl.BlockSpec(memory_space=pltpu.VMEM)
        hbm = pl.BlockSpec(memory_space=pltpu.HBM)
        in_specs = [hbm] * 13 + [hbm if ring else vmem]
        dma = pltpu.SemaphoreType.DMA
        wo_shape = (n_sp,) + out_weight.shape if ring else (1, 2, 16, 128)
        return pl.pallas_call(
            functools.partial(kernel, (n_sp, n_fs, n_tp, ring)),
            out_shape=jax.ShapeDtypeStruct(tokens.shape, bf16),
            in_specs=in_specs,
            out_specs=vmem,
            scratch_shapes=[
                pltpu.VMEM((rows, width), bf16),
                pltpu.VMEM((width, 4 * head), bf16),
                pltpu.VMEM((4 * maps, width), bf16),
                *[pltpu.VMEM(args[i].shape, args[i].dtype) for i in (0, 1, 5, 6, 7, 11, 12)],
                pltpu.VMEM((n_sp, rows, 2 * head), bf16),
                pltpu.VMEM((n_sp, head + own_rows, head), bf16),
                pltpu.VMEM(wo_shape, bf16),
                pltpu.VMEM((n_tp, n_fs * own_rows, width), bf16),
                pltpu.VMEM((n_tp, n_fs * own_rows, width), bf16),
                pltpu.VMEM((n_fs, own_rows, width), bf16),
                pltpu.VMEM((n_fs, own_rows, width), bf16),
                dma((14,)),
                dma((TOKEN_CHUNKS, n_fs)),
                dma((TOKEN_CHUNKS, n_fs * n_tp)),
                dma((TOKEN_CHUNKS, n_fs, n_tp)),
                dma((n_sp,)),
                dma((n_sp,)),
                dma((n_sp,)),
                dma((n_sp,)),
                dma((2, n_sp)),
                dma((n_sp,)),
                dma((chunks, n_tp)),
                dma((chunks, n_tp)),
                dma((chunks, n_fs)),
                dma((chunks, n_fs)),
            ],
            compiler_params=pltpu.CompilerParams(
                collective_id=0, has_side_effects=True, vmem_limit_bytes=67043328
            ),
            name="layer",
        )(*args)

    in_specs = (
        P(("sp", "fs", "tp"), None),
        P(),
        P(None, ("fs", "tp")),
        P(None, ("fs", "tp")),
        P(None, ("fs", "tp")),
        P(("fs", "tp"), "sp"),
        P(("fs", "tp"), None, None),
        P(("fs", "tp")),
        P(None, None, ("fs", "tp")),
        P(None, None, ("fs", "tp")),
        P(None, ("fs", "tp")),
        P(("fs", "tp")),
        P(("fs", "tp")),
        P(None, ("fs", "tp"), "sp"),
    )
    out_specs = P(("sp", "fs", "tp"), None)
    return jax.shard_map(local, mesh=mesh, in_specs=in_specs, out_specs=out_specs, check_vma=False)
```

```python
import functools

import jax
import jax.numpy as jnp
from jax import lax
from jax.experimental import pallas as pl
from jax.experimental.pallas import tpu as pltpu
from jax.sharding import PartitionSpec as P

EPS = 1e-06
HUGE = 1e30
TOKEN_CHUNKS = 1
DOWN = 2
EARLY = True
SEQUENCE = ("c1", "s0", "d0", "c2b", "s1b", "c3b", "c2+a", "s1+a", "c3+a", "p0a", "q0", "c2-a", "s1-a", "c3-a", "d1+", "s2+", "d2+", "s3+", "d3+", "p0b", "d1-a", "p1a", "s2-a", "d2-a", "d3-a", "q1", "s3-a", "d1-b", "s2-b", "p1b", "d2-b", "m0+f", "p2", "s3-b", "d3-b", "q2", "p3", "q3")
f32 = jnp.float32
bf16 = jnp.bfloat16


def kernel(
    sizes,
    tokens,
    in_gain,
    ret_query,
    ret_key,
    ret_value,
    decay_log,
    init_state,
    ret_gain,
    diff_query,
    diff_key,
    diff_value,
    diff_lambda,
    diff_gain,
    out_weight,
    out,
    x_all,
    w_all,
    w_pair,
    tok_in,
    gain_in,
    decay_in,
    init_in,
    ret_gain_in,
    lambda_in,
    diff_gain_in,
    kv,
    st,
    wo,
    part,
    sib,
    red,
    rcv,
    load_sem,
    tok_send,
    tok_recv,
    fwd_send,
    kv_send,
    kv_recv,
    st_send,
    st_recv,
    wo_send,
    wo_recv,
    sib_send,
    sib_recv,
    rs_send,
    rs_recv,
):
    n_sp, n_fs, n_tp, ring = sizes
    own_rows, width = tokens.shape
    rows = own_rows * n_fs * n_tp
    head = ret_query.shape[1]
    maps = diff_query.shape[0] // 2
    sp, fs, tp = lax.axis_index("sp"), lax.axis_index("fs"), lax.axis_index("tp")
    half = max(n_fs // 2, 1)
    fs_peers = []
    for d in range(1, n_fs):
        if n_fs % 2 == 0:
            fs_peers.append(
                lax.rem(lax.div(fs, 2) + d // 2, half) * 2 + lax.rem(lax.rem(fs, 2) + d % 2, 2)
            )
        else:
            fs_peers.append(lax.rem(fs + d, n_fs))
    tp_peers = [lax.rem(tp + d, n_tp) for d in range(1, n_tp)]

    def remote(src, dst, send, recv, s, f, t):
        return pltpu.make_async_remote_copy(
            src_ref=src,
            dst_ref=dst,
            send_sem=send,
            recv_sem=recv,
            device_id=(s, f, t),
            device_id_type=pl.DeviceIdType.MESH,
        )

    barrier = pltpu.get_barrier_semaphore()

    def greet(s, f, t):
        pl.semaphore_signal(
            barrier, inc=1, device_id=(s, f, t), device_id_type=pl.DeviceIdType.MESH
        )

    for f in fs_peers:
        greet(sp, f, tp)
    for t in tp_peers:
        greet(sp, fs, t)

    def greet_sp(d, c):
        greet(lax.rem(sp + d, n_sp), fs, tp)
        return c

    if n_sp <= 8:
        for d in range(1, n_sp):
            greet_sp(d, 0)
    else:
        lax.fori_loop(1, n_sp, greet_sp, 0)

    def col(slot):
        return w_all.at[:, pl.ds(slot * head, head)]

    loads = [
        (tokens, tok_in),
        (in_gain, gain_in),
        (decay_log, decay_in),
        (init_state, init_in),
        (ret_gain, ret_gain_in),
        (diff_lambda, lambda_in),
        (diff_gain, diff_gain_in),
        (ret_query, col(0)),
        (ret_key, col(1)),
        (ret_value, col(2)),
        (diff_value, col(3)),
        (diff_key, w_pair.at[pl.ds(0, head)]),
        (diff_query, w_pair.at[pl.ds(head, head)]),
    ]
    load_copies = [
        pltpu.make_async_copy(src, dst, load_sem.at[i]) for i, (src, dst) in enumerate(loads)
    ]
    for c in load_copies:
        c.start()
    if ring:
        own_wo = pltpu.make_async_copy(out_weight, wo.at[sp], load_sem.at[len(loads)])
        own_wo.start()

    me = fs * n_tp + tp
    own = pl.ds(pl.multiple_of(me * own_rows, own_rows), own_rows)
    load_copies[0].wait()
    load_copies[1].wait()
    wide = tok_in[...].astype(f32)
    scale = lax.rsqrt(jnp.mean(wide * wide, axis=-1, keepdims=True) + EPS)
    x_all[own, :] = (wide * scale * gain_in[...].reshape(1, width)).astype(bf16)

    pl.semaphore_wait(barrier, len(fs_peers) + len(tp_peers) + n_sp - 1)

    cw = width // TOKEN_CHUNKS

    def block(rank, c):
        return x_all.at[
            pl.ds(pl.multiple_of(rank * own_rows, own_rows), own_rows), pl.ds(c * cw, cw)
        ]

    def tok_copy(c, rank, send, f, t):
        return remote(block(rank, c), block(rank, c), send, tok_recv.at[c, rank], sp, f, t)

    pending = []
    for c in range(TOKEN_CHUNKS):
        for i, f in enumerate(fs_peers):
            cp = tok_copy(c, me, tok_send.at[c, i], f, tp)
            cp.start()
            pending.append(cp)
        for i, t in enumerate(tp_peers):
            cp = tok_copy(c, me, fwd_send.at[c, n_fs - 1, i], fs, t)
            cp.start()
            pending.append(cp)

    def wo_copy(origin, way, step):
        src = out_weight if step == 0 else wo.at[origin]
        dest = sp + 1 - 2 * way
        return remote(
            src, wo.at[origin], wo_send.at[way, step], wo_recv.at[origin], dest, fs, tp
        )

    def each_way(step, go):
        for way in range(2):
            origin = sp - step if way == 0 else sp + step
            inside = origin >= 0 if way == 0 else origin < n_sp
            onward = sp < n_sp - 1 if way == 0 else sp > 0

            @pl.when(jnp.logical_and(inside, onward))
            def _():
                go(wo_copy(lax.rem(origin + n_sp, n_sp), way, step))

    def pass_on(step):
        def go(cp):
            if step:
                cp.wait_recv()
            cp.start()

        each_way(step, go)

    if ring:
        pass_on(0)

    load_copies[2].wait()
    d_row = decay_in[...]
    row_at = lax.broadcasted_iota(jnp.int32, (rows, rows), 0)
    col_at = lax.broadcasted_iota(jnp.int32, (rows, rows), 1)
    lower = row_at >= col_at
    d_wide = jnp.broadcast_to(d_row, (rows, rows))
    cum_col = jnp.sum(jnp.where(lower, d_wide, 0.0), axis=1, keepdims=True)
    d_col = jnp.sum(jnp.where(row_at == col_at, d_wide, 0.0), axis=1, keepdims=True)
    cum_row = jnp.sum(jnp.where(row_at <= col_at, d_col, 0.0), axis=0, keepdims=True)
    cum_last = jnp.sum(d_row, axis=1, keepdims=True)
    fade = jnp.exp(jnp.where(lower, cum_col - cum_row, -HUGE)) * head ** (-0.5)
    key_weight = jnp.exp(cum_last - cum_col) * head ** (-0.5)
    query_weight = jnp.exp(cum_col)
    decay = jnp.broadcast_to(jnp.exp(cum_last), (own_rows, head))
    decay_high = decay.astype(bf16).astype(f32)
    first = lax.broadcasted_iota(jnp.int32, (own_rows, head), 0) < own_rows // 2
    st[sp, pl.ds(head, own_rows), :] = jnp.where(first, decay_high, decay - decay_high).astype(bf16)

    for c in load_copies[3:]:
        c.wait()

    total = None
    for c in range(TOKEN_CHUNKS):
        if ring and c == TOKEN_CHUNKS - 1:
            pass_on(1)
        for k, f in enumerate(fs_peers):
            rank = f * n_tp + tp
            tok_copy(c, rank, tok_send.at[c, k], fs, tp).wait_recv()
            for i, t in enumerate(tp_peers):
                cp = tok_copy(c, rank, fwd_send.at[c, k, i], fs, t)
                cp.start()
                pending.append(cp)
        for t in tp_peers:
            for f in [fs] + fs_peers:
                tok_copy(c, f * n_tp + t, tok_send.at[c, 0], fs, tp).wait_recv()
        cols = slice(c * cw, (c + 1) * cw)
        piece = (
            jnp.dot(x_all[:, cols], w_all[cols, :], preferred_element_type=f32),
            lax.dot_general(
                x_all[:, cols],
                w_pair[:, cols],
                (((1,), (1,)), ((), ())),
                preferred_element_type=f32,
            ),
        )
        total = piece if total is None else (total[0] + piece[0], total[1] + piece[1])
    proj, pairs = total[0].astype(bf16), total[1].astype(bf16)
    ret_q, ret_k, ret_v, diff_v = (proj[:, i * head : (i + 1) * head] for i in range(4))
    diff_k, diff_q = pairs[:, :head], pairs[:, head:]
    kv[sp, :, :head] = diff_k
    kv[sp, :, head:] = diff_v

    def to_later(buf, send, recv, go):
        def one(d, c):
            @pl.when(sp + d < n_sp)
            def _():
                cp = remote(buf.at[sp], buf.at[sp], send.at[d], recv.at[sp], sp + d, fs, tp)
                go(cp)

            return c

        if n_sp <= 8:
            for d in range(n_sp - 1, 0, -1):
                one(d, 0)
        else:
            lax.fori_loop(1, n_sp, one, 0)

    to_later(kv, kv_send, kv_recv, lambda cp: cp.start())
    weighted = (ret_k.astype(f32) * key_weight).astype(bf16)
    state = lax.dot_general(
        weighted, ret_v, (((0,), (0,)), ((), ())), preferred_element_type=f32
    )
    st[sp, pl.ds(0, head), :] = state.astype(bf16)
    to_later(st, st_send, st_recv, lambda cp: cp.start())

    scores = lax.dot_general(ret_q, ret_k, (((1,), (1,)), ((), ())), preferred_element_type=f32)
    inner = jnp.dot((scores * fade).astype(bf16), ret_v, preferred_element_type=f32)
    lane = lax.broadcasted_iota(jnp.int32, (rows, 2 * maps), 1)
    zero = jnp.zeros_like(diff_q)
    pair_q = jnp.concatenate(
        [jnp.where(lane < maps, diff_q, zero), jnp.where(lane < maps, zero, diff_q)], axis=0
    )

    def one_block(keys, values, allowed):
        s = lax.dot_general(pair_q, keys, (((1,), (1,)), ((), ())), preferred_element_type=f32)
        s = s * maps ** (-0.5)
        if allowed is not None:
            s = jnp.where(allowed, s, -HUGE)
        peak = jnp.max(s, axis=1, keepdims=True)
        w = jnp.exp(s - peak)
        return (
            peak,
            jnp.sum(w, axis=1, keepdims=True),
            jnp.dot(w.astype(bf16), values, preferred_element_type=f32),
        )

    peak, whole, summed = one_block(diff_k, diff_v, jnp.concatenate([lower, lower], axis=0))

    if ring:
        for step in range(2, n_sp - 1):
            pass_on(step)

    def earlier(d, carry):
        peak, whole, summed, run, entering = carry
        b = sp - d
        remote(kv.at[b], kv.at[b], kv_send.at[0], kv_recv.at[b], sp, fs, tp).wait_recv()
        peak_b, whole_b, sum_b = one_block(kv[b, :, :head], kv[b, :, head:], None)
        top = jnp.maximum(peak, peak_b)
        before, after = jnp.exp(peak - top), jnp.exp(peak_b - top)
        remote(st.at[b], st.at[b], st_send.at[0], st_recv.at[b], sp, fs, tp).wait_recv()
        entering = entering + run * st[b, pl.ds(0, head), :].astype(f32)
        tail = st[b, pl.ds(head, own_rows), :].astype(f32)
        last = own_rows // 2
        return (
            top,
            whole * before + whole_b * after,
            summed * before + sum_b * after,
            run * (tail[0:1] + tail[last : last + 1]),
            entering,
        )

    peak, whole, summed, run, entering = lax.fori_loop(
        1,
        sp + 1,
        earlier,
        (peak, whole, summed, jnp.ones((1, head), f32), jnp.zeros((head, head), f32)),
    )
    entering = entering + run * init_in[0].astype(f32)
    reached = jnp.dot(ret_q, entering.astype(bf16), preferred_element_type=f32)
    ret_out = inner + query_weight * reached
    centre = ret_out - jnp.mean(ret_out, axis=-1, keepdims=True)
    ret_mix = (
        centre
        * lax.rsqrt(jnp.mean(centre * centre, axis=-1, keepdims=True) + EPS)
        * ret_gain_in[...].reshape(1, head)
    ).astype(bf16)
    lam = lambda_in[...].reshape(1, 1)
    ratio = summed / whole
    diff_out = ratio[:rows] - lam * ratio[rows:]
    diff_mix = (
        diff_out
        * lax.rsqrt(jnp.mean(diff_out * diff_out, axis=-1, keepdims=True) + EPS)
        * diff_gain_in[...].reshape(1, head)
    ).astype(bf16)
    mixed = jnp.concatenate([ret_mix, diff_mix], axis=1)

    if ring:
        own_wo.wait()
        order = [sp]
        low, high = sp - 1, sp + 1
        for _ in range(1, n_sp):
            down = jnp.logical_and(
                low >= 0, jnp.logical_or(high >= n_sp, sp - low <= high - sp)
            )
            order.append(jnp.where(down, low, high))
            low, high = jnp.where(down, low - 1, low), jnp.where(down, high, high + 1)
        span = out_weight.shape[2]
    else:
        order = list(range(4))
        span = width // 4

    def columns(s):
        if isinstance(s, int):
            return pl.ds(s * span, span)
        return pl.ds(pl.multiple_of(s * span, 128), span)

    def sib_copy(k, i, t):
        cols = columns(order[k])
        return remote(
            part.at[t, :, cols], sib.at[tp, :, cols], sib_send.at[k, i], sib_recv.at[k, tp], sp, fs, t
        )

    def rs_copy(k, i, f):
        cols = columns(order[k])
        return remote(
            red.at[f, :, cols], rcv.at[fs, :, cols], rs_send.at[k, i], rs_recv.at[k, fs], sp, f, tp
        )

    def reduce_pair(k):
        cols = columns(order[k])
        acc = part[tp, :, cols].astype(f32)
        for i, t in enumerate(tp_peers):
            remote(
                part.at[t, :, cols], sib.at[t, :, cols], sib_send.at[k, i], sib_recv.at[k, t], sp, fs, tp
            ).wait_recv()
            acc = acc + sib[t, :, cols].astype(f32)
        red[:, :, cols] = acc.astype(bf16).reshape(n_fs, own_rows, span)
        for i, f in enumerate(fs_peers):
            cp = rs_copy(k, i, f)
            cp.start()
            pending.append(cp)

    for k, s in enumerate(order):
        if ring and k:

            @pl.when(jnp.logical_or(sp == 0, sp == n_sp - 1))
            def _():
                wo_copy(s, 0, k).wait_recv()

        if ring:
            w = wo[s].reshape(2 * head, span)
        else:
            w = out_weight[:, :, s * span : (s + 1) * span].reshape(2 * head, span)
        value = jnp.dot(mixed, w, preferred_element_type=f32).astype(bf16)
        cols = columns(s)
        for f in range(n_fs):
            for t in range(n_tp):
                at = (f * n_tp + t) * own_rows
                part[t, pl.ds(f * own_rows, own_rows), cols] = value[at : at + own_rows]
        for i, t in enumerate(tp_peers):
            cp = sib_copy(k, i, t)
            cp.start()
            pending.append(cp)
        if k >= 1:
            reduce_pair(k - 1)
    reduce_pair(len(order) - 1)

    for k, s in enumerate(order):
        cols = columns(s)
        acc = red[fs, :, cols].astype(f32)
        for i, f in enumerate(fs_peers):
            remote(
                red.at[f, :, cols], rcv.at[f, :, cols], rs_send.at[k, i], rs_recv.at[k, f], sp, fs, tp
            ).wait_recv()
            acc = acc + rcv[f, :, cols].astype(f32)
        out[:, cols] = acc.astype(bf16)

    for cp in pending:
        cp.wait_send()
    if ring:
        for step in range(n_sp - 1):
            each_way(step, lambda cp: cp.wait_send())
    to_later(kv, kv_send, kv_recv, lambda cp: cp.wait_send())
    to_later(st, st_send, st_recv, lambda cp: cp.wait_send())


def plane_order(sp, n_sp):
    return [jnp.where(i <= sp, sp - i, i) for i in range(n_sp)]


def gather_plan(n_sp):
    plan = []
    for i in range(1, n_sp):
        plan.append(("", "own", i))
    for d in "XYDS":
        plan.append(("", "pass", "Z", 0, d))

    def column(i):
        plan.append(("wait", "Z", i))
        plan.extend(("pass", "Z", i, d) for d in "XYS")
        plan.append(("corner", i))

    def sides(i):
        for k in "XY":
            plan.append(("wait", k, i))
            plan.append(("pass", k, i, "S"))

    def corner(i):
        plan.append(("wait", "D", i))
        if i == 0:
            plan.append(("down",))
        plan.append(("pass", "D", i, "S"))

    for step in SEQUENCE:
        name, i, flags = step[0], int(step[1]), step[2:]
        begin = len(plan)
        if name in "pqm":
            plan.append(({"p": "project", "q": "rows", "m": "borrow"}[name], i))
        else:
            {"c": column, "s": sides, "d": corner}[name](i)
        plan[begin:] = [(flags,) + entry for entry in plan[begin:]]
    return plan


def row_plan(n_sp, plane):
    last = n_sp - 1
    steps, waiting, late, own = [], [], [], []
    for i in range(n_sp):
        ready = list(range(i + 1)) if i == plane else [i] if i > plane else []
        if plane:
            ready = [r for r in ready if r]
        if plane < i == last - 1:
            late, ready = ready, []
        elif 0 < i == plane < last - 1:
            own, ready = ready[-1:], ready[:-1]
        if i == last:
            ready = ready + late + own
        ops, fresh = [], []
        if plane and i == last - 1:
            ops.append(("borrow", 0))
            fresh.append(0)
        if plane == last == i or (EARLY and plane == 0 and i == 1):
            ops.append(("reduce", waiting.pop()))
        for n, r in enumerate(ready):
            ops.append(("finish", r))
            if i == last and n == 0:
                ops += [("reduce", b) for b in waiting]
            if fresh and i >= last - 1:
                ops.append(("reduce", fresh.pop(0)))
            fresh.append(r)
        if i == last:
            if plane:
                ops.append(("collect", 0))
            ops += [("reduce", r) for r in fresh]
            done = [op[1] for step in steps + [ops] for op in step if op[0] == "reduce"]
            ops += [("collect", r) for r in done if r or not plane]
        else:
            waiting += fresh
        steps.append(ops)
    return steps


def whole_kernel(
    sizes,
    plan,
    tokens,
    in_gain,
    ret_query,
    ret_key,
    ret_value,
    decay_log,
    init_state,
    ret_gain,
    diff_query,
    diff_key,
    diff_value,
    diff_lambda,
    diff_gain,
    out_weight,
    out,
    x_all,
    w_all,
    w_pair,
    tok_in,
    gain_in,
    decays,
    init_in,
    ret_gain_in,
    lambda_in,
    diff_gain_in,
    wo,
    pair_q,
    ret_q,
    ret_k,
    ret_v,
    diff_k,
    diff_v,
    states,
    mix,
    part,
    sib,
    red,
    rcv,
    fin,
    got,
    load_sem,
    tok_send,
    tok_recv,
    mate_recv,
    decay_send,
    decay_recv,
    sib_send,
    sib_recv,
    rs_send,
    rs_recv,
    fin_send,
    fin_recv,
    mix_send,
    mix_recv,
):
    n_sp, n_fs, n_tp = sizes
    own_rows, width = tokens.shape
    rows = own_rows * n_fs * n_tp
    head = ret_query.shape[1]
    maps = diff_query.shape[0] // 2
    span = out_weight.shape[2]
    sp, fs, tp = lax.axis_index("sp"), lax.axis_index("fs"), lax.axis_index("tp")
    side = fs + 1 - 2 * lax.rem(fs, 2)
    ahead = lax.rem(fs + 2, 4)
    corner = side + ahead - fs
    mate = 1 - tp
    chip = {"Z": fs, "X": side, "Y": ahead, "D": corner}
    order = plane_order(sp, n_sp)

    def remote(src, dst, send, recv, s, f, t):
        return pltpu.make_async_remote_copy(
            src_ref=src,
            dst_ref=dst,
            send_sem=send,
            recv_sem=recv,
            device_id=(s, f, t),
            device_id_type=pl.DeviceIdType.MESH,
        )

    barrier = pltpu.get_barrier_semaphore()
    peers = [(order[i], fs, tp) for i in range(1, n_sp)]
    peers += [(sp, f, tp) for f in (side, ahead, corner)] + [(sp, fs, mate)]
    for peer in peers:
        pl.semaphore_signal(
            barrier, inc=1, device_id=peer, device_id_type=pl.DeviceIdType.MESH
        )

    def col(slot):
        return w_all.at[:, pl.ds(slot * head, head)]

    loads = [
        (tokens, tok_in),
        (in_gain, gain_in),
        (decay_log, decays.at[sp]),
        (init_state, init_in),
        (ret_gain, ret_gain_in),
        (diff_lambda, lambda_in),
        (diff_gain, diff_gain_in),
        (ret_query, col(0)),
        (ret_key, col(1)),
        (ret_value, col(2)),
        (diff_value, col(3)),
        (diff_key, w_pair.at[pl.ds(0, head)]),
        (diff_query, w_pair.at[pl.ds(head, head)]),
        (out_weight, wo),
    ]
    groups = [0, 1, 2, 3, 4, 5, 6, 7, 7, 7, 7, 8, 8, 9]
    load_copies = [
        pltpu.make_async_copy(src, dst, load_sem.at[i]) for i, (src, dst) in zip(groups, loads)
    ]
    later_loads = load_copies[3:7] + [
        pltpu.make_async_copy(w_all, w_all, load_sem.at[7]),
        pltpu.make_async_copy(w_pair, w_pair, load_sem.at[8]),
        load_copies[13],
    ]
    for c in load_copies:
        c.start()
    me = (sp * n_fs + fs) * n_tp + tp
    own = pl.ds(pl.multiple_of(me * own_rows, own_rows), own_rows)
    load_copies[0].wait()
    load_copies[1].wait()
    wide = tok_in[...].astype(f32)
    scale = lax.rsqrt(jnp.mean(wide * wide, axis=-1, keepdims=True) + EPS)
    x_all[own, :] = (wide * scale * gain_in[...].reshape(1, width)).astype(bf16)
    load_copies[2].wait()
    pl.semaphore_wait(barrier, len(peers))

    pending = [0] * n_sp

    def block(k, i, t):
        rank = (order[i] * n_fs + chip[k]) * n_tp + t
        return x_all.at[pl.ds(pl.multiple_of(rank * own_rows, own_rows), own_rows)]

    def tok_copy(k, i, s, f, dest):
        recv = mate_recv.at[order[i]] if dest is mate else tok_recv.at[order[i], chip[k]]
        return remote(block(k, i, tp), block(k, i, tp), tok_send, recv, s, f, dest)

    tests = {"+": tp == 1, "-": tp == 0, "a": sp == 0, "b": sp > 0, "h": sp >= DOWN, "f": sp > 1}
    least = {"b": 1, "h": DOWN}

    def run(flags, go):
        if flags:
            pl.when(functools.reduce(jnp.logical_and, [tests[f] for f in flags]))(go)
        else:
            go()

    def send_tok(flags, *where):
        if "-" not in flags:
            for plane in range(n_sp):
                if plane >= max(least.get(f, 0) for f in flags + "+") and not ("a" in flags and plane):
                    pending[plane] += 1
        run(flags, tok_copy(*where).start)

    row_at = lax.broadcasted_iota(jnp.int32, (rows, rows), 0)
    col_at = lax.broadcasted_iota(jnp.int32, (rows, rows), 1)
    lower = row_at >= col_at
    lane = lax.broadcasted_iota(jnp.int32, (rows, 2 * maps), 1)

    def cumulate(d_row):
        d_wide = jnp.broadcast_to(d_row, (rows, rows))
        return d_wide, jnp.sum(jnp.where(lower, d_wide, 0.0), axis=1, keepdims=True)

    def project(i):
        p = order[i]
        quarter = x_all.at[pl.ds(0, n_fs * own_rows)]
        remote(quarter, quarter, tok_send, mate_recv.at[p], sp, fs, tp).wait_recv()
        if i == 1:
            far_decays.wait_recv()
        if i == 0:
            for c in later_loads:
                c.wait()
        x = x_all[pl.ds(pl.multiple_of(p * rows, rows), rows), :]
        proj = jnp.dot(x, w_all[...], preferred_element_type=f32).astype(bf16)
        pairs = lax.dot_general(
            x, w_pair[...], (((1,), (1,)), ((), ())), preferred_element_type=f32
        ).astype(bf16)
        q, k, v, dv = (proj[:, j * head : (j + 1) * head] for j in range(4))
        dk, dq = pairs[:, :head], pairs[:, head:]
        zero = jnp.zeros_like(dq)
        d_row = decays[p]
        cum_col = cumulate(d_row)[1]
        cum_last = jnp.sum(d_row, axis=1, keepdims=True)
        key_weight = jnp.exp(cum_last - cum_col) * head ** (-0.5)
        states[p] = lax.dot_general(
            (k.astype(f32) * key_weight).astype(bf16),
            v,
            (((0,), (0,)), ((), ())),
            preferred_element_type=f32,
        )
        ret_q[p], ret_k[p], ret_v[p], diff_k[p], diff_v[p] = q, k, v, dk, dv
        pair_q[p] = jnp.concatenate(
            [jnp.where(lane < maps, dq, zero), jnp.where(lane < maps, zero, dq)], axis=0
        )

    fs_peers = [corner, side, ahead]

    def sib_copy(r):
        return remote(part.at[r, mate], sib.at[r], sib_send, sib_recv.at[r], sp, fs, mate)

    def place(f):
        return jnp.where(fs > f, fs - 1, fs)

    def rs_copy(r, j):
        f = fs_peers[j]
        return remote(red.at[r, f], rcv.at[r, place(f)], rs_send.at[r], rs_recv.at[r], sp, f, tp)

    def fin_copy(r):
        return remote(fin.at[r], got.at[sp], fin_send, fin_recv, r, fs, tp)

    def finish(r):
        q, k, v = ret_q[r], ret_k[r], ret_v[r]
        scores = lax.dot_general(q, k, (((1,), (1,)), ((), ())), preferred_element_type=f32)
        keys = diff_k[0 : r + 1].reshape((r + 1) * rows, head)
        s = lax.dot_general(
            pair_q[r], keys, (((1,), (1,)), ((), ())), preferred_element_type=f32
        )
        s = [s[:, b * rows : (b + 1) * rows] for b in range(r + 1)]
        s[r] = jnp.where(jnp.concatenate([lower, lower], axis=0), s[r], -HUGE)
        entering = init_in[0].astype(f32)
        for b in range(r):
            entering = jnp.exp(jnp.sum(decays[b], axis=1, keepdims=True)) * entering + states[b]
        reached = jnp.dot(q, entering.astype(bf16), preferred_element_type=f32)
        d_wide, cum_col = cumulate(decays[r])
        d_col = jnp.sum(jnp.where(row_at == col_at, d_wide, 0.0), axis=1, keepdims=True)
        cum_row = jnp.sum(jnp.where(row_at <= col_at, d_col, 0.0), axis=0, keepdims=True)
        fade = jnp.exp(jnp.where(lower, cum_col - cum_row, -HUGE)) * head ** (-0.5)
        inner = jnp.dot((scores * fade).astype(bf16), v, preferred_element_type=f32)
        peak = jnp.max(functools.reduce(jnp.maximum, s), axis=1, keepdims=True)
        w = [jnp.exp((part_s - peak) * maps ** (-0.5)) for part_s in s]
        whole = jnp.sum(functools.reduce(jnp.add, w), axis=1, keepdims=True)
        summed = functools.reduce(
            jnp.add,
            [
                jnp.dot(w[b].astype(bf16), diff_v[b], preferred_element_type=f32)
                for b in range(r + 1)
            ],
        )
        ret_out = inner + jnp.exp(cum_col) * reached
        centre = ret_out - jnp.mean(ret_out, axis=-1, keepdims=True)
        ret_mix = (
            centre
            * lax.rsqrt(jnp.mean(centre * centre, axis=-1, keepdims=True) + EPS)
            * ret_gain_in[...].reshape(1, head)
        ).astype(bf16)
        ratio = summed * (1.0 / whole)
        diff_out = ratio[:rows] - lambda_in[...].reshape(1, 1) * ratio[rows:]
        diff_mix = (
            diff_out
            * lax.rsqrt(jnp.mean(diff_out * diff_out, axis=-1, keepdims=True) + EPS)
            * diff_gain_in[...].reshape(1, head)
        ).astype(bf16)
        mixed = jnp.concatenate([ret_mix, diff_mix], axis=1)
        if r == 0:
            mix[...] = mixed
            for i in range(n_sp - 1, 0, -1):
                mix_copy(i).start()
        emit(r, mixed)

    def mix_copy(i):
        return remote(mix, mix, mix_send.at[i], mix_recv, order[i], fs, tp)

    def borrow(r):
        mix_copy(0).wait_recv()
        emit(r, mix[...])

    def emit(r, mixed):
        value = jnp.dot(mixed, wo[...].reshape(2 * head, span), preferred_element_type=f32).astype(bf16)
        for f in range(n_fs):
            for t in range(n_tp):
                at = (f * n_tp + t) * own_rows
                part[r, t, pl.ds(f * own_rows, own_rows), :] = value[at : at + own_rows]
        sib_copy(r).start()

    def reduce_pair(r):
        sib_copy(r).wait_recv()
        total = part[r, tp].astype(f32) + sib[r].astype(f32)
        red[r] = total.astype(bf16).reshape(n_fs, own_rows, span)
        for j in range(3):
            rs_copy(r, j).start()

    def collect(r):
        shares = rcv.at[r]
        remote(shares, shares, rs_send.at[r], rs_recv.at[r], sp, fs, tp).wait_recv()
        total = red[r, fs].astype(f32)
        for j in range(n_fs - 1):
            total = total + rcv[r, j].astype(f32)
        fin[r] = total.astype(bf16)

        @pl.when(r != sp)
        def _():
            fin_copy(r).start()

    dest = {"X": (sp, side, tp), "Y": (sp, ahead, tp), "D": (sp, corner, tp), "S": (sp, fs, mate)}
    stages = {"finish": finish, "borrow": borrow, "reduce": reduce_pair, "collect": collect}
    row_plans = [row_plan(n_sp, plane) for plane in range(n_sp)]

    all_decays = decays.at[pl.ds(0, n_sp - 1)]
    far_decays = remote(all_decays, all_decays, decay_send, decay_recv, sp, fs, tp)
    for flags, kind, *step in plan:
        if kind == "own":
            i = step[0]
            send_tok(flags, "Z", 0, order[i], fs, tp)
            remote(
                decays.at[sp], decays.at[sp], decay_send, decay_recv, order[i], fs, tp
            ).start()
        elif kind == "pass":
            send_tok(flags, *step[:2], *dest[step[2]])
        elif kind == "corner":
            far = step[0] >= DOWN
            if not (far and "a" in flags):
                send_tok(flags + "b" * (far and "b" not in flags), "Z", step[0], *dest["D"])
        elif kind == "down":
            if "a" not in flags:
                send_tok(flags + "h", "D", 0, 0, fs, tp)
        elif kind == "wait":
            run(flags, tok_copy(*step, sp, fs, tp).wait_recv)
        elif kind == "project":
            run(flags, functools.partial(project, step[0]))
        elif kind == "borrow":
            run(flags, functools.partial(borrow, 0))
        else:
            i = step[0]
            for plane in range(n_sp):

                def rows_done(ops=row_plans[plane][i], plane=plane):
                    for stage, r in ops:
                        if stage == "borrow" and plane > 1:
                            run("-", functools.partial(borrow, r))
                        else:
                            stages[stage](r)

                if row_plans[plane][i]:
                    pl.when(sp == plane)(rows_done)

    others = got.at[pl.ds(0, n_sp - 1)]
    arrived = remote(others, others, fin_send, fin_recv, sp, fs, tp)
    arrived.wait_recv()
    for c in range(n_sp):
        out[:, c * span : (c + 1) * span] = jnp.where(sp == c, fin[c], got[c])

    for plane, count in enumerate(pending):
        sent = x_all.at[pl.ds(0, count * own_rows)]
        pl.when(sp == plane)(
            remote(sent, sent, tok_send, mate_recv.at[0], sp, fs, tp).wait_send
        )
    far_decays.wait_send()
    halves = part.at[:, 0]
    remote(halves, halves, sib_send, sib_recv.at[0], sp, fs, tp).wait_send()
    for r in range(n_sp):
        shares = rcv.at[r]
        remote(shares, shares, rs_send.at[r], rs_recv.at[r], sp, fs, tp).wait_send()
    arrived.wait_send()

    @pl.when(sp == 0)
    def _():
        for i in range(1, n_sp):
            mix_copy(i).wait_send()


def whole_call(mesh_sizes, args):
    n_sp, n_fs, n_tp = mesh_sizes
    tokens, ret_query, diff_query, out_weight = args[0], args[2], args[8], args[13]
    own_rows, width = tokens.shape
    rows = own_rows * n_fs * n_tp
    head = ret_query.shape[1]
    span = out_weight.shape[2]
    plan = gather_plan(n_sp)
    hbm = pl.BlockSpec(memory_space=pltpu.HBM)
    dma = pltpu.SemaphoreType.DMA
    loaded = lambda i: pltpu.VMEM(args[i].shape, args[i].dtype)
    return pl.pallas_call(
        functools.partial(whole_kernel, mesh_sizes, plan),
        out_shape=pltpu.VMEM(tokens.shape, bf16),
        in_specs=[hbm] * 14,
        out_specs=pl.BlockSpec(memory_space=pltpu.VMEM),
        scratch_shapes=[
            pltpu.VMEM((n_sp * rows, width), bf16),
            pltpu.VMEM((width, 4 * head), bf16),
            pltpu.VMEM((2 * head, width), bf16),
            loaded(0),
            loaded(1),
            pltpu.VMEM((n_sp,) + args[5].shape, f32),
            *[loaded(i) for i in (6, 7, 11, 12)],
            loaded(13),
            pltpu.VMEM((n_sp, 2 * rows, head), bf16),
            *[pltpu.VMEM((n_sp, rows, head), bf16) for _ in range(5)],
            pltpu.VMEM((n_sp, head, head), f32),
            pltpu.VMEM((rows, 2 * head), bf16),
            pltpu.VMEM((n_sp, n_tp, n_fs * own_rows, span), bf16),
            pltpu.VMEM((n_sp, n_fs * own_rows, span), bf16),
            pltpu.VMEM((n_sp, n_fs, own_rows, span), bf16),
            pltpu.VMEM((n_sp, n_fs - 1, own_rows, span), bf16),
            *[pltpu.VMEM((n_sp, own_rows, span), bf16) for _ in range(2)],
            dma((10,)),
            dma,
            dma((n_sp, n_fs)),
            dma((n_sp,)),
            dma,
            dma,
            dma,
            dma((n_sp,)),
            dma((n_sp,)),
            dma((n_sp,)),
            dma,
            dma,
            dma((n_sp,)),
            dma,
        ],
        compiler_params=pltpu.CompilerParams(
            collective_id=0, has_side_effects=True, vmem_limit_bytes=66900000
        ),
        name="layer",
    )(*args)


def solution(mesh):
    n_sp, n_fs, n_tp = (mesh.shape[a] for a in ("sp", "fs", "tp"))

    def local(*args):
        args = list(args)
        tokens, ret_query, diff_query, out_weight = args[0], args[2], args[8], args[13]
        own_rows, width = tokens.shape
        rows = own_rows * n_fs * n_tp
        head = ret_query.shape[1]
        maps = diff_query.shape[2]
        assert 2 * maps == head
        assert args[5].shape[1] == rows == head
        ring = out_weight.shape[2] % 128 == 0 and 1 < n_sp <= 8
        whole = ring and n_sp == 4 and n_fs == 4 and n_tp == 2
        if not ring:
            args[13] = lax.all_gather(out_weight, "sp", axis=2, tiled=True)
        for i in (8, 9):
            args[i] = jnp.swapaxes(args[i], 1, 2).reshape(2 * maps, width)
        if whole:
            return whole_call((n_sp, n_fs, n_tp), args)
        chunks = n_sp if ring else 4
        vmem = pl.BlockSpec(memory_space=pltpu.VMEM)
        hbm = pl.BlockSpec(memory_space=pltpu.HBM)
        in_specs = [hbm] * 13 + [hbm if ring else vmem]
        dma = pltpu.SemaphoreType.DMA
        wo_shape = (n_sp,) + out_weight.shape if ring else (1, 2, 16, 128)
        return pl.pallas_call(
            functools.partial(kernel, (n_sp, n_fs, n_tp, ring)),
            out_shape=jax.ShapeDtypeStruct(tokens.shape, bf16),
            in_specs=in_specs,
            out_specs=vmem,
            scratch_shapes=[
                pltpu.VMEM((rows, width), bf16),
                pltpu.VMEM((width, 4 * head), bf16),
                pltpu.VMEM((4 * maps, width), bf16),
                *[pltpu.VMEM(args[i].shape, args[i].dtype) for i in (0, 1, 5, 6, 7, 11, 12)],
                pltpu.VMEM((n_sp, rows, 2 * head), bf16),
                pltpu.VMEM((n_sp, head + own_rows, head), bf16),
                pltpu.VMEM(wo_shape, bf16),
                pltpu.VMEM((n_tp, n_fs * own_rows, width), bf16),
                pltpu.VMEM((n_tp, n_fs * own_rows, width), bf16),
                pltpu.VMEM((n_fs, own_rows, width), bf16),
                pltpu.VMEM((n_fs, own_rows, width), bf16),
                dma((14,)),
                dma((TOKEN_CHUNKS, n_fs)),
                dma((TOKEN_CHUNKS, n_fs * n_tp)),
                dma((TOKEN_CHUNKS, n_fs, n_tp)),
                dma((n_sp,)),
                dma((n_sp,)),
                dma((n_sp,)),
                dma((n_sp,)),
                dma((2, n_sp)),
                dma((n_sp,)),
                dma((chunks, n_tp)),
                dma((chunks, n_tp)),
                dma((chunks, n_fs)),
                dma((chunks, n_fs)),
            ],
            compiler_params=pltpu.CompilerParams(
                collective_id=0, has_side_effects=True, vmem_limit_bytes=67043328
            ),
            name="layer",
        )(*args)

    in_specs = (
        P(("sp", "fs", "tp"), None),
        P(),
        P(None, ("fs", "tp")),
        P(None, ("fs", "tp")),
        P(None, ("fs", "tp")),
        P(("fs", "tp"), "sp"),
        P(("fs", "tp"), None, None),
        P(("fs", "tp")),
        P(None, None, ("fs", "tp")),
        P(None, None, ("fs", "tp")),
        P(None, ("fs", "tp")),
        P(("fs", "tp")),
        P(("fs", "tp")),
        P(None, ("fs", "tp"), "sp"),
    )
    out_specs = P(("sp", "fs", "tp"), None)
    return jax.shard_map(local, mesh=mesh, in_specs=in_specs, out_specs=out_specs, check_vma=False)
```
